32 devices in a mesh: grp: 2 (over x), sp: 8 (over z, y), tp: 2 (over core).
Axes of the slice: x: 2, y: 2, z: 4, core: 2. Of those that a mesh axis runs over, the one named last changes fastest.
Arguments:
- tokens: bfloat16 [8192, 2048], P(('grp', 'sp', 'tp')), parts along dimension 0, may hold values from -60 to 60
- query_weight: bfloat16 [2048, 1024], P(None, 'tp'), may hold values from -0.125 to 0.125
- key_weight: bfloat16 [2048, 1024], P(None, 'tp'), may hold values from -0.125 to 0.125
- value_weight: bfloat16 [2048, 1024], P(None, 'tp'), may hold values from -0.125 to 0.125
- output_weight: bfloat16 [1024, 2048], P(None, 'tp'), may hold values from -1.5 to 1.5
Outputs:
- attended: bfloat16 [8192, 2048], P(('grp', 'sp'), 'tp'), parts along dimension 0
The draws below stay inside these ranges and needn't reach their ends.
There are 2 independent parts, one for each index of `grp`. The reference program is written for one: setup_inputs(seed, part) draws one part's arguments, and reference() takes and returns one part's arrays. A program takes and returns all parts, laid end to end along the dimension named above; an argument that names none is the same for every part. Nothing has to cross between parts.
All inputs are finite; a program needn't handle non-finite values.
Results may differ from the reference program's by a relative error of at most 0.012.
The reference program's roundings to bfloat16 on the way (of `queries`, `keys`, `values`, `weights` and `mixed`) count: a program that leaves them out, or rounds other values in their place, can miss the bound.
Values may be sent and summed in bfloat16 or wider, within the bound.
No kernel may reach another device: no remote copies, remote signals or barrier semaphores. Data moves between devices by JAX's collectives and lax.ppermute only.
A program may use at most 128 MiB of HBM per device.

```python
import jax
import jax.numpy as jnp
from jax import lax

D = 2048
HEADS = 8
HEAD = 128
REACH_STEPS = 128
MIDDLE_DILATION = 4
FAR_DILATION = 16
TOKENS = 4096


def draw_tokens(key, part):
    key_base = jax.random.fold_in(key, 11)
    base = jnp.clip(jax.random.normal(key_base, (TOKENS, D), jnp.float32), -6.0, 6.0)
    return base.astype(jnp.bfloat16)


def steps_of(rng, shape, cuts, smallest, largest):
    gain, own = 1.0, jax.random.fold_in(rng, 6)
    for position, blocks in cuts:
        draws = jnp.exp(jax.random.uniform(jax.random.fold_in(own, position), (blocks,), jnp.float32, smallest / len(cuts), largest / len(cuts)))
        gain = gain * jnp.repeat(draws, shape[position] // blocks).reshape([-1 if axis == position else 1 for axis in range(len(shape))])
    return gain


def gaussian(key, extent, deviation, reach, shards=(), kind=jnp.bfloat16):
    factor_of = steps_of(key, extent, shards, -0.22, 0.18) if shards else 1.0
    entries = jax.random.normal(key, extent, jnp.float32) * deviation * factor_of
    return jnp.minimum(jnp.maximum(entries, -reach), reach).astype(kind)


def setup_inputs(seed: int = 0, part: int = 0) -> dict:
    key_of = jax.random.split(jax.random.key(seed), 6)
    own_keys = jax.random.split(jax.random.fold_in(key_of[5], part), 6)
    tokens = draw_tokens(jax.random.fold_in(jax.random.fold_in(key_of[5], part), 71), part)
    query_weight = gaussian(key_of[1], (D, HEADS * HEAD), D ** -0.5, 0.125, ((1, 2),))
    key_weight = gaussian(key_of[2], (D, HEADS * HEAD), D ** -0.5, 0.125, ((1, 2),))
    value_weight = gaussian(key_of[3], (D, HEADS * HEAD), D ** -0.5, 0.125, ((1, 2),))
    output_weight = gaussian(key_of[4], (HEADS * HEAD, D), (REACH_STEPS // 8) ** -0.5, 1.5, ((1, 2),))
    return dict(tokens=tokens, query_weight=query_weight, key_weight=key_weight, value_weight=value_weight, output_weight=output_weight)


THETA_BASE = 500000.0


def rotate(values, positions):
    half = values.shape[-1] // 2
    inverse = THETA_BASE ** (-jnp.arange(half, dtype=jnp.float32) / half)
    angles = positions[:, None, None] * inverse
    cosine = jnp.cos(angles)
    sine = jnp.sin(angles)
    first = values[..., :half]
    second = values[..., half:]
    return jnp.concatenate([first * cosine - second * sine, second * cosine + first * sine], axis=-1)


def pattern(queries, keys, values, pattern_dilation):
    length = queries.shape[0]
    unit = pattern_dilation * REACH_STEPS
    padded = -(-length // unit) * unit
    blocks = padded // unit

    def regroup(array):
        array = jnp.pad(array, ((0, padded - length), (0, 0), (0, 0)))
        return array.reshape(blocks, REACH_STEPS, pattern_dilation, HEADS, HEAD).astype(jnp.float32)

    def with_prev(array):
        earlier = jnp.pad(array, ((1, 0), (0, 0), (0, 0), (0, 0), (0, 0)))[:-1]
        return jnp.concatenate([earlier, array], axis=1)

    query_sub = regroup(queries)
    key_sub = with_prev(regroup(keys))
    value_sub = with_prev(regroup(values))
    scores = jnp.einsum('nqrhd,nkrhd->nrhqk', query_sub, key_sub) * HEAD ** -0.5
    query_index = jnp.arange(REACH_STEPS)[:, None] + REACH_STEPS
    key_index = jnp.arange(2 * REACH_STEPS)[None, :]
    distance = query_index - key_index
    key_global = jnp.arange(blocks)[:, None, None] * REACH_STEPS + key_index[None] - REACH_STEPS
    allowed = ((distance >= 0) & (distance <= REACH_STEPS))[None] & (key_global >= 0)
    scores = jnp.where(allowed[:, None, None], scores, -jnp.inf)
    top = jnp.max(scores, axis=-1, keepdims=True)
    offset_keys = jnp.exp(scores - top)
    total = jnp.sum(offset_keys, axis=-1, keepdims=True)
    weights = lax.optimization_barrier((offset_keys / total).astype(jnp.bfloat16)).astype(jnp.float32)
    result = jnp.einsum('nrhqk,nkrhd->nqrhd', weights, value_sub).reshape(padded, HEADS, HEAD)[:length]
    lse = jnp.transpose((top + jnp.log(total))[..., 0], (0, 3, 1, 2)).reshape(padded, HEADS)[:length]
    return result, lse


def reference(tokens, query_weight, key_weight, value_weight, output_weight):
    length = tokens.shape[0]
    positions = jnp.arange(length).astype(jnp.float32)
    query_proj = jnp.dot(tokens, query_weight, preferred_element_type=jnp.float32).reshape(length, HEADS, HEAD)
    key_proj = jnp.dot(tokens, key_weight, preferred_element_type=jnp.float32).reshape(length, HEADS, HEAD)
    queries = rotate(query_proj, positions).astype(jnp.bfloat16)
    keys = rotate(key_proj, positions).astype(jnp.bfloat16)
    values = jnp.dot(tokens, value_weight, preferred_element_type=jnp.float32).astype(jnp.bfloat16)
    values = values.reshape(length, HEADS, HEAD)
    results = []
    lses = []
    for pattern_dilation in (1, MIDDLE_DILATION, FAR_DILATION):
        result, lse = pattern(queries, keys, values, pattern_dilation)
        results.append(result)
        lses.append(lse)
    mixing = jax.nn.softmax(jnp.stack(lses, axis=0), axis=0)
    mixed = jnp.sum(mixing[..., None] * jnp.stack(results, axis=0), axis=0)
    mixed = mixed.astype(jnp.bfloat16).reshape(length, HEADS * HEAD)
    return jnp.dot(mixed, output_weight, preferred_element_type=jnp.float32).astype(jnp.bfloat16)
```

```python
import functools

import jax
import jax.numpy as jnp
from jax import lax
from jax.experimental import pallas as pl
from jax.experimental.pallas import tpu as pltpu
from jax.sharding import PartitionSpec as P

HEAD = 128
REACH_STEPS = 128
MIDDLE_DILATION = 4
FAR_DILATION = 16
THETA_BASE = 500000.0
TILE = 16
MASKED = -1e30
SCALE = HEAD ** -0.5 * 1.4426950408889634
F32 = jnp.float32
BF16 = jnp.bfloat16


def proj_kernel(sc_ref, xo_ref, xp_ref, cos_ref, sin_ref, wq_ref, wk_ref, wv_ref,
                kq_ref, kkv_ref, sq_ref, skv_ref, buf_ref):
    g = pl.program_id(0)
    tp = sc_ref[0]
    half = xo_ref.shape[0]
    nq_half = half // FAR_DILATION
    nq = 2 * nq_half

    def place(out, lead, values, part):
        buf_ref[...] = values
        start = jnp.where(part == 0, tp, 1 - tp) * nq_half
        for r in range(FAR_DILATION):
            piece = buf_ref[pl.ds(r, nq_half, stride=FAR_DILATION), :]
            at = pl.multiple_of(r * nq + start, TILE)
            out[lead + (pl.ds(at, nq_half), slice(None))] = piece.astype(BF16)

    def work(q_out, kv_out):
        for part, x_ref in enumerate((xo_ref, xp_ref)):
            x = x_ref[...]
            cos = cos_ref[part * half:(part + 1) * half, :]
            sin = sin_ref[part * half:(part + 1) * half, :]
            for which, w_ref in enumerate((wk_ref, wv_ref, wq_ref)):
                acc = jnp.dot(x, w_ref[...], preferred_element_type=F32)
                for h in range(acc.shape[1] // HEAD):
                    val = acc[:, h * HEAD:(h + 1) * HEAD]
                    if which != 1:
                        val = val * cos + pltpu.roll(val, HEAD // 2, 1) * sin
                    if which == 2:
                        place(q_out, (h,), val, part)
                    else:
                        place(kv_out, (which, h), val, part)

    @pl.when(g == 0)
    def _():
        work(sq_ref, skv_ref)

    @pl.when(g == 1)
    def _():
        work(kq_ref, kkv_ref)


def project(scalars, x_own, x_partner, cos, sin, wq, wk, wv):
    half, depth = x_own.shape
    rows = 2 * half
    width = wq.shape[1] // 2
    heads = width // HEAD
    whole = lambda shape: pl.BlockSpec(shape, lambda g, sc: (0,) * len(shape))
    weight = pl.BlockSpec((depth, width), lambda g, sc: (0, jnp.where(g == 0, 1 - sc[1], sc[1])))
    q_shape = (heads, rows, HEAD)
    kv_shape = (2, heads, rows, HEAD)
    return pl.pallas_call(
        proj_kernel,
        grid_spec=pltpu.PrefetchScalarGridSpec(
            num_scalar_prefetch=1,
            grid=(2,),
            in_specs=[whole(x_own.shape), whole(x_partner.shape), whole(cos.shape), whole(sin.shape),
                      weight, weight, weight],
            out_specs=[whole(q_shape), whole(kv_shape), whole(q_shape), whole(kv_shape)],
            scratch_shapes=[pltpu.VMEM((half, HEAD), F32)],
        ),
        out_shape=[jax.ShapeDtypeStruct(s, BF16) for s in (q_shape, kv_shape, q_shape, kv_shape)],
        cost_estimate=pl.CostEstimate(flops=2 * rows * depth * width * 6, transcendentals=0,
                                      bytes_accessed=depth * width * 12 + rows * depth * 2),
        name="project",
    )(scalars, x_own, x_partner, cos, sin, wq, wk, wv)


def gather(dst_ref, own, other, par):
    nq = own.shape[0] // FAR_DILATION
    for r in range(FAR_DILATION):
        for part, block in ((par, own), (1 - par, other)):
            at = pl.multiple_of(r * 2 * nq + part * nq, TILE)
            dst_ref[pl.ds(at, nq), :] = block[r * nq:(r + 1) * nq, :]


def scores_of(q, k):
    return lax.dot_general(q, k, (((1,), (1,)), ((), ())), preferred_element_type=F32)


def partial(q, k, v, bias):
    s = scores_of(q, k)
    if bias is not None:
        s = s + bias
    top = jnp.max(s, axis=-1, keepdims=True)
    p = jnp.exp2((s - top) * SCALE).astype(BF16)
    vl = jnp.concatenate([v, jnp.ones_like(v)], axis=1)
    return top, jnp.dot(p, vl, preferred_element_type=F32)


def pieces(ref, rows, lead=()):
    parts = [ref[lead + (slice(a, a + n), slice(None))] for a, n in rows]
    return parts[0] if len(parts) == 1 else jnp.concatenate(parts, axis=0)


def merge(m_ref, l_ref, o_ref, rows, top, ol):
    at = 0
    for a, n in rows:
        here = slice(a, a + n)
        t = jnp.broadcast_to(top[at:at + n], (n, HEAD))
        old = m_ref[here, :]
        new = jnp.maximum(old, t)
        keep = jnp.exp2((old - new) * SCALE)
        add = jnp.exp2((t - new) * SCALE)
        m_ref[here, :] = new
        o_ref[here, :] = o_ref[here, :] * keep + ol[at:at + n, :HEAD] * add
        l_ref[here, :] = l_ref[here, :] * keep + ol[at:at + n, HEAD:] * add
        at += n


def far_rows(r, nq):
    return [(r * 2 * nq, 2 * nq)]


def middle_rows(r4, nq, block=None):
    step = MIDDLE_DILATION
    if block is None:
        return [((r4 + step * j) * 2 * nq, 2 * nq) for j in range(FAR_DILATION // step)]
    return [((r4 + step * j) * 2 * nq + block * nq, nq) for j in range(FAR_DILATION // step)]


def near_rows(c, nq):
    return [(r * 2 * nq + c * TILE, TILE) for r in range(FAR_DILATION)]


def bias_of(tq, tk, shift):
    d = tq[:, None] + shift - tk[None, :]
    return jnp.where((d >= 0) & (d <= REACH_STEPS), 0.0, MASKED).astype(F32)


def biases(nq):
    i = jnp.arange(2 * nq)
    far0 = bias_of(i, i, 0)
    far2 = bias_of(i, i, 4 * nq)
    step = FAR_DILATION // MIDDLE_DILATION
    j, i = jnp.arange(step)[:, None], jnp.arange(2 * nq)[None, :]
    t = (i * step + j).reshape(-1)
    mid0 = bias_of(t, t, 0)
    t = (jnp.arange(nq)[None, :] * step + j).reshape(-1)
    mid1 = bias_of(t, t, nq * step)
    r, u = jnp.arange(FAR_DILATION)[:, None], jnp.arange(TILE)[None, :]
    t = (u * FAR_DILATION + r).reshape(-1)
    near0 = bias_of(t, t, 0)
    near1 = bias_of(t, t, TILE * FAR_DILATION)
    return far0, far2, mid0, mid1, near0, near1


def local_kernel(sc_ref, qo_ref, qy_ref, kvo_ref, kvy_ref, far_ref, mid_ref, near0_ref, near1_ref,
                 q_ref, m_ref, l_ref, o_ref, k_s, v_s):
    par = sc_ref[1]
    nq = qo_ref.shape[1] // FAR_DILATION
    q_ref, m_ref, l_ref, o_ref = q_ref.at[0], m_ref.at[0], l_ref.at[0], o_ref.at[0]
    gather(q_ref, qo_ref.at[0], qy_ref.at[0], par)
    gather(k_s, kvo_ref.at[0, 0], kvy_ref.at[0, 0], par)
    gather(v_s, kvo_ref.at[1, 0], kvy_ref.at[1, 0], par)
    for r in range(FAR_DILATION):
        rows = far_rows(r, nq)
        top, ol = partial(pieces(q_ref, rows), pieces(k_s, rows), pieces(v_s, rows), far_ref[...])
        (a, n), = rows
        m_ref[a:a + n, :] = jnp.broadcast_to(top, (n, HEAD))
        o_ref[a:a + n, :] = ol[:, :HEAD]
        l_ref[a:a + n, :] = ol[:, HEAD:]
    for r4 in range(MIDDLE_DILATION):
        rows = middle_rows(r4, nq)
        top, ol = partial(pieces(q_ref, rows), pieces(k_s, rows), pieces(v_s, rows), mid_ref[...])
        merge(m_ref, l_ref, o_ref, rows, top, ol)
    for c in range(2 * nq // TILE):
        rows = near_rows(c, nq)
        keys, bias = rows, near0_ref[...]
        if c:
            keys = near_rows(c - 1, nq) + rows
            bias = jnp.concatenate([near1_ref[...], bias], axis=1)
        top, ol = partial(pieces(q_ref, rows), pieces(k_s, keys), pieces(v_s, keys), bias)
        merge(m_ref, l_ref, o_ref, rows, top, ol)


def one_kernel(sc_ref, q_ref, m_in, l_in, o_in, kvo_ref, kvy_ref, mid_ref, near_ref,
               m_ref, l_ref, o_ref, k_s, v_s):
    par = sc_ref[1]
    q_ref = q_ref.at[0]
    nq = q_ref.shape[0] // FAR_DILATION // 2
    m_ref, l_ref, o_ref = m_ref.at[0], l_ref.at[0], o_ref.at[0]
    m_ref[...] = m_in[0]
    l_ref[...] = l_in[0]
    o_ref[...] = o_in[0]

    @pl.when(sc_ref[2] >= 1)
    def _():
        gather(k_s, kvo_ref.at[0, 0], kvy_ref.at[0, 0], par)
        gather(v_s, kvo_ref.at[1, 0], kvy_ref.at[1, 0], par)
        for r in range(FAR_DILATION):
            rows = far_rows(r, nq)
            top, ol = partial(pieces(q_ref, rows), pieces(k_s, rows), pieces(v_s, rows), None)
            merge(m_ref, l_ref, o_ref, rows, top, ol)
        for r4 in range(MIDDLE_DILATION):
            rows, keys = middle_rows(r4, nq, 0), middle_rows(r4, nq, 1)
            top, ol = partial(pieces(q_ref, rows), pieces(k_s, keys), pieces(v_s, keys), mid_ref[...])
            merge(m_ref, l_ref, o_ref, rows, top, ol)
        rows, keys = near_rows(0, nq), near_rows(2 * nq // TILE - 1, nq)
        top, ol = partial(pieces(q_ref, rows), pieces(k_s, keys), pieces(v_s, keys), near_ref[...])
        merge(m_ref, l_ref, o_ref, rows, top, ol)


def two_kernel(sc_ref, q_ref, m_ref, l_ref, o_ref, kvo_ref, kvy_ref, far_ref,
               keep_ref, send_ref, k_s, v_s, mix_s):
    par = sc_ref[1]
    q_ref, m_ref, l_ref, o_ref = q_ref.at[0], m_ref.at[0], l_ref.at[0], o_ref.at[0]
    nq = q_ref.shape[0] // FAR_DILATION // 2

    def settle(r, o, l):
        val = o / l
        mix_s[0, pl.ds(r, nq, stride=FAR_DILATION), :] = val[:nq]
        mix_s[1, pl.ds(r, nq, stride=FAR_DILATION), :] = val[nq:]

    @pl.when(sc_ref[2] >= 2)
    def _():
        gather(k_s, kvo_ref.at[0, 0], kvy_ref.at[0, 0], par)
        gather(v_s, kvo_ref.at[1, 0], kvy_ref.at[1, 0], par)
        for r in range(FAR_DILATION):
            rows = far_rows(r, nq)
            top, ol = partial(pieces(q_ref, rows), pieces(k_s, rows), pieces(v_s, rows), far_ref[...])
            (a, n), = rows
            old = m_ref[a:a + n, :]
            t = jnp.broadcast_to(top, old.shape)
            new = jnp.maximum(old, t)
            keep = jnp.exp2((old - new) * SCALE)
            add = jnp.exp2((t - new) * SCALE)
            settle(r, o_ref[a:a + n, :] * keep + ol[:, :HEAD] * add,
                   l_ref[a:a + n, :] * keep + ol[:, HEAD:] * add)

    @pl.when(sc_ref[2] < 2)
    def _():
        for r in range(FAR_DILATION):
            (a, n), = far_rows(r, nq)
            settle(r, o_ref[a:a + n, :], l_ref[a:a + n, :])

    keep_ref[...] = mix_s[pl.ds(par, 1)][0].astype(BF16)
    send_ref[...] = mix_s[pl.ds(1 - par, 1)][0].astype(BF16)


def attention_call(kernel, scalars, inputs, outputs, scratch, flops, name):
    def spec(shape, dim):
        if dim is None:
            return pl.BlockSpec(shape, lambda h, sc: (0,) * len(shape))
        block = tuple(shape[i] if i != dim else (1 if dim < len(shape) - 1 else HEAD) for i in range(len(shape)))
        return pl.BlockSpec(block, lambda h, sc: tuple(h if i == dim else 0 for i in range(len(shape))))

    heads = inputs[0][0].shape[0]
    return pl.pallas_call(
        kernel,
        grid_spec=pltpu.PrefetchScalarGridSpec(
            num_scalar_prefetch=1,
            grid=(heads,),
            in_specs=[spec(a.shape, d) for a, d in inputs],
            out_specs=[spec(s.shape, d) for s, d in outputs],
            scratch_shapes=scratch,
        ),
        out_shape=[s for s, _ in outputs],
        cost_estimate=pl.CostEstimate(flops=flops, transcendentals=0, bytes_accessed=0),
        name=name,
    )(scalars, *[a for a, _ in inputs])


def out_kernel(sc_ref, a_ref, b_ref, c_ref, d_ref, w_ref, o_ref):
    tp, par = sc_ref[0], sc_ref[1]
    width = a_ref.shape[1]

    def term(x_ref, index):
        at = pl.multiple_of(index * width, width)
        return jnp.dot(x_ref[...], w_ref[pl.ds(at, width), :], preferred_element_type=F32)

    total = term(a_ref, 2 * tp + par) + term(b_ref, 2 * tp + 1 - par)
    total += term(c_ref, 2 * (1 - tp) + par) + term(d_ref, 2 * (1 - tp) + 1 - par)
    o_ref[...] = total.astype(BF16)


def out_project(scalars, parts, weight):
    rows, width = parts[0].shape
    depth, columns = weight.shape
    block = columns // 4
    part = pl.BlockSpec((rows, width), lambda j, sc: (0, 0))
    return pl.pallas_call(
        out_kernel,
        grid_spec=pltpu.PrefetchScalarGridSpec(
            num_scalar_prefetch=1,
            grid=(4,),
            in_specs=[part] * 4 + [pl.BlockSpec((depth, block), lambda j, sc: (0, j))],
            out_specs=pl.BlockSpec((rows, block), lambda j, sc: (0, j)),
        ),
        out_shape=jax.ShapeDtypeStruct((rows, columns), BF16),
        cost_estimate=pl.CostEstimate(flops=2 * rows * depth * columns, transcendentals=0,
                                      bytes_accessed=depth * columns * 2),
        name="out_project",
    )(scalars, *parts, weight)


def swap(x, axis):
    return lax.ppermute(x, axis, [(i, i ^ 1) for i in range(lax.axis_size(axis))])


def onward(x):
    n = lax.axis_size("sp")
    return lax.ppermute(x, "sp", [(i, i + 2) for i in range(n - 2)])


def body(tokens, query_weight, key_weight, value_weight, output_weight):
    half = tokens.shape[0]
    rows = 2 * half
    nq = rows // FAR_DILATION
    assert 4 * rows == FAR_DILATION * REACH_STEPS
    sp, tp = lax.axis_index("sp"), lax.axis_index("tp")
    scalars = jnp.stack([tp, sp % 2, sp // 2]).astype(jnp.int32)
    partner = swap(tokens, "tp")
    i = jnp.arange(rows, dtype=jnp.int32)
    positions = sp * rows + jnp.where(i < half, i + tp * half, i - half + (1 - tp) * half)
    inverse = THETA_BASE ** (-jnp.arange(HEAD // 2, dtype=F32) / (HEAD // 2))
    angles = positions.astype(F32)[:, None] * inverse
    cosine, sine = jnp.cos(angles), jnp.sin(angles)
    cosine = jnp.concatenate([cosine, cosine], axis=1)
    sine = jnp.concatenate([-sine, sine], axis=1)
    far0, far2, mid0, mid1, near0, near1 = biases(nq)
    q_own, kv_own, q_send, kv_send = project(
        scalars, tokens, partner, cosine, sine, query_weight, key_weight, value_weight)
    heads = q_own.shape[0]
    kv1_own = onward(kv_own)
    kv_y = swap(kv_send, "sp")
    q_y = swap(q_send, "sp")
    kv1_y = onward(kv_y)
    kv2_own = onward(kv1_own)
    kv2_y = onward(kv1_y)
    group = 2 * rows
    state = jax.ShapeDtypeStruct((heads, group, HEAD), F32)
    kv_scratch = [pltpu.VMEM((group, HEAD), BF16)] * 2
    q, m, l, o = attention_call(
        local_kernel, scalars,
        [(q_own, 0), (q_y, 0), (kv_own, 1), (kv_y, 1), (far0, None), (mid0, None), (near0, None), (near1, None)],
        [(jax.ShapeDtypeStruct((heads, group, HEAD), BF16), 0), (state, 0), (state, 0), (state, 0)],
        kv_scratch, 3 * 10 ** 9, "attend_local")
    m, l, o = attention_call(
        one_kernel, scalars,
        [(q, 0), (m, 0), (l, 0), (o, 0), (kv1_own, 1), (kv1_y, 1), (mid1, None), (near1, None)],
        [(state, 0), (state, 0), (state, 0)],
        kv_scratch, 10 ** 9, "attend_one")
    mixed = jax.ShapeDtypeStruct((rows, heads * HEAD), BF16)
    keep, send = attention_call(
        two_kernel, scalars,
        [(q, 0), (m, 0), (l, 0), (o, 0), (kv2_own, 1), (kv2_y, 1), (far2, None)],
        [(mixed, 1), (mixed, 1)],
        kv_scratch + [pltpu.VMEM((2, rows, HEAD), F32)], 10 ** 9, "attend_two")
    keep_tp = swap(keep, "tp")
    from_y = swap(send, "sp")
    from_y_tp = swap(from_y, "tp")
    return out_project(scalars, [keep, from_y, keep_tp, from_y_tp], output_weight)


def solution(mesh):
    in_specs = (
        P(("grp", "sp", "tp"), None),
        P(None, "tp"),
        P(None, "tp"),
        P(None, "tp"),
        P(None, "tp"),
    )
    out_specs = P(("grp", "sp"), "tp")
    return jax.shard_map(body, mesh=mesh, in_specs=in_specs, out_specs=out_specs, check_vma=False)
```

```python
import functools

import jax
import jax.numpy as jnp
import numpy as np
from jax import lax
from jax.experimental import pallas as pl
from jax.experimental.pallas import tpu as pltpu
from jax.sharding import PartitionSpec as P

HEAD = 128
REACH_STEPS = 128
MIDDLE_DILATION = 4
FAR_DILATION = 16
THETA_BASE = 500000.0
TILE = 16
MASKED = -1e30
SCALE = HEAD ** -0.5 * 1.4426950408889634
F32 = jnp.float32
BF16 = jnp.bfloat16


def proj_kernel(sc_ref, xo_ref, xp_ref, cos_ref, sin_ref, *refs, rotated):
    count = len(rotated)
    w_refs, (keep_ref, send_ref, buf_ref) = refs[:count], refs[count:]
    tp, par = sc_ref[0], sc_ref[1]
    half = xo_ref.shape[0]
    nq_half = half // FAR_DILATION
    nq = 2 * nq_half
    heads = keep_ref.shape[1]
    width = heads * HEAD
    slot = 0
    for out_ref, side in ((keep_ref, par), (send_ref, 1 - par)):
        for which in range(count):
            w = w_refs[which][:, pl.ds(pl.multiple_of(side * width, width), width)]
            for part, x_ref in enumerate((xo_ref, xp_ref)):
                acc = jnp.dot(x_ref[...], w, preferred_element_type=F32)
                start = (tp if part == 0 else 1 - tp) * nq_half
                for h in range(heads):
                    val = acc[:, h * HEAD:(h + 1) * HEAD]
                    if rotated[which]:
                        cos = cos_ref[part * half:(part + 1) * half, :]
                        sin = sin_ref[part * half:(part + 1) * half, :]
                        val = val * cos + pltpu.roll(val, HEAD // 2, 1) * sin
                    buf_ref[slot] = val
                    for r in range(FAR_DILATION):
                        piece = buf_ref[slot, pl.ds(r, nq_half, stride=FAR_DILATION), :]
                        at = pl.multiple_of(r * nq + start, TILE)
                        out_ref[which, h, pl.ds(at, nq_half), :] = piece.astype(BF16)
                    slot += 1


def in_vmem(count):
    return [pl.BlockSpec(memory_space=pltpu.VMEM)] * count


def project(scalars, x_own, x_partner, cos, sin, weights, rotated, name):
    half, depth = x_own.shape
    rows = 2 * half
    count = len(weights)
    heads = weights[0].shape[1] // 2 // HEAD
    shape = jax.ShapeDtypeStruct((count, heads, rows, HEAD), BF16)
    return pl.pallas_call(
        functools.partial(proj_kernel, rotated=rotated),
        in_specs=[pl.BlockSpec(memory_space=pltpu.SMEM)] + in_vmem(4 + count),
        out_specs=in_vmem(2),
        out_shape=[shape, shape],
        scratch_shapes=[pltpu.VMEM((4 * count * heads, half, HEAD), F32)],
        compiler_params=pltpu.CompilerParams(vmem_limit_bytes=24 * 2 ** 20),
        cost_estimate=pl.CostEstimate(flops=2 * rows * depth * 2 * heads * HEAD * count, transcendentals=0,
                                      bytes_accessed=0),
        name=name,
    )(scalars, x_own, x_partner, cos, sin, *weights)


def gather(dst_ref, own, other, par):
    nq = own.shape[0] // FAR_DILATION
    for r in range(FAR_DILATION):
        for part, block in ((par, own), (1 - par, other)):
            at = pl.multiple_of(r * 2 * nq + part * nq, TILE)
            dst_ref[pl.ds(at, nq), :] = block[r * nq:(r + 1) * nq, :]


def scores_of(q, k):
    return lax.dot_general(q, k, (((1,), (1,)), ((), ())), preferred_element_type=F32)


def take(ref, rows):
    parts = [ref[a:a + n, :] for a, n in rows]
    return parts[0] if len(parts) == 1 else jnp.concatenate(parts, axis=0)


def put(ref, rows, value):
    at = 0
    for a, n in rows:
        ref[a:a + n, :] = value[at:at + n]
        at += n


def widened(stat, columns):
    return jnp.concatenate([stat] * (columns // HEAD), axis=1) if columns > HEAD else stat


def scored(item, q_ref, k_ref, s_ref, m_ref, fresh):
    rows, keys, bias, at = item
    s = scores_of(take(q_ref, rows), take(k_ref, keys))
    if bias is not None:
        s = s + bias
    n, columns = s.shape
    s_ref[at:at + n, :columns] = s
    top = jnp.broadcast_to(jnp.max(s, axis=-1, keepdims=True), (n, HEAD))
    put(m_ref, rows, top if fresh else jnp.maximum(take(m_ref, rows), top))


def weighed(item, v_ref, s_ref, m_ref, columns):
    rows, keys, _, at = item
    n = sum(c for _, c in rows)
    p = jnp.exp2((s_ref[at:at + n, :columns] - widened(take(m_ref, rows), columns)) * SCALE).astype(BF16)
    v = take(v_ref, keys)
    return jnp.dot(p, jnp.concatenate([v, jnp.ones_like(v)], axis=1), preferred_element_type=F32)


def length(rows):
    return sum(n for _, n in rows)


def group_rows(r4, nq):
    return [((r4 + MIDDLE_DILATION * j) * 2 * nq, 2 * nq) for j in range(FAR_DILATION // MIDDLE_DILATION)]


def near_rows(c, nq):
    return [(r * 2 * nq + c * TILE, TILE) for r in range(FAR_DILATION)]


def pair_rows(i, nq):
    return [(i * 4 * nq, 4 * nq)]


def near_of(tq, tk):
    return (tq - tk >= 0) & (tq - tk <= REACH_STEPS)


def every(tq, tk, step):
    return (tq % step == tk % step) & (tq - tk >= 0) & (tq - tk <= REACH_STEPS * step)


def bias_of(count):
    return np.where(count > 0, np.log2(np.maximum(count, 1)) / SCALE, MASKED).astype(np.float32)


def biases(nq):
    group = 2 * nq * FAR_DILATION
    j = np.arange(FAR_DILATION // MIDDLE_DILATION)[:, None]
    t = (np.arange(2 * nq)[None, :] * FAR_DILATION + j * MIDDLE_DILATION).reshape(-1)
    tq, tk = t[:, None], t[None, :]
    both = lambda tq, tk: every(tq, tk, MIDDLE_DILATION).astype(int) + every(tq, tk, FAR_DILATION)
    group0, group1 = both(tq, tk), both(tq + group, tk)
    r = np.arange(FAR_DILATION)[:, None]
    t = (np.arange(TILE)[None, :] * FAR_DILATION + r).reshape(-1)
    tq, tk = t[:, None], t[None, :]
    near0, near1 = near_of(tq, tk), near_of(tq + TILE * FAR_DILATION, tk)
    r = np.arange(2)[:, None]
    t = (np.arange(2 * nq)[None, :] * FAR_DILATION + r).reshape(-1)
    pair2 = every(t[:, None] + 2 * group, t[None, :], FAR_DILATION)
    return [bias_of(np.asarray(x, int)) for x in (group0, group1, near0, near1, pair2)]


def local_kernel(sc_ref, qo_ref, qy_ref, kvo_ref, kvy_ref, group_ref, near0_ref, near1_ref,
                 q_ref, m_ref, l_ref, o_ref, k_s, v_s, s_s):
    par = sc_ref[1]
    nq = qo_ref.shape[2] // FAR_DILATION
    for h in range(q_ref.shape[0]):
        q, m, l, o, k, v, sh = (x.at[h] for x in (q_ref, m_ref, l_ref, o_ref, k_s, v_s, s_s))
        gather(q, qo_ref.at[0, h], qy_ref.at[0, h], par)
        gather(k, kvo_ref.at[0, h], kvy_ref.at[0, h], par)
        gather(v, kvo_ref.at[1, h], kvy_ref.at[1, h], par)
        at = 0
        items = []
        for r4 in range(MIDDLE_DILATION):
            rows = group_rows(r4, nq)
            items.append((rows, rows, group_ref[...], at))
            scored(items[-1], q, k, sh, m, True)
            at += length(rows)
        for c in range(2 * nq // TILE):
            rows = near_rows(c, nq)
            keys, bias = rows, near0_ref[...]
            if c:
                keys = near_rows(c - 1, nq) + rows
                bias = jnp.concatenate([near1_ref[...], bias], axis=1)
            items.append((rows, keys, bias, at))
            scored(items[-1], q, k, sh, m, False)
            at += length(rows)
        for i, item in enumerate(items):
            ol = weighed(item, v, sh, m, length(item[1]))
            if i < MIDDLE_DILATION:
                put(o, item[0], ol[:, :HEAD])
                put(l, item[0], ol[:, HEAD:])
            else:
                put(o, item[0], take(o, item[0]) + ol[:, :HEAD])
                put(l, item[0], take(l, item[0]) + ol[:, HEAD:])


def one_kernel(sc_ref, q_ref, m_in, l_in, o_in, kvo_ref, kvy_ref, group_ref, near_ref,
               m_ref, l_ref, o_ref, k_s, v_s, s_s, n_s):
    par = sc_ref[1]
    nq = kvo_ref.shape[2] // FAR_DILATION

    @pl.when(sc_ref[2] >= 1)
    def _():
        for h in range(q_ref.shape[0]):
            q, mi, li, oi, m, l, o, k, v, sh, n = (x.at[h] for x in (
                q_ref, m_in, l_in, o_in, m_ref, l_ref, o_ref, k_s, v_s, s_s, n_s))
            gather(k, kvo_ref.at[0, h], kvy_ref.at[0, h], par)
            gather(v, kvo_ref.at[1, h], kvy_ref.at[1, h], par)
            near = (near_rows(0, nq), near_rows(2 * nq // TILE - 1, nq), near_ref[...], 0)
            at = length(near[0])
            items = []
            for r4 in range(MIDDLE_DILATION):
                rows = group_rows(r4, nq)
                items.append((rows, rows, group_ref[...], at))
                scored(items[-1], q, k, sh, n, True)
                at += length(rows)
            scored(near, q, k, sh, n, False)
            for item in items:
                rows = item[0]
                old = take(mi, rows)
                new = jnp.maximum(old, take(n, rows))
                keep = jnp.exp2((old - new) * SCALE)
                put(m, rows, new)
                ol = weighed(item, v, sh, m, length(item[1]))
                put(o, rows, take(oi, rows) * keep + ol[:, :HEAD])
                put(l, rows, take(li, rows) * keep + ol[:, HEAD:])
            ol = weighed(near, v, sh, m, length(near[1]))
            put(o, near[0], take(o, near[0]) + ol[:, :HEAD])
            put(l, near[0], take(l, near[0]) + ol[:, HEAD:])


def two_kernel(sc_ref, q_ref, m_ref, l_ref, o_ref, kvo_ref, kvy_ref, pair_ref,
               keep_ref, send_ref, k_s, v_s, mix_s):
    par = sc_ref[1]
    nq = kvo_ref.shape[2] // FAR_DILATION
    heads = q_ref.shape[0]

    def settle(h, i, val):
        for part in range(4):
            r, block = 2 * i + part // 2, part % 2
            mix_s[h, block, pl.ds(r, nq, stride=FAR_DILATION), :] = val[part * nq:(part + 1) * nq]

    @pl.when(sc_ref[2] >= 2)
    def _():
        for h in range(heads):
            q, m, l, o, k, v = (x.at[h] for x in (q_ref, m_ref, l_ref, o_ref, k_s, v_s))
            gather(k, kvo_ref.at[0, h], kvy_ref.at[0, h], par)
            gather(v, kvo_ref.at[1, h], kvy_ref.at[1, h], par)
            for i in range(FAR_DILATION // 2):
                rows = pair_rows(i, nq)
                s = scores_of(take(q, rows), take(k, rows)) + pair_ref[...]
                old = take(m, rows)
                new = jnp.maximum(old, jnp.max(s, axis=-1, keepdims=True))
                keep = jnp.exp2((old - new) * SCALE)
                p = jnp.exp2((s - new) * SCALE).astype(BF16)
                vs = take(v, rows)
                ol = jnp.dot(p, jnp.concatenate([vs, jnp.ones_like(vs)], axis=1), preferred_element_type=F32)
                settle(h, i, (take(o, rows) * keep + ol[:, :HEAD]) / (take(l, rows) * keep + ol[:, HEAD:]))

    @pl.when(sc_ref[2] < 2)
    def _():
        for h in range(heads):
            for i in range(FAR_DILATION // 2):
                rows = pair_rows(i, nq)
                settle(h, i, take(o_ref.at[h], rows) / take(l_ref.at[h], rows))

    for h in range(heads):
        keep_ref[:, h * HEAD:(h + 1) * HEAD] = mix_s[h, pl.ds(par, 1)][0].astype(BF16)
        send_ref[:, h * HEAD:(h + 1) * HEAD] = mix_s[h, pl.ds(1 - par, 1)][0].astype(BF16)


def attention_call(kernel, scalars, inputs, outputs, scratch, flops, name, aliases={}):
    return pl.pallas_call(
        kernel,
        in_specs=[pl.BlockSpec(memory_space=pltpu.SMEM)] + in_vmem(len(inputs)),
        out_specs=in_vmem(len(outputs)),
        out_shape=outputs,
        scratch_shapes=scratch,
        input_output_aliases=aliases,
        compiler_params=pltpu.CompilerParams(vmem_limit_bytes=28 * 2 ** 20),
        cost_estimate=pl.CostEstimate(flops=flops, transcendentals=0, bytes_accessed=0),
        name=name,
    )(scalars, *inputs)


def out_kernel(sc_ref, a_ref, b_ref, c_ref, d_ref, w_ref, o_ref):
    tp, par = sc_ref[0], sc_ref[1]
    width = a_ref.shape[1]
    block = o_ref.shape[1]
    column = pl.multiple_of(pl.program_id(0) * block, block)
    order = (2 * tp + par, 2 * tp + 1 - par, 2 * (1 - tp) + par, 2 * (1 - tp) + 1 - par)
    x = jnp.concatenate([a_ref[...], b_ref[...], c_ref[...], d_ref[...]], axis=1)
    w = jnp.concatenate(
        [w_ref[pl.ds(pl.multiple_of(i * width, width), width), pl.ds(column, block)] for i in order], axis=0)
    o_ref[...] = jnp.dot(x, w, preferred_element_type=F32).astype(BF16)


def out_project(scalars, parts, weight):
    rows = parts[0].shape[0]
    depth, columns = weight.shape
    steps = columns // 256
    return pl.pallas_call(
        out_kernel,
        grid=(steps,),
        in_specs=[pl.BlockSpec(memory_space=pltpu.SMEM)] + in_vmem(5),
        out_specs=pl.BlockSpec((rows, columns // steps), lambda j: (0, j)),
        out_shape=jax.ShapeDtypeStruct((rows, columns), BF16),
        compiler_params=pltpu.CompilerParams(vmem_limit_bytes=16 * 2 ** 20),
        cost_estimate=pl.CostEstimate(flops=2 * rows * depth * columns, transcendentals=0,
                                      bytes_accessed=depth * columns * 2),
        name="out_project",
    )(scalars, *parts, weight)


def swap(x, axis):
    return lax.ppermute(x, axis, [(i, i ^ 1) for i in range(lax.axis_size(axis))])


def onward(x):
    n = lax.axis_size("sp")
    return lax.ppermute(x, "sp", [(i, i + 2) for i in range(n - 2)])


def body(tokens, query_weight, key_weight, value_weight, output_weight):
    half = tokens.shape[0]
    rows = 2 * half
    nq = rows // FAR_DILATION
    assert 4 * rows == FAR_DILATION * REACH_STEPS
    sp, tp = lax.axis_index("sp"), lax.axis_index("tp")
    scalars = jnp.stack([tp, sp % 2, sp // 2]).astype(jnp.int32)
    partner = swap(tokens, "tp")
    i = jnp.arange(rows, dtype=jnp.int32)
    positions = sp * rows + jnp.where(i < half, i + tp * half, i - half + (1 - tp) * half)
    inverse = THETA_BASE ** (-jnp.arange(HEAD // 2, dtype=F32) / (HEAD // 2))
    angles = positions.astype(F32)[:, None] * inverse
    cosine, sine = jnp.cos(angles), jnp.sin(angles)
    cosine = jnp.concatenate([cosine, cosine], axis=1)
    sine = jnp.concatenate([-sine, sine], axis=1)
    group0, group1, near0, near1, pair2 = biases(nq)
    kv_own, kv_send = project(scalars, tokens, partner, cosine, sine, (key_weight, value_weight),
                              (True, False), "project_kv")
    kv1_own = onward(kv_own)
    kv_y = swap(kv_send, "sp")
    q_own, q_send = project(scalars, tokens, partner, cosine, sine, (query_weight,), (True,), "project_q")
    q_y = swap(q_send, "sp")
    kv1_y = onward(kv_y)
    kv2_own = onward(kv1_own)
    kv2_y = onward(kv1_y)
    heads = q_own.shape[1]
    group = 2 * rows
    state = jax.ShapeDtypeStruct((heads, group, HEAD), F32)
    kv_scratch = [pltpu.VMEM((heads, group, HEAD), BF16)] * 2
    q, m, l, o = attention_call(
        local_kernel, scalars, [q_own, q_y, kv_own, kv_y, group0, near0, near1],
        [jax.ShapeDtypeStruct((heads, group, HEAD), BF16), state, state, state],
        kv_scratch + [pltpu.VMEM((heads, 2 * group, 4 * HEAD), F32)], 3 * 10 ** 9, "attend_local")
    m, l, o = attention_call(
        one_kernel, scalars, [q, m, l, o, kv1_own, kv1_y, group1, near1], [state, state, state],
        kv_scratch + [pltpu.VMEM((heads, 2 * group, 2 * HEAD), F32), pltpu.VMEM((heads, group, HEAD), F32)],
        10 ** 9, "attend_one", {2: 0, 3: 1, 4: 2})
    mixed = jax.ShapeDtypeStruct((rows, heads * HEAD), BF16)
    keep, send = attention_call(
        two_kernel, scalars, [q, m, l, o, kv2_own, kv2_y, pair2], [mixed, mixed],
        kv_scratch + [pltpu.VMEM((heads, 2, rows, HEAD), F32)], 10 ** 9, "attend_two")
    keep_tp = swap(keep, "tp")
    from_y = swap(send, "sp")
    from_y_tp = swap(from_y, "tp")
    return out_project(scalars, [keep, from_y, keep_tp, from_y_tp], output_weight)


def solution(mesh):
    in_specs = (
        P(("grp", "sp", "tp"), None),
        P(None, "tp"),
        P(None, "tp"),
        P(None, "tp"),
        P(None, "tp"),
    )
    out_specs = P(("grp", "sp"), "tp")
    return jax.shard_map(body, mesh=mesh, in_specs=in_specs, out_specs=out_specs, check_vma=False)
```

```python
import functools

import jax
import jax.numpy as jnp
import numpy as np
from jax import lax
from jax.experimental import pallas as pl
from jax.experimental.pallas import tpu as pltpu
from jax.sharding import PartitionSpec as P

HEAD = 128
REACH_STEPS = 128
MIDDLE_DILATION = 4
FAR_DILATION = 16
THETA_BASE = 500000.0
TILE = 16
MASKED = -1e30
SCALE = HEAD ** -0.5 * 1.4426950408889634
F32 = jnp.float32
BF16 = jnp.bfloat16


def in_vmem(count):
    return [pl.BlockSpec(memory_space=pltpu.VMEM)] * count


def rotated(val, cos, sin):
    return val * cos + pltpu.roll(val, HEAD // 2, 1) * sin


def place(out_ref, lead, val, buf_ref, slot, first):
    nq_half = val.shape[0] // FAR_DILATION
    buf_ref[slot] = val
    for r in range(FAR_DILATION):
        piece = buf_ref[slot, pl.ds(r, nq_half, stride=FAR_DILATION), :]
        at = r * nq_half if first is None else pl.multiple_of((2 * r + first) * nq_half, TILE)
        out_ref[lead + (pl.ds(at, nq_half), slice(None))] = piece.astype(BF16)


def kv_half(x_ref, w_ref, keep_ref, send_ref, cos_ref, sin_ref, buf_ref, part, ready=None):
    cos, sin = cos_ref.at[part], sin_ref.at[part]
    slot = 0
    for side, out_ref in enumerate((keep_ref, send_ref)):
        for which in (1, 0):
            if ready is not None:
                ready(side, which)
            acc = jnp.dot(x_ref[...], w_ref[side, which], preferred_element_type=F32)
            for h in range(acc.shape[1] // HEAD):
                val = acc[:, h * HEAD:(h + 1) * HEAD]
                if which == 0:
                    val = rotated(val, cos[...], sin[...])
                place(out_ref, (h, which), val, buf_ref, slot, None)
                slot += 1


def own_kernel(sc_ref, x_hbm, wk_hbm, wv_hbm, inv_ref,
               keep_ref, send_ref, w_ref, cos_ref, sin_ref, x_ref, buf_ref, sems):
    tp, par, sp = sc_ref[0], sc_ref[1], sc_ref[3]
    half = x_ref.shape[0]
    width = w_ref.shape[3]
    copies = {}
    copies["x"] = pltpu.make_async_copy(x_hbm, x_ref, sems.at[0])
    copies["x"].start()
    for side in range(2):
        column = pl.multiple_of((par if side == 0 else 1 - par) * width, width)
        for which, hbm in ((1, wv_hbm), (0, wk_hbm)):
            copy = pltpu.make_async_copy(hbm.at[:, pl.ds(column, width)], w_ref.at[side, which],
                                         sems.at[1 + 2 * side + which])
            copy.start()
            copies[side, which] = copy
    steps = half // FAR_DILATION
    lane = lax.broadcasted_iota(jnp.int32, (2 * steps, HEAD), 1)
    row = lax.broadcasted_iota(jnp.int32, (2 * steps, HEAD), 0)
    part = jnp.where(row < steps, tp, 1 - tp)
    position = sp * (2 * half) + part * half + (row % steps) * FAR_DILATION
    coarse = position.astype(F32) * inv_ref[...]
    fine = lax.broadcasted_iota(jnp.int32, (FAR_DILATION, HEAD), 0).astype(F32) * inv_ref[...]
    cos_c, sin_c = jnp.cos(coarse)[:, None, :], jnp.sin(coarse)[:, None, :]
    cos_f, sin_f = jnp.cos(fine)[None], jnp.sin(fine)[None]
    sign = jnp.where(lane[:1] < HEAD // 2, -1.0, 1.0)[None]
    cos_ref[...] = (cos_c * cos_f - sin_c * sin_f).reshape(2, half, HEAD)
    sin_ref[...] = ((sin_c * cos_f + cos_c * sin_f) * sign).reshape(2, half, HEAD)
    copies["x"].wait()
    kv_half(x_ref, w_ref, keep_ref, send_ref, cos_ref, sin_ref, buf_ref, 0,
            lambda side, which: copies[side, which].wait())


def rest_kernel(sc_ref, x_ref, w_ref, cos_ref, sin_ref, keep_ref, send_ref, buf_ref):
    kv_half(x_ref, w_ref, keep_ref, send_ref, cos_ref, sin_ref, buf_ref, 1)


def q_kernel(sc_ref, xo_ref, xp_ref, cos_ref, sin_ref, w_ref, keepa_ref, keepb_ref, send_ref, buf_ref):
    tp, par = sc_ref[0], sc_ref[1]
    heads = send_ref.shape[0]
    width = heads * HEAD
    slot = 0
    for side in (1, 0):
        w = w_ref[:, pl.ds(pl.multiple_of((1 - par if side else par) * width, width), width)]
        for part, x_ref in enumerate((xo_ref, xp_ref)):
            acc = jnp.dot(x_ref[...], w, preferred_element_type=F32)
            for h in range(heads):
                val = rotated(acc[:, h * HEAD:(h + 1) * HEAD], cos_ref[part], sin_ref[part])
                if side:
                    place(send_ref, (h,), val, buf_ref, slot, tp if part == 0 else 1 - tp)
                else:
                    place((keepa_ref, keepb_ref)[part], (h,), val, buf_ref, slot, None)
                slot += 1


def call(kernel, scalars, inputs, outputs, scratch, flops, aliases={}, limit=28, hbm=()):
    spaces = [pltpu.HBM if i in hbm else pltpu.VMEM for i in range(len(inputs))]
    return pl.pallas_call(
        kernel,
        in_specs=[pl.BlockSpec(memory_space=pltpu.SMEM)] + [pl.BlockSpec(memory_space=m) for m in spaces],
        out_specs=in_vmem(len(outputs)),
        out_shape=outputs,
        scratch_shapes=scratch,
        input_output_aliases=aliases,
        compiler_params=pltpu.CompilerParams(vmem_limit_bytes=limit * 2 ** 20),
        cost_estimate=pl.CostEstimate(flops=flops, transcendentals=0, bytes_accessed=0),
    )(scalars, *[pltpu.with_memory_space_constraint(x, pltpu.HBM) if i in hbm else x for i, x in enumerate(inputs)])


def gather(dst_ref, nq, sources):
    for r in range(FAR_DILATION):
        for source, block, half in sources:
            rows = nq if half is None else nq // 2
            start = 0 if half is None else half * (nq // 2)
            at = pl.multiple_of(r * 2 * nq + block * nq + start, TILE)
            dst_ref[pl.ds(at, rows), :] = source[r * rows:(r + 1) * rows, :]


def gather_kv(k_ref, v_ref, refs, nq, tp, par):
    places = ((par, tp), (par, 1 - tp), (1 - par, tp), (1 - par, 1 - tp))
    for which, dst_ref in enumerate((k_ref, v_ref)):
        gather(dst_ref, nq, [(ref.at[which], block, half) for ref, (block, half) in zip(refs, places)])


def scores_of(q, k):
    return lax.dot_general(q, k, (((1,), (1,)), ((), ())), preferred_element_type=F32)


def take(ref, rows):
    parts = [ref[a:a + n, :] for a, n in rows]
    return parts[0] if len(parts) == 1 else jnp.concatenate(parts, axis=0)


def put(ref, rows, value):
    at = 0
    for a, n in rows:
        ref[a:a + n, :] = value[at:at + n]
        at += n


def widened(stat, columns):
    return jnp.concatenate([stat] * (columns // HEAD), axis=1) if columns > HEAD else stat


def scored(item, q_ref, k_ref, s_ref, m_ref, fresh):
    rows, keys, bias, at = item
    s = scores_of(take(q_ref, rows), take(k_ref, keys))
    if bias is not None:
        s = s + bias
    n, columns = s.shape
    s_ref[at:at + n, :columns] = s
    top = jnp.broadcast_to(jnp.max(s, axis=-1, keepdims=True), (n, HEAD))
    put(m_ref, rows, top if fresh else jnp.maximum(take(m_ref, rows), top))


def weighed(item, v_ref, s_ref, m_ref, columns):
    rows, keys, _, at = item
    n = sum(c for _, c in rows)
    p = jnp.exp2((s_ref[at:at + n, :columns] - widened(take(m_ref, rows), columns)) * SCALE).astype(BF16)
    v = take(v_ref, keys)
    return jnp.dot(p, jnp.concatenate([v, jnp.ones_like(v)], axis=1), preferred_element_type=F32)


def length(rows):
    return sum(n for _, n in rows)


def group_rows(r4, nq):
    return [((r4 + MIDDLE_DILATION * j) * 2 * nq, 2 * nq) for j in range(FAR_DILATION // MIDDLE_DILATION)]


def near_rows(c, nq):
    return [(r * 2 * nq + c * TILE, TILE) for r in range(FAR_DILATION)]


def pair_rows(i, nq):
    return [(i * 4 * nq, 4 * nq)]


def near_of(tq, tk):
    return (tq - tk >= 0) & (tq - tk <= REACH_STEPS)


def every(tq, tk, step):
    return (tq % step == tk % step) & (tq - tk >= 0) & (tq - tk <= REACH_STEPS * step)


def bias_of(count):
    return np.where(count > 0, np.log2(np.maximum(count, 1)) / SCALE, MASKED).astype(np.float32)


def biases(nq):
    group = 2 * nq * FAR_DILATION
    j = np.arange(FAR_DILATION // MIDDLE_DILATION)[:, None]
    t = (np.arange(2 * nq)[None, :] * FAR_DILATION + j * MIDDLE_DILATION).reshape(-1)
    tq, tk = t[:, None], t[None, :]
    both = lambda tq, tk: every(tq, tk, MIDDLE_DILATION).astype(int) + every(tq, tk, FAR_DILATION)
    group0, group1 = both(tq, tk), both(tq + group, tk)
    r = np.arange(FAR_DILATION)[:, None]
    t = (np.arange(TILE)[None, :] * FAR_DILATION + r).reshape(-1)
    tq, tk = t[:, None], t[None, :]
    near0, near1 = near_of(tq, tk), near_of(tq + TILE * FAR_DILATION, tk)
    r = np.arange(2)[:, None]
    t = (np.arange(2 * nq)[None, :] * FAR_DILATION + r).reshape(-1)
    pair2 = every(t[:, None] + 2 * group, t[None, :], FAR_DILATION)
    return [bias_of(np.asarray(x, int)) for x in (group0, group1, near0, near1, pair2)]


def local_kernel(sc_ref, qa_ref, qb_ref, qy_ref, kva_ref, kvb_ref, kvya_ref, kvyb_ref, group_ref, near0_ref, near1_ref,
                 q_ref, m_ref, l_ref, o_ref, k_s, v_s, s_s):
    tp, par = sc_ref[0], sc_ref[1]
    nq = qy_ref.shape[1] // FAR_DILATION
    for h in range(q_ref.shape[0]):
        q, m, l, o, k, v, sh = (x.at[h] for x in (q_ref, m_ref, l_ref, o_ref, k_s, v_s, s_s))
        gather(q, nq, [(qa_ref.at[h], par, tp), (qb_ref.at[h], par, 1 - tp), (qy_ref.at[h], 1 - par, None)])
        gather_kv(k, v, [x.at[h] for x in (kva_ref, kvb_ref, kvya_ref, kvyb_ref)], nq, tp, par)
        at = 0
        items = []
        for r4 in range(MIDDLE_DILATION):
            rows = group_rows(r4, nq)
            items.append((rows, rows, group_ref[...], at))
            scored(items[-1], q, k, sh, m, True)
            at += length(rows)
        for c in range(2 * nq // TILE):
            rows = near_rows(c, nq)
            keys, bias = rows, near0_ref[...]
            if c:
                keys = near_rows(c - 1, nq) + rows
                bias = jnp.concatenate([near1_ref[...], bias], axis=1)
            items.append((rows, keys, bias, at))
            scored(items[-1], q, k, sh, m, False)
            at += length(rows)
        for i, item in enumerate(items):
            ol = weighed(item, v, sh, m, length(item[1]))
            if i < MIDDLE_DILATION:
                put(o, item[0], ol[:, :HEAD])
                put(l, item[0], ol[:, HEAD:])
            else:
                put(o, item[0], take(o, item[0]) + ol[:, :HEAD])
                put(l, item[0], take(l, item[0]) + ol[:, HEAD:])


def one_kernel(sc_ref, q_ref, m_in, l_in, o_in, kva_ref, kvb_ref, kvya_ref, kvyb_ref, group_ref, near_ref,
               m_ref, l_ref, o_ref, k_s, v_s, s_s, n_s):
    tp, par = sc_ref[0], sc_ref[1]
    nq = kvya_ref.shape[2] // FAR_DILATION * 2

    @pl.when(sc_ref[2] >= 1)
    def _():
        for h in range(q_ref.shape[0]):
            q, mi, li, oi, m, l, o, k, v, sh, n = (x.at[h] for x in (
                q_ref, m_in, l_in, o_in, m_ref, l_ref, o_ref, k_s, v_s, s_s, n_s))
            gather_kv(k, v, [x.at[h] for x in (kva_ref, kvb_ref, kvya_ref, kvyb_ref)], nq, tp, par)
            near = (near_rows(0, nq), near_rows(2 * nq // TILE - 1, nq), near_ref[...], 0)
            at = length(near[0])
            items = []
            for r4 in range(MIDDLE_DILATION):
                rows = group_rows(r4, nq)
                items.append((rows, rows, group_ref[...], at))
                scored(items[-1], q, k, sh, n, True)
                at += length(rows)
            scored(near, q, k, sh, n, False)
            for item in items:
                rows = item[0]
                old = take(mi, rows)
                new = jnp.maximum(old, take(n, rows))
                keep = jnp.exp2((old - new) * SCALE)
                put(m, rows, new)
                ol = weighed(item, v, sh, m, length(item[1]))
                put(o, rows, take(oi, rows) * keep + ol[:, :HEAD])
                put(l, rows, take(li, rows) * keep + ol[:, HEAD:])
            ol = weighed(near, v, sh, m, length(near[1]))
            put(o, near[0], take(o, near[0]) + ol[:, :HEAD])
            put(l, near[0], take(l, near[0]) + ol[:, HEAD:])


def two_kernel(sc_ref, q_ref, m_ref, l_ref, o_ref, kva_ref, kvb_ref, kvy_ref, pair_ref,
               keep_ref, send_ref, k_s, v_s, s_s, n_s, mix_s, *, head):
    tp, par = sc_ref[0], sc_ref[1]
    nq = kvy_ref.shape[2] // FAR_DILATION * 2
    q, m, l, o = (x.at[head] for x in (q_ref, m_ref, l_ref, o_ref))
    pairs = [pair_rows(i, nq) for i in range(FAR_DILATION // 2)]

    def settle(i, val):
        for part in range(4):
            r, block = 2 * i + part // 2, part % 2
            mix_s[block, pl.ds(r, nq, stride=FAR_DILATION), :] = val[part * nq:(part + 1) * nq]

    @pl.when(sc_ref[2] >= 2)
    def _():
        gather_kv(k_s, v_s, [kva_ref.at[head], kvb_ref.at[head], kvy_ref.at[0], kvy_ref.at[1]], nq, tp, par)
        items = [(rows, rows, pair_ref[...], i * length(rows)) for i, rows in enumerate(pairs)]
        for item in items:
            put(n_s, item[0], take(m, item[0]))
            scored(item, q, k_s, s_s, n_s, False)
        for i, item in enumerate(items):
            rows = item[0]
            ol = weighed(item, v_s, s_s, n_s, length(rows))
            keep = jnp.exp2((take(m, rows) - take(n_s, rows)) * SCALE)
            settle(i, (take(o, rows) * keep + ol[:, :HEAD]) / (take(l, rows) * keep + ol[:, HEAD:]))

    @pl.when(sc_ref[2] < 2)
    def _():
        for i, rows in enumerate(pairs):
            settle(i, take(o, rows) / take(l, rows))

    keep_ref[...] = mix_s[pl.ds(par, 1)][0].astype(BF16)
    send_ref[...] = mix_s[pl.ds(1 - par, 1)][0].astype(BF16)


def out_terms(sc_ref, x_refs, w_ref, column, block, head):
    tp, par = sc_ref[0], sc_ref[1]
    heads = w_ref.shape[0] // HEAD // 4
    order = (2 * tp + par, 2 * tp + 1 - par, 2 * (1 - tp) + par, 2 * (1 - tp) + 1 - par)
    x = jnp.concatenate([x_ref[...] for x_ref in x_refs], axis=1)
    w = jnp.concatenate([w_ref[pl.ds(pl.multiple_of((i * heads + head) * HEAD, HEAD), HEAD), pl.ds(column, block)]
                         for i in order], axis=0)
    return jnp.dot(x, w, preferred_element_type=F32)


def out_first_kernel(sc_ref, a_ref, b_ref, c_ref, d_ref, w_ref, o_ref):
    block = 2 * HEAD
    for j in range(o_ref.shape[1] // block):
        o_ref[:, j * block:(j + 1) * block] = out_terms(
            sc_ref, (a_ref, b_ref, c_ref, d_ref), w_ref, j * block, block, 0)


def out_last_kernel(sc_ref, a_ref, b_ref, c_ref, d_ref, w_ref, t_ref, o_ref):
    block = o_ref.shape[1]
    column = pl.multiple_of(pl.program_id(0) * block, block)
    total = out_terms(sc_ref, (a_ref, b_ref, c_ref, d_ref), w_ref, column, block, 1)
    o_ref[...] = (t_ref[:, pl.ds(column, block)] + total).astype(BF16)


def out_last(scalars, parts, weight, total):
    rows, columns = total.shape
    steps = columns // (2 * HEAD)
    return pl.pallas_call(
        out_last_kernel,
        grid=(steps,),
        in_specs=[pl.BlockSpec(memory_space=pltpu.SMEM)] + in_vmem(6),
        out_specs=pl.BlockSpec((rows, columns // steps), lambda j: (0, j)),
        out_shape=jax.ShapeDtypeStruct((rows, columns), BF16),
        compiler_params=pltpu.CompilerParams(vmem_limit_bytes=16 * 2 ** 20),
        cost_estimate=pl.CostEstimate(flops=rows * weight.size, transcendentals=0, bytes_accessed=0),
        name="out_last",
    )(scalars, *parts, weight, total)


def swap(x, axis):
    return lax.ppermute(x, axis, [(i, i ^ 1) for i in range(lax.axis_size(axis))])


def onward(x):
    n = lax.axis_size("sp")
    return lax.ppermute(x, "sp", [(i, i + 2) for i in range(n - 2)])


def body(tokens, query_weight, key_weight, value_weight, output_weight):
    half, depth = tokens.shape
    rows = 2 * half
    group = 2 * rows
    nq = rows // FAR_DILATION
    assert 2 * group == FAR_DILATION * REACH_STEPS
    heads = query_weight.shape[1] // HEAD // 2
    width = heads * HEAD
    flops = 2 * rows * depth * width
    sp, tp = lax.axis_index("sp"), lax.axis_index("tp")
    scalars = jnp.stack([tp, sp % 2, sp // 2, sp]).astype(jnp.int32)
    inverse = THETA_BASE ** (-jnp.arange(HEAD // 2, dtype=F32) / (HEAD // 2))
    inverse = jnp.concatenate([inverse, inverse])[None]
    group0, group1, near0, near1, pair2 = biases(nq)
    shape = jax.ShapeDtypeStruct
    kv = shape((heads, 2, half, HEAD), BF16)
    q_shape, q_half = shape((heads, rows, HEAD), BF16), shape((heads, half, HEAD), BF16)
    table = shape((2, half, HEAD), F32)
    buffers = pltpu.VMEM((4 * heads, half, HEAD), F32)

    partner = swap(tokens, "tp")
    kv_a, send_a, weights, cosine, sine = call(
        own_kernel, scalars, [tokens, key_weight, value_weight, inverse],
        [kv, kv, shape((2, 2, depth, width), BF16), table, table],
        [pltpu.VMEM((half, depth), BF16), buffers, pltpu.SemaphoreType.DMA((5,))],
        2 * flops, hbm=(0, 1, 2))
    kv1_a = onward(kv_a)
    kv_ya = swap(send_a, "sp")
    kv_b, send_b = call(
        rest_kernel, scalars, [partner, weights, cosine, sine], [kv, kv], [buffers], 2 * flops)
    kv1_b = onward(kv_b)
    kv_yb = swap(send_b, "sp")
    q_a, q_b, q_send = call(
        q_kernel, scalars, [tokens, partner, cosine, sine, query_weight], [q_half, q_half, q_shape],
        [buffers], 2 * flops)
    q_y = swap(q_send, "sp")
    kv1_ya = onward(kv_ya)
    kv1_yb = onward(kv_yb)
    kv2_a = onward(kv1_a)
    kv2_b = onward(kv1_b)
    kv2_y = []
    for h in range(heads):
        kv2_y.append(onward(jnp.stack([kv1_ya[h], kv1_yb[h]])))
    state = shape((heads, group, HEAD), F32)
    kv_scratch = [pltpu.VMEM((heads, group, HEAD), BF16)] * 2
    q, m, l, o = call(
        local_kernel, scalars, [q_a, q_b, q_y, kv_a, kv_b, kv_ya, kv_yb, group0, near0, near1],
        [shape((heads, group, HEAD), BF16), state, state, state],
        kv_scratch + [pltpu.VMEM((heads, 2 * group, 4 * HEAD), F32)], 3 * 10 ** 9)
    m, l, o = call(
        one_kernel, scalars, [q, m, l, o, kv1_a, kv1_b, kv1_ya, kv1_yb, group1, near1], [state, state, state],
        kv_scratch + [pltpu.VMEM((heads, 2 * group, 2 * HEAD), F32), pltpu.VMEM((heads, group, HEAD), F32)],
        10 ** 9, {2: 0, 3: 1, 4: 2})
    mixed = shape((rows, HEAD), BF16)
    parts = []
    for h in range(heads):
        keep, send = call(
            functools.partial(two_kernel, head=h), scalars, [q, m, l, o, kv2_a, kv2_b, kv2_y[h], pair2], [mixed, mixed],
            [pltpu.VMEM((group, HEAD), BF16)] * 2 + [pltpu.VMEM((group, HEAD), F32)] * 2
            + [pltpu.VMEM((2, rows, HEAD), F32)], 10 ** 9)
        keep_tp = swap(keep, "tp")
        from_y = swap(send, "sp")
        parts.append([keep, from_y, keep_tp, swap(from_y, "tp")])
    total = call(out_first_kernel, scalars, parts[0] + [output_weight],
                 [shape((rows, output_weight.shape[1]), F32)], [], rows * output_weight.size, limit=16)[0]
    return out_last(scalars, parts[1], output_weight, total)


def solution(mesh):
    in_specs = (
        P(("grp", "sp", "tp"), None),
        P(None, "tp"),
        P(None, "tp"),
        P(None, "tp"),
        P(None, "tp"),
    )
    out_specs = P(("grp", "sp"), "tp")

    return jax.shard_map(body, mesh=mesh, in_specs=in_specs, out_specs=out_specs, check_vma=False)
```

```python
import functools

import jax
import jax.numpy as jnp
import numpy as np
from jax import lax
from jax.experimental import pallas as pl
from jax.experimental.pallas import tpu as pltpu
from jax.sharding import PartitionSpec as P

HEAD = 128
REACH_STEPS = 128
MIDDLE_DILATION = 4
FAR_DILATION = 16
THETA_BASE = 500000.0
TILE = 16
MASKED = -1e30
SCALE = HEAD ** -0.5 * 1.4426950408889634
F32 = jnp.float32
BF16 = jnp.bfloat16


def in_vmem(count):
    return [pl.BlockSpec(memory_space=pltpu.VMEM)] * count


def rotated(val, cos, sin):
    return val * cos + pltpu.roll(val, HEAD // 2, 1) * sin


def place(out_ref, lead, val, buf_ref, slot, first):
    nq_half = val.shape[0] // FAR_DILATION
    buf_ref[slot] = val
    for r in range(FAR_DILATION):
        piece = buf_ref[slot, pl.ds(r, nq_half, stride=FAR_DILATION), :]
        at = r * nq_half if first is None else pl.multiple_of((2 * r + first) * nq_half, TILE)
        out_ref[lead + (pl.ds(at, nq_half), slice(None))] = piece.astype(BF16)


def kv_part(x_ref, w_ref, out_ref, cos_ref, sin_ref, buf_ref, ready=None):
    slot = 0
    for which in (1, 0):
        if ready is not None:
            ready[which].wait()
        acc = jnp.dot(x_ref[...], w_ref[which], preferred_element_type=F32)
        for h in range(acc.shape[1] // HEAD):
            val = acc[:, h * HEAD:(h + 1) * HEAD]
            if which == 0:
                val = rotated(val, cos_ref[...], sin_ref[...])
            place(out_ref, (h, which), val, buf_ref, slot, None)
            slot += 1


def weight_copies(wk_hbm, wv_hbm, w_ref, side, sems):
    width = w_ref.shape[2]
    column = pl.multiple_of(side * width, width)
    return [pltpu.make_async_copy(hbm.at[:, pl.ds(column, width)], w_ref.at[which], sems.at[which])
            for which, hbm in enumerate((wk_hbm, wv_hbm))]


def own_keep_kernel(sc_ref, x_hbm, wk_hbm, wv_hbm, inv_ref,
                    out_ref, x_ref, w_ref, cos_ref, sin_ref, buf_ref, sems):
    tp, par, sp = sc_ref[0], sc_ref[1], sc_ref[3]
    half = x_ref.shape[0]
    x_copy = pltpu.make_async_copy(x_hbm, x_ref, sems.at[2])
    copies = weight_copies(wk_hbm, wv_hbm, w_ref, par, sems)
    x_copy.start()
    copies[1].start()
    copies[0].start()
    steps = half // FAR_DILATION
    lane = lax.broadcasted_iota(jnp.int32, (2 * steps, HEAD), 1)
    row = lax.broadcasted_iota(jnp.int32, (2 * steps, HEAD), 0)
    part = jnp.where(row < steps, tp, 1 - tp)
    position = sp * (2 * half) + part * half + (row % steps) * FAR_DILATION
    coarse = position.astype(F32) * inv_ref[...]
    fine = lax.broadcasted_iota(jnp.int32, (FAR_DILATION, HEAD), 0).astype(F32) * inv_ref[...]
    cos_c, sin_c = jnp.cos(coarse)[:, None, :], jnp.sin(coarse)[:, None, :]
    cos_f, sin_f = jnp.cos(fine)[None], jnp.sin(fine)[None]
    sign = jnp.where(lane[:1] < HEAD // 2, -1.0, 1.0)[None]
    cos_ref[...] = (cos_c * cos_f - sin_c * sin_f).reshape(2, half, HEAD)
    sin_ref[...] = ((sin_c * cos_f + cos_c * sin_f) * sign).reshape(2, half, HEAD)
    x_copy.wait()
    kv_part(x_ref, w_ref, out_ref, cos_ref.at[0], sin_ref.at[0], buf_ref, copies)


def rest_keep_kernel(sc_ref, x_ref, w_ref, cos_ref, sin_ref, wk_hbm, wv_hbm, out_ref, w_send_ref, buf_ref, sems):
    copies = weight_copies(wk_hbm, wv_hbm, w_send_ref, 1 - sc_ref[1], sems)
    for copy in copies:
        copy.start()
    kv_part(x_ref, w_ref, out_ref, cos_ref.at[1], sin_ref.at[1], buf_ref)
    for copy in copies:
        copy.wait()


def send_kernel(sc_ref, x_ref, w_ref, cos_ref, sin_ref, out_ref, buf_ref, *, part):
    kv_part(x_ref, w_ref, out_ref, cos_ref.at[part], sin_ref.at[part], buf_ref)


def q_kernel(sc_ref, xo_ref, xp_ref, cos_ref, sin_ref, w_ref, keepa_ref, keepb_ref, send_ref, buf_ref):
    tp, par = sc_ref[0], sc_ref[1]
    heads = send_ref.shape[0]
    width = heads * HEAD
    slot = 0
    for side in (1, 0):
        w = w_ref[:, pl.ds(pl.multiple_of((1 - par if side else par) * width, width), width)]
        for part, x_ref in enumerate((xo_ref, xp_ref)):
            acc = jnp.dot(x_ref[...], w, preferred_element_type=F32)
            for h in range(heads):
                val = rotated(acc[:, h * HEAD:(h + 1) * HEAD], cos_ref[part], sin_ref[part])
                if side:
                    place(send_ref, (h,), val, buf_ref, slot, tp if part == 0 else 1 - tp)
                else:
                    place((keepa_ref, keepb_ref)[part], (h,), val, buf_ref, slot, None)
                slot += 1


def call(kernel, scalars, inputs, outputs, scratch, flops, aliases={}, limit=28, hbm=()):
    spaces = [pltpu.HBM if i in hbm else pltpu.VMEM for i in range(len(inputs))]
    return pl.pallas_call(
        kernel,
        in_specs=[pl.BlockSpec(memory_space=pltpu.SMEM)] + [pl.BlockSpec(memory_space=m) for m in spaces],
        out_specs=in_vmem(len(outputs)),
        out_shape=outputs,
        scratch_shapes=scratch,
        input_output_aliases=aliases,
        compiler_params=pltpu.CompilerParams(vmem_limit_bytes=limit * 2 ** 20),
        cost_estimate=pl.CostEstimate(flops=flops, transcendentals=0, bytes_accessed=0),
    )(scalars, *[pltpu.with_memory_space_constraint(x, pltpu.HBM) if i in hbm else x for i, x in enumerate(inputs)])


def gather(dst_ref, nq, sources):
    for r in range(FAR_DILATION):
        for source, block, half in sources:
            rows = nq if half is None else nq // 2
            start = 0 if half is None else half * (nq // 2)
            at = pl.multiple_of(r * 2 * nq + block * nq + start, TILE)
            dst_ref[pl.ds(at, rows), :] = source[r * rows:(r + 1) * rows, :]


def gather_kv(k_ref, v_ref, refs, nq, tp, par):
    places = ((par, tp), (par, 1 - tp), (1 - par, tp), (1 - par, 1 - tp))
    for which, dst_ref in enumerate((k_ref, v_ref)):
        gather(dst_ref, nq, [(ref.at[which], block, half) for ref, (block, half) in zip(refs, places)])


def scores_of(q, k):
    return lax.dot_general(q, k, (((1,), (1,)), ((), ())), preferred_element_type=F32)


def take(ref, rows):
    parts = [ref[a:a + n, :] for a, n in rows]
    return parts[0] if len(parts) == 1 else jnp.concatenate(parts, axis=0)


def put(ref, rows, value):
    at = 0
    for a, n in rows:
        ref[a:a + n, :] = value[at:at + n]
        at += n


def widened(stat, columns):
    return jnp.concatenate([stat] * (columns // HEAD), axis=1) if columns > HEAD else stat


def scored(item, q_ref, k_ref, s_ref, m_ref, fresh):
    rows, keys, bias, at = item
    s = scores_of(take(q_ref, rows), take(k_ref, keys))
    if bias is not None:
        s = s + bias
    n, columns = s.shape
    s_ref[at:at + n, :columns] = s
    top = jnp.broadcast_to(jnp.max(s, axis=-1, keepdims=True), (n, HEAD))
    put(m_ref, rows, top if fresh else jnp.maximum(take(m_ref, rows), top))


def weighed(item, v_ref, s_ref, m_ref, columns):
    rows, keys, _, at = item
    n = sum(c for _, c in rows)
    p = jnp.exp2((s_ref[at:at + n, :columns] - widened(take(m_ref, rows), columns)) * SCALE).astype(BF16)
    v = take(v_ref, keys)
    return jnp.dot(p, jnp.concatenate([v, jnp.ones_like(v)], axis=1), preferred_element_type=F32)


def length(rows):
    return sum(n for _, n in rows)


def group_rows(r4, nq):
    return [((r4 + MIDDLE_DILATION * j) * 2 * nq, 2 * nq) for j in range(FAR_DILATION // MIDDLE_DILATION)]


def near_rows(c, nq):
    return [(r * 2 * nq + c * TILE, TILE) for r in range(FAR_DILATION)]


def pair_rows(i, nq):
    return [(i * 4 * nq, 4 * nq)]


def near_of(tq, tk):
    return (tq - tk >= 0) & (tq - tk <= REACH_STEPS)


def every(tq, tk, step):
    return (tq % step == tk % step) & (tq - tk >= 0) & (tq - tk <= REACH_STEPS * step)


def bias_of(count):
    return np.where(count > 0, np.log2(np.maximum(count, 1)) / SCALE, MASKED).astype(np.float32)


def biases(nq):
    group = 2 * nq * FAR_DILATION
    j = np.arange(FAR_DILATION // MIDDLE_DILATION)[:, None]
    t = (np.arange(2 * nq)[None, :] * FAR_DILATION + j * MIDDLE_DILATION).reshape(-1)
    tq, tk = t[:, None], t[None, :]
    both = lambda tq, tk: every(tq, tk, MIDDLE_DILATION).astype(int) + every(tq, tk, FAR_DILATION)
    group0, group1 = both(tq, tk), both(tq + group, tk)
    r = np.arange(FAR_DILATION)[:, None]
    t = (np.arange(TILE)[None, :] * FAR_DILATION + r).reshape(-1)
    tq, tk = t[:, None], t[None, :]
    near0, near1 = near_of(tq, tk), near_of(tq + TILE * FAR_DILATION, tk)
    r = np.arange(2)[:, None]
    t = (np.arange(2 * nq)[None, :] * FAR_DILATION + r).reshape(-1)
    pair2 = every(t[:, None] + 2 * group, t[None, :], FAR_DILATION)
    return [bias_of(np.asarray(x, int)) for x in (group0, group1, near0, near1, pair2)]


def local_kernel(sc_ref, qa_ref, qb_ref, qy_ref, kva_ref, kvb_ref, kvya_ref, kvyb_ref, group_ref, near0_ref, near1_ref,
                 q_ref, m_ref, l_ref, o_ref, k_s, v_s, s_s):
    tp, par = sc_ref[0], sc_ref[1]
    nq = qy_ref.shape[1] // FAR_DILATION
    for h in range(q_ref.shape[0]):
        q, m, l, o, k, v, sh = (x.at[h] for x in (q_ref, m_ref, l_ref, o_ref, k_s, v_s, s_s))
        gather(q, nq, [(qa_ref.at[h], par, tp), (qb_ref.at[h], par, 1 - tp), (qy_ref.at[h], 1 - par, None)])
        gather_kv(k, v, [x.at[h] for x in (kva_ref, kvb_ref, kvya_ref, kvyb_ref)], nq, tp, par)
        at = 0
        items = []
        for r4 in range(MIDDLE_DILATION):
            rows = group_rows(r4, nq)
            items.append((rows, rows, group_ref[...], at))
            scored(items[-1], q, k, sh, m, True)
            at += length(rows)
        for c in range(2 * nq // TILE):
            rows = near_rows(c, nq)
            keys, bias = rows, near0_ref[...]
            if c:
                keys = near_rows(c - 1, nq) + rows
                bias = jnp.concatenate([near1_ref[...], bias], axis=1)
            items.append((rows, keys, bias, at))
            scored(items[-1], q, k, sh, m, False)
            at += length(rows)
        for i, item in enumerate(items):
            ol = weighed(item, v, sh, m, length(item[1]))
            if i < MIDDLE_DILATION:
                put(o, item[0], ol[:, :HEAD])
                put(l, item[0], ol[:, HEAD:])
            else:
                put(o, item[0], take(o, item[0]) + ol[:, :HEAD])
                put(l, item[0], take(l, item[0]) + ol[:, HEAD:])


def one_kernel(sc_ref, q_ref, m_in, l_in, o_in, kva_ref, kvb_ref, kvya_ref, kvyb_ref, group_ref, near_ref,
               m_ref, l_ref, o_ref, k_s, v_s, s_s, n_s):
    tp, par = sc_ref[0], sc_ref[1]
    nq = kvya_ref.shape[2] // FAR_DILATION * 2

    @pl.when(sc_ref[2] >= 1)
    def _():
        for h in range(q_ref.shape[0]):
            q, mi, li, oi, m, l, o, k, v, sh, n = (x.at[h] for x in (
                q_ref, m_in, l_in, o_in, m_ref, l_ref, o_ref, k_s, v_s, s_s, n_s))
            gather_kv(k, v, [x.at[h] for x in (kva_ref, kvb_ref, kvya_ref, kvyb_ref)], nq, tp, par)
            near = (near_rows(0, nq), near_rows(2 * nq // TILE - 1, nq), near_ref[...], 0)
            at = length(near[0])
            items = []
            for r4 in range(MIDDLE_DILATION):
                rows = group_rows(r4, nq)
                items.append((rows, rows, group_ref[...], at))
                scored(items[-1], q, k, sh, n, True)
                at += length(rows)
            scored(near, q, k, sh, n, False)
            for item in items:
                rows = item[0]
                old = take(mi, rows)
                new = jnp.maximum(old, take(n, rows))
                keep = jnp.exp2((old - new) * SCALE)
                put(m, rows, new)
                ol = weighed(item, v, sh, m, length(item[1]))
                put(o, rows, take(oi, rows) * keep + ol[:, :HEAD])
                put(l, rows, take(li, rows) * keep + ol[:, HEAD:])
            ol = weighed(near, v, sh, m, length(near[1]))
            put(o, near[0], take(o, near[0]) + ol[:, :HEAD])
            put(l, near[0], take(l, near[0]) + ol[:, HEAD:])


def two_kernel(sc_ref, q_ref, m_ref, l_ref, o_ref, kva_ref, kvb_ref, kvy_ref, pair_ref,
               keep_ref, send_ref, k_s, v_s, s_s, n_s, mix_s, *, head):
    tp, par = sc_ref[0], sc_ref[1]
    nq = kvy_ref.shape[2] // FAR_DILATION * 2
    q, m, l, o = (x.at[head] for x in (q_ref, m_ref, l_ref, o_ref))
    pairs = [pair_rows(i, nq) for i in range(FAR_DILATION // 2)]

    def settle(i, val):
        for part in range(4):
            r, block = 2 * i + part // 2, part % 2
            mix_s[block, pl.ds(r, nq, stride=FAR_DILATION), :] = val[part * nq:(part + 1) * nq]

    @pl.when(sc_ref[2] >= 2)
    def _():
        gather_kv(k_s, v_s, [kva_ref.at[head], kvb_ref.at[head], kvy_ref.at[0], kvy_ref.at[1]], nq, tp, par)
        items = [(rows, rows, pair_ref[...], i * length(rows)) for i, rows in enumerate(pairs)]
        for item in items:
            put(n_s, item[0], take(m, item[0]))
            scored(item, q, k_s, s_s, n_s, False)
        for i, item in enumerate(items):
            rows = item[0]
            ol = weighed(item, v_s, s_s, n_s, length(rows))
            keep = jnp.exp2((take(m, rows) - take(n_s, rows)) * SCALE)
            settle(i, (take(o, rows) * keep + ol[:, :HEAD]) / (take(l, rows) * keep + ol[:, HEAD:]))

    @pl.when(sc_ref[2] < 2)
    def _():
        for i, rows in enumerate(pairs):
            settle(i, take(o, rows) / take(l, rows))

    keep_ref[...] = mix_s[pl.ds(par, 1)][0].astype(BF16)
    send_ref[...] = mix_s[pl.ds(1 - par, 1)][0].astype(BF16)


def out_terms(sc_ref, x_refs, w_ref, column, block, head):
    tp, par = sc_ref[0], sc_ref[1]
    heads = w_ref.shape[0] // HEAD // 4
    order = (2 * tp + par, 2 * tp + 1 - par, 2 * (1 - tp) + par, 2 * (1 - tp) + 1 - par)
    x = jnp.concatenate([x_ref[...] for x_ref in x_refs], axis=1)
    w = jnp.concatenate([w_ref[pl.ds(pl.multiple_of((i * heads + head) * HEAD, HEAD), HEAD), pl.ds(column, block)]
                         for i in order], axis=0)
    return jnp.dot(x, w, preferred_element_type=F32)


def out_first_kernel(sc_ref, a_ref, b_ref, c_ref, d_ref, w_ref, o_ref):
    block = 2 * HEAD
    for j in range(o_ref.shape[1] // block):
        o_ref[:, j * block:(j + 1) * block] = out_terms(
            sc_ref, (a_ref, b_ref, c_ref, d_ref), w_ref, j * block, block, 0)


def out_last_kernel(sc_ref, a_ref, b_ref, c_ref, d_ref, w_ref, t_ref, o_ref):
    block = o_ref.shape[1]
    column = pl.multiple_of(pl.program_id(0) * block, block)
    total = out_terms(sc_ref, (a_ref, b_ref, c_ref, d_ref), w_ref, column, block, 1)
    o_ref[...] = (t_ref[:, pl.ds(column, block)] + total).astype(BF16)


def out_last(scalars, parts, weight, total):
    rows, columns = total.shape
    steps = 2
    return pl.pallas_call(
        out_last_kernel,
        grid=(steps,),
        in_specs=[pl.BlockSpec(memory_space=pltpu.SMEM)] + in_vmem(6),
        out_specs=pl.BlockSpec((rows, columns // steps), lambda j: (0, j)),
        out_shape=jax.ShapeDtypeStruct((rows, columns), BF16),
        compiler_params=pltpu.CompilerParams(vmem_limit_bytes=16 * 2 ** 20),
        cost_estimate=pl.CostEstimate(flops=rows * weight.size, transcendentals=0, bytes_accessed=0),
        name="out_last",
    )(scalars, *parts, weight, total)


def swap(x, axis):
    return lax.ppermute(x, axis, [(i, i ^ 1) for i in range(lax.axis_size(axis))])


def onward(x):
    n = lax.axis_size("sp")
    return lax.ppermute(x, "sp", [(i, i + 2) for i in range(n - 2)])


def body(tokens, query_weight, key_weight, value_weight, output_weight):
    half, depth = tokens.shape
    rows = 2 * half
    group = 2 * rows
    nq = rows // FAR_DILATION
    assert 2 * group == FAR_DILATION * REACH_STEPS
    heads = query_weight.shape[1] // HEAD // 2
    width = heads * HEAD
    flops = 2 * rows * depth * width
    sp, tp = lax.axis_index("sp"), lax.axis_index("tp")
    scalars = jnp.stack([tp, sp % 2, sp // 2, sp]).astype(jnp.int32)
    inverse = THETA_BASE ** (-jnp.arange(HEAD // 2, dtype=F32) / (HEAD // 2))
    inverse = jnp.concatenate([inverse, inverse])[None]
    group0, group1, near0, near1, pair2 = biases(nq)
    shape = jax.ShapeDtypeStruct
    kv = shape((heads, 2, half, HEAD), BF16)
    q_shape, q_half = shape((heads, rows, HEAD), BF16), shape((heads, half, HEAD), BF16)
    table = shape((2, half, HEAD), F32)
    buffers = pltpu.VMEM((4 * heads, half, HEAD), F32)

    partner = swap(tokens, "tp")
    weights = shape((2, depth, width), BF16)
    kv_a, own, w_keep, cosine, sine = call(
        own_keep_kernel, scalars, [tokens, key_weight, value_weight, inverse],
        [kv, shape((half, depth), BF16), weights, table, table],
        [buffers, pltpu.SemaphoreType.DMA((3,))], flops, hbm=(0, 1, 2))
    kv1_a = onward(kv_a)
    kv_b, w_send = call(
        rest_keep_kernel, scalars, [partner, w_keep, cosine, sine, key_weight, value_weight], [kv, weights],
        [buffers, pltpu.SemaphoreType.DMA((2,))], flops, hbm=(4, 5))
    kv1_b = onward(kv_b)
    send_a, = call(functools.partial(send_kernel, part=0), scalars, [own, w_send, cosine, sine], [kv], [buffers],
                   flops)
    kv_ya = swap(send_a, "sp")
    send_b, = call(functools.partial(send_kernel, part=1), scalars, [partner, w_send, cosine, sine], [kv], [buffers],
                   flops)
    kv_yb = swap(send_b, "sp")
    q_a, q_b, q_send = call(
        q_kernel, scalars, [own, partner, cosine, sine, query_weight], [q_half, q_half, q_shape],
        [buffers], 2 * flops)
    q_y = swap(q_send, "sp")
    kv1_ya = onward(kv_ya)
    kv1_yb = onward(kv_yb)
    kv2_a = onward(kv1_a)
    kv2_b = onward(kv1_b)
    kv2_y = []
    for h in range(heads):
        kv2_y.append(onward(jnp.stack([kv1_ya[h], kv1_yb[h]])))
    state = shape((heads, group, HEAD), F32)
    kv_scratch = [pltpu.VMEM((heads, group, HEAD), BF16)] * 2
    q, m, l, o = call(
        local_kernel, scalars, [q_a, q_b, q_y, kv_a, kv_b, kv_ya, kv_yb, group0, near0, near1],
        [shape((heads, group, HEAD), BF16), state, state, state],
        kv_scratch + [pltpu.VMEM((heads, 2 * group, 4 * HEAD), F32)], 3 * 10 ** 9)
    m, l, o = call(
        one_kernel, scalars, [q, m, l, o, kv1_a, kv1_b, kv1_ya, kv1_yb, group1, near1], [state, state, state],
        kv_scratch + [pltpu.VMEM((heads, 2 * group, 2 * HEAD), F32), pltpu.VMEM((heads, group, HEAD), F32)],
        10 ** 9, {2: 0, 3: 1, 4: 2})
    mixed = shape((rows, HEAD), BF16)
    parts = []
    for h in range(heads):
        keep, send = call(
            functools.partial(two_kernel, head=h), scalars, [q, m, l, o, kv2_a, kv2_b, kv2_y[h], pair2], [mixed, mixed],
            [pltpu.VMEM((group, HEAD), BF16)] * 2 + [pltpu.VMEM((group, HEAD), F32)] * 2
            + [pltpu.VMEM((2, rows, HEAD), F32)], 10 ** 9)
        keep_tp = swap(keep, "tp")
        from_y = swap(send, "sp")
        parts.append([keep, from_y, keep_tp, swap(from_y, "tp")])
    total = call(out_first_kernel, scalars, parts[0] + [output_weight],
                 [shape((rows, output_weight.shape[1]), F32)], [], rows * output_weight.size, limit=16)[0]
    return out_last(scalars, parts[1], output_weight, total)


def solution(mesh):
    in_specs = (
        P(("grp", "sp", "tp"), None),
        P(None, "tp"),
        P(None, "tp"),
        P(None, "tp"),
        P(None, "tp"),
    )
    out_specs = P(("grp", "sp"), "tp")

    return jax.shard_map(body, mesh=mesh, in_specs=in_specs, out_specs=out_specs, check_vma=False)
```

```python
import functools

import jax
import jax.numpy as jnp
import numpy as np
from jax import lax
from jax.experimental import pallas as pl
from jax.experimental.pallas import tpu as pltpu
from jax.sharding import PartitionSpec as P

HEAD = 128
REACH_STEPS = 128
MIDDLE_DILATION = 4
FAR_DILATION = 16
THETA_BASE = 500000.0
TILE = 16
RELAYED = 1
MASKED = -1e30
SCALE = HEAD ** -0.5 * 1.4426950408889634
F32 = jnp.float32
BF16 = jnp.bfloat16


def in_vmem(count):
    return [pl.BlockSpec(memory_space=pltpu.VMEM)] * count


def rotated(val, cos, sin):
    return val * cos + pltpu.roll(val, HEAD // 2, 1) * sin


def place(out_ref, lead, val, buf_ref, slot, first):
    nq_half = val.shape[0] // FAR_DILATION
    buf_ref[slot] = val
    for r in range(FAR_DILATION):
        piece = buf_ref[slot, pl.ds(r, nq_half, stride=FAR_DILATION), :]
        at = r * nq_half if first is None else pl.multiple_of((2 * r + first) * nq_half, TILE)
        out_ref[lead + (pl.ds(at, nq_half), slice(None))] = piece.astype(BF16)


def kv_part(x_ref, w_refs, out_ref, cos_ref, sin_ref, buf_ref, ready=None):
    slot = 0
    for which in (1, 0):
        if ready is not None:
            ready[which].wait()
        acc = jnp.dot(x_ref[...], w_refs[which][...], preferred_element_type=F32)
        for h in range(acc.shape[1] // HEAD):
            val = acc[:, h * HEAD:(h + 1) * HEAD]
            if which == 0:
                val = rotated(val, cos_ref[...], sin_ref[...])
            place(out_ref, (h, which), val, buf_ref, slot, None)
            slot += 1


def weight_copies(wk_hbm, wv_hbm, w_ref, side, sems):
    width = w_ref.shape[2]
    column = pl.multiple_of(side * width, width)
    return [pltpu.make_async_copy(hbm.at[:, pl.ds(column, width)], w_ref.at[which], sems.at[which])
            for which, hbm in enumerate((wk_hbm, wv_hbm))]


def own_keep_kernel(sc_ref, x_hbm, wk_hbm, wv_hbm, inv_ref,
                    out_ref, x_ref, w_ref, cos_ref, sin_ref, buf_ref, sems):
    tp, par, sp = sc_ref[0], sc_ref[1], sc_ref[3]
    half = x_ref.shape[0]
    x_copy = pltpu.make_async_copy(x_hbm, x_ref, sems.at[2])
    copies = weight_copies(wk_hbm, wv_hbm, w_ref, par, sems)
    x_copy.start()
    copies[1].start()
    steps = half // FAR_DILATION
    lane = lax.broadcasted_iota(jnp.int32, (2 * steps, HEAD), 1)
    row = lax.broadcasted_iota(jnp.int32, (2 * steps, HEAD), 0)
    part = jnp.where(row < steps, tp, 1 - tp)
    position = sp * (2 * half) + part * half + (row % steps) * FAR_DILATION
    coarse = position.astype(F32) * inv_ref[...]
    fine = lax.broadcasted_iota(jnp.int32, (FAR_DILATION, HEAD), 0).astype(F32) * inv_ref[...]
    cos_c, sin_c = jnp.cos(coarse)[:, None, :], jnp.sin(coarse)[:, None, :]
    cos_f, sin_f = jnp.cos(fine)[None], jnp.sin(fine)[None]
    sign = jnp.where(lane[:1] < HEAD // 2, -1.0, 1.0)[None]
    cos_ref[...] = (cos_c * cos_f - sin_c * sin_f).reshape(2, half, HEAD)
    sin_ref[...] = ((sin_c * cos_f + cos_c * sin_f) * sign).reshape(2, half, HEAD)
    x_copy.wait()
    copies[0].start()
    kv_part(x_ref, (w_ref.at[0], w_ref.at[1]), out_ref, cos_ref.at[0], sin_ref.at[0], buf_ref, copies)


def rest_keep_kernel(sc_ref, x_ref, w_ref, cos_ref, sin_ref, out_ref, buf_ref):
    kv_part(x_ref, (w_ref.at[0], w_ref.at[1]), out_ref, cos_ref.at[1], sin_ref.at[1], buf_ref)


def send_kernel(sc_ref, x_ref, wk_ref, wv_ref, cos_ref, sin_ref, out_ref, buf_ref, *, part):
    width = out_ref.shape[0] * HEAD
    column = pl.ds(pl.multiple_of((1 - sc_ref[1]) * width, width), width)
    kv_part(x_ref, (wk_ref.at[:, column], wv_ref.at[:, column]), out_ref, cos_ref.at[part], sin_ref.at[part], buf_ref)


def q_kernel(sc_ref, xo_ref, xp_ref, cos_ref, sin_ref, w_ref, keepa_ref, keepb_ref, send_ref,
             back_ref, buf_ref):
    tp, par = sc_ref[0], sc_ref[1]
    heads = send_ref.shape[0]
    width = heads * HEAD
    slot = 0
    for side in (1, 0):
        w = w_ref[:, pl.ds(pl.multiple_of((1 - par if side else par) * width, width), width)]
        for part, x_ref in enumerate((xo_ref, xp_ref)):
            acc = jnp.dot(x_ref[...], w, preferred_element_type=F32)
            for h in range(heads):
                val = rotated(acc[:, h * HEAD:(h + 1) * HEAD], cos_ref[part], sin_ref[part])
                if side:
                    place(send_ref, (h,), val, buf_ref, slot, tp if part == 0 else 1 - tp)
                else:
                    place((keepa_ref, keepb_ref)[part], (h,), val, buf_ref, slot, None)
                if h >= RELAYED and not side:
                    place(back_ref, (h - RELAYED, part), val, buf_ref, slot, None)
                slot += 1


def call(kernel, scalars, inputs, outputs, scratch, flops, aliases={}, limit=28, hbm=()):
    spaces = [pltpu.HBM if i in hbm else pltpu.VMEM for i in range(len(inputs))]
    return pl.pallas_call(
        kernel,
        in_specs=[pl.BlockSpec(memory_space=pltpu.SMEM)] + [pl.BlockSpec(memory_space=m) for m in spaces],
        out_specs=in_vmem(len(outputs)),
        out_shape=outputs,
        scratch_shapes=scratch,
        input_output_aliases=aliases,
        compiler_params=pltpu.CompilerParams(vmem_limit_bytes=limit * 2 ** 20),
        cost_estimate=pl.CostEstimate(flops=flops, transcendentals=0, bytes_accessed=0),
    )(scalars, *[pltpu.with_memory_space_constraint(x, pltpu.HBM) if i in hbm else x for i, x in enumerate(inputs)])


def gather(dst_ref, nq, sources):
    for r in range(FAR_DILATION):
        for source, block, half in sources:
            rows = nq if half is None else nq // 2
            start = 0 if half is None else half * (nq // 2)
            at = pl.multiple_of(r * 2 * nq + block * nq + start, TILE)
            dst_ref[pl.ds(at, rows), :] = source[r * rows:(r + 1) * rows, :]


def gather_kv(k_ref, v_ref, refs, nq, tp, par):
    places = ((par, tp), (par, 1 - tp), (1 - par, tp), (1 - par, 1 - tp))
    for which, dst_ref in enumerate((k_ref, v_ref)):
        gather(dst_ref, nq, [(ref.at[which], block, half) for ref, (block, half) in zip(refs, places)])


def scores_of(q, k):
    return lax.dot_general(q, k, (((1,), (1,)), ((), ())), preferred_element_type=F32)


def take(ref, rows):
    parts = [ref[a:a + n, :] for a, n in rows]
    return parts[0] if len(parts) == 1 else jnp.concatenate(parts, axis=0)


def put(ref, rows, value):
    at = 0
    for a, n in rows:
        ref[a:a + n, :] = value[at:at + n]
        at += n


def widened(stat, columns):
    return jnp.concatenate([stat] * (columns // HEAD), axis=1) if columns > HEAD else stat


def scored(item, q_ref, k_ref, s_ref, m_ref, fresh):
    rows, keys, bias, at = item
    s = scores_of(take(q_ref, rows), take(k_ref, keys))
    if bias is not None:
        s = s + bias
    n, columns = s.shape
    s_ref[at:at + n, :columns] = s
    top = jnp.broadcast_to(jnp.max(s, axis=-1, keepdims=True), (n, HEAD))
    put(m_ref, rows, top if fresh else jnp.maximum(take(m_ref, rows), top))


def weighed(item, v_ref, s_ref, m_ref, columns):
    rows, keys, _, at = item
    n = sum(c for _, c in rows)
    p = jnp.exp2((s_ref[at:at + n, :columns] - widened(take(m_ref, rows), columns)) * SCALE).astype(BF16)
    v = take(v_ref, keys)
    return jnp.dot(p, jnp.concatenate([v, jnp.ones_like(v)], axis=1), preferred_element_type=F32)


def length(rows):
    return sum(n for _, n in rows)


def group_rows(r4, nq):
    return [((r4 + MIDDLE_DILATION * j) * 2 * nq, 2 * nq) for j in range(FAR_DILATION // MIDDLE_DILATION)]


def near_rows(c, nq):
    return [(r * 2 * nq + c * TILE, TILE) for r in range(FAR_DILATION)]


def pair_rows(i, nq):
    return [(i * 4 * nq, 4 * nq)]


def near_of(tq, tk):
    return (tq - tk >= 0) & (tq - tk <= REACH_STEPS)


def every(tq, tk, step):
    return (tq % step == tk % step) & (tq - tk >= 0) & (tq - tk <= REACH_STEPS * step)


def bias_of(count):
    return np.where(count > 0, np.log2(np.maximum(count, 1)) / SCALE, MASKED).astype(np.float32)


def biases(nq):
    group = 2 * nq * FAR_DILATION
    j = np.arange(FAR_DILATION // MIDDLE_DILATION)[:, None]
    t = (np.arange(2 * nq)[None, :] * FAR_DILATION + j * MIDDLE_DILATION).reshape(-1)
    tq, tk = t[:, None], t[None, :]
    both = lambda tq, tk: every(tq, tk, MIDDLE_DILATION).astype(int) + every(tq, tk, FAR_DILATION)
    group0, group1 = both(tq, tk), both(tq + group, tk)
    r = np.arange(FAR_DILATION)[:, None]
    t = (np.arange(TILE)[None, :] * FAR_DILATION + r).reshape(-1)
    tq, tk = t[:, None], t[None, :]
    near0, near1 = near_of(tq, tk), near_of(tq + TILE * FAR_DILATION, tk)
    r = np.arange(2)[:, None]
    t = (np.arange(2 * nq)[None, :] * FAR_DILATION + r).reshape(-1)
    pair2 = every(t[:, None] + 2 * group, t[None, :], FAR_DILATION)
    return [bias_of(np.asarray(x, int)) for x in (group0, group1, near0, near1, pair2)]


def local_kernel(sc_ref, qa_ref, qb_ref, qy_ref, kva_ref, kvb_ref, kvya_ref, kvyb_ref, group_ref, near0_ref, near1_ref,
                 q_ref, m_ref, l_ref, o_ref, k_s, v_s, s_s):
    tp, par = sc_ref[0], sc_ref[1]
    nq = qy_ref.shape[1] // FAR_DILATION
    for h in range(q_ref.shape[0]):
        q, m, l, o, k, v, sh = (x.at[h] for x in (q_ref, m_ref, l_ref, o_ref, k_s, v_s, s_s))
        gather(q, nq, [(qa_ref.at[h], par, tp), (qb_ref.at[h], par, 1 - tp), (qy_ref.at[h], 1 - par, None)])
        gather_kv(k, v, [x.at[h] for x in (kva_ref, kvb_ref, kvya_ref, kvyb_ref)], nq, tp, par)
        at = 0
        items = []
        for r4 in range(MIDDLE_DILATION):
            rows = group_rows(r4, nq)
            items.append((rows, rows, group_ref[...], at))
            scored(items[-1], q, k, sh, m, True)
            at += length(rows)
        for c in range(2 * nq // TILE):
            rows = near_rows(c, nq)
            keys, bias = rows, near0_ref[...]
            if c:
                keys = near_rows(c - 1, nq) + rows
                bias = jnp.concatenate([near1_ref[...], bias], axis=1)
            items.append((rows, keys, bias, at))
            scored(items[-1], q, k, sh, m, False)
            at += length(rows)
        for i, item in enumerate(items):
            ol = weighed(item, v, sh, m, length(item[1]))
            if i < MIDDLE_DILATION:
                put(o, item[0], ol[:, :HEAD])
                put(l, item[0], ol[:, HEAD:])
            else:
                put(o, item[0], take(o, item[0]) + ol[:, :HEAD])
                put(l, item[0], take(l, item[0]) + ol[:, HEAD:])


def one_kernel(sc_ref, q_ref, m_in, l_in, o_in, kva_ref, kvb_ref, kvya_ref, kvyb_ref, group_ref, near_ref,
               m_ref, l_ref, o_ref, state_ref, k_s, v_s, s_s, n_s, piece_s, stat_s):
    tp, par = sc_ref[0], sc_ref[1]
    nq = kvya_ref.shape[2] // FAR_DILATION * 2

    @pl.when(sc_ref[2] >= 1)
    def _():
        for h in range(q_ref.shape[0]):
            q, mi, li, oi, m, l, o, k, v, sh, n = (x.at[h] for x in (
                q_ref, m_in, l_in, o_in, m_ref, l_ref, o_ref, k_s, v_s, s_s, n_s))
            gather_kv(k, v, [x.at[h] for x in (kva_ref, kvb_ref, kvya_ref, kvyb_ref)], nq, tp, par)
            near = (near_rows(0, nq), near_rows(2 * nq // TILE - 1, nq), near_ref[...], 0)
            at = length(near[0])
            items = []
            for r4 in range(MIDDLE_DILATION):
                rows = group_rows(r4, nq)
                items.append((rows, rows, group_ref[...], at))
                scored(items[-1], q, k, sh, n, True)
                at += length(rows)
            scored(near, q, k, sh, n, False)
            for item in items:
                rows = item[0]
                old = take(mi, rows)
                new = jnp.maximum(old, take(n, rows))
                keep = jnp.exp2((old - new) * SCALE)
                put(m, rows, new)
                ol = weighed(item, v, sh, m, length(item[1]))
                put(o, rows, take(oi, rows) * keep + ol[:, :HEAD])
                put(l, rows, take(li, rows) * keep + ol[:, HEAD:])
            ol = weighed(near, v, sh, m, length(near[1]))
            put(o, near[0], take(o, near[0]) + ol[:, :HEAD])
            put(l, near[0], take(l, near[0]) + ol[:, HEAD:])

    for i in range(FAR_DILATION // 2):
        rows = pair_rows(i, nq)
        m, l, o = (take(x.at[RELAYED], rows) for x in (m_ref, l_ref, o_ref))
        pack_rows(piece_s, stat_s, i, o / l, m, l)
    pack_out(state_ref, piece_s, stat_s, 1 - par)


def two_kernel(sc_ref, q_ref, m_ref, l_ref, o_ref, kvo_ref, kvy_ref, pair_ref,
               keep_ref, send_ref, k_s, v_s, s_s, n_s, mix_s, *, head):
    tp, par = sc_ref[0], sc_ref[1]
    nq = kvy_ref.shape[2] // FAR_DILATION * 2
    q, m, l, o = (x.at[head] for x in (q_ref, m_ref, l_ref, o_ref))
    pairs = [pair_rows(i, nq) for i in range(FAR_DILATION // 2)]

    def settle(i, val):
        for part in range(4):
            r, block = 2 * i + part // 2, part % 2
            mix_s[block, pl.ds(r, nq, stride=FAR_DILATION), :] = val[part * nq:(part + 1) * nq]

    @pl.when(sc_ref[2] >= 2)
    def _():
        gather_kv(k_s, v_s, [kvo_ref.at[0], kvo_ref.at[1], kvy_ref.at[0], kvy_ref.at[1]], nq, tp, par)
        items = [(rows, rows, pair_ref[...], i * length(rows)) for i, rows in enumerate(pairs)]
        for item in items:
            put(n_s, item[0], take(m, item[0]))
            scored(item, q, k_s, s_s, n_s, False)
        for i, item in enumerate(items):
            rows = item[0]
            ol = weighed(item, v_s, s_s, n_s, length(rows))
            keep = jnp.exp2((take(m, rows) - take(n_s, rows)) * SCALE)
            settle(i, (take(o, rows) * keep + ol[:, :HEAD]) / (take(l, rows) * keep + ol[:, HEAD:]))

    @pl.when(sc_ref[2] < 2)
    def _():
        for i, rows in enumerate(pairs):
            settle(i, take(o, rows) / take(l, rows))

    keep_ref[...] = mix_s[pl.ds(par, 1)][0].astype(BF16)
    send_ref[...] = mix_s[pl.ds(1 - par, 1)][0].astype(BF16)


def diagonal(n):
    return lax.broadcasted_iota(jnp.int32, (n, n), 0) == lax.broadcasted_iota(jnp.int32, (n, n), 1)


def pack_rows(piece_s, stat_s, i, value, top, total):
    nq = value.shape[0] // 4
    eye = diagonal(HEAD)
    for part in range(4):
        r, block = 2 * i + part // 2, part % 2
        piece_s[block, r * nq:(r + 1) * nq, :] = value[part * nq:(part + 1) * nq].astype(BF16)
    for which, stat in enumerate((top, total)):
        at = which * (FAR_DILATION // 2) + i
        stat_s[at:at + 1, :] = jnp.sum(jnp.where(eye, stat, 0.0), axis=0, keepdims=True)


def pack_out(out_ref, piece_s, stat_s, block):
    rows, count = piece_s.shape[1], stat_s.shape[0]
    out_ref[:rows, :] = piece_s[pl.ds(block, 1)][0]
    rest = stat_s[...]
    for term in range(3):
        low = rest.astype(BF16)
        out_ref[rows + term * count:rows + (term + 1) * count, :] = low
        rest = rest - low.astype(F32)


def unpacked_stats(ref, rows):
    return sum(ref[rows + t * FAR_DILATION:rows + (t + 1) * FAR_DILATION, :].astype(F32) for t in range(3))


def foreign_kernel(sc_ref, qn_ref, kva_ref, kvb_ref, kvya_ref, kvyb_ref, pair_ref,
                   own_ref, diag_ref, q_s, k_s, v_s, s_s, n_s, piece_s, stat_s, *, head):
    tp, par = sc_ref[0], sc_ref[1]
    nq = kvya_ref.shape[2] // FAR_DILATION * 2
    half = kvya_ref.shape[2]
    gather(q_s, nq, [(qn_ref.at[0, :half], par, tp), (qn_ref.at[0, half:], par, 1 - tp), (qn_ref.at[1], 1 - par, None)])
    gather_kv(k_s, v_s, [x.at[head] for x in (kva_ref, kvb_ref, kvya_ref, kvyb_ref)], nq, tp, par)
    pairs = [pair_rows(i, nq) for i in range(FAR_DILATION // 2)]
    items = [(rows, rows, pair_ref[...], i * length(rows)) for i, rows in enumerate(pairs)]
    for item in items:
        scored(item, q_s, k_s, s_s, n_s, True)
    for i, item in enumerate(items):
        ol = weighed(item, v_s, s_s, n_s, length(item[0]))
        total = ol[:, HEAD:]
        pack_rows(piece_s, stat_s, i, ol[:, :HEAD] / total, take(n_s, item[0]), total)
    pack_out(own_ref, piece_s, stat_s, par)
    pack_out(diag_ref, piece_s, stat_s, 1 - par)


def final_kernel(sc_ref, m_ref, l_ref, o_ref, state_ref, own_ref, diag_ref, out_ref, mix_s, *, head):
    par = sc_ref[1]
    m, l, o = (x.at[head] for x in (m_ref, l_ref, o_ref))
    rows = out_ref.shape[1]
    nq = rows // FAR_DILATION
    count = FAR_DILATION // 2
    far = sc_ref[2] >= 2
    eye = diagonal(HEAD)

    def columns(ref):
        stats = unpacked_stats(ref, rows)
        result = []
        for i in range(2 * count):
            spread = jnp.sum(jnp.where(eye, stats[i:i + 1, :], 0.0), axis=1, keepdims=True)
            result.append(jnp.broadcast_to(spread, (HEAD, HEAD)))
        return result

    def rows_of(result, which, r):
        column = result[which * count + r // 2]
        at = (r % 2) * 2 * nq
        return jnp.where(par == 0, column[at:at + nq], column[at + nq:at + 2 * nq])

    def joined(top, total, numerator, ref, result, r):
        top2, total2 = rows_of(result, 0, r), rows_of(result, 1, r)
        top2 = jnp.where(far, top2, MASKED)
        new = jnp.maximum(top, top2)
        keep = jnp.exp2((top - new) * SCALE)
        add = jnp.where(far, jnp.exp2((top2 - new) * SCALE) * total2, 0.0)
        part = jnp.where(far, ref[r * nq:(r + 1) * nq, :].astype(F32), 0.0)
        return (numerator * keep + part * add) / (total * keep + add)

    own_stats, diag_stats, state_stats = columns(own_ref), columns(diag_ref), columns(state_ref)
    for r in range(FAR_DILATION):
        here = pl.ds(pl.multiple_of(r * 2 * nq + par * nq, TILE), nq)
        mix_s[0, pl.ds(r, nq, stride=FAR_DILATION), :] = joined(
            m[here, :], l[here, :], o[here, :], own_ref, own_stats, r)
        top, total = rows_of(state_stats, 0, r), rows_of(state_stats, 1, r)
        mix_s[1, pl.ds(r, nq, stride=FAR_DILATION), :] = joined(
            top, total, state_ref[r * nq:(r + 1) * nq, :].astype(F32) * total, diag_ref, diag_stats, r)
    out_ref[...] = mix_s[...].astype(BF16)


def out_kernel(sc_ref, a_ref, b_ref, c_ref, d_ref, own_ref, tp_ref, w_ref, o_ref):
    tp, par = sc_ref[0], sc_ref[1]
    block = o_ref.shape[1]
    heads = w_ref.shape[0] // HEAD // 4
    column = pl.multiple_of(pl.program_id(0) * block, block)
    order = (2 * tp + par, 2 * tp + 1 - par, 2 * (1 - tp) + par, 2 * (1 - tp) + 1 - par)
    x_refs = (own_ref.at[0], own_ref.at[1], tp_ref.at[0], tp_ref.at[1], a_ref, b_ref, c_ref, d_ref)
    x = jnp.concatenate([x_ref[...] for x_ref in x_refs], axis=1)
    w = jnp.concatenate([w_ref[pl.ds(pl.multiple_of((i * heads + head) * HEAD, HEAD), HEAD), pl.ds(column, block)]
                         for head in (1, 0) for i in order], axis=0)
    o_ref[...] = jnp.dot(x, w, preferred_element_type=F32).astype(BF16)


def out_project(scalars, first, last, weight):
    rows, columns = first[0].shape[0], weight.shape[1]
    steps = 2
    return pl.pallas_call(
        out_kernel,
        grid=(steps,),
        in_specs=[pl.BlockSpec(memory_space=pltpu.SMEM)] + in_vmem(7),
        out_specs=pl.BlockSpec((rows, columns // steps), lambda j: (0, j)),
        out_shape=jax.ShapeDtypeStruct((rows, columns), BF16),
        compiler_params=pltpu.CompilerParams(vmem_limit_bytes=16 * 2 ** 20),
        cost_estimate=pl.CostEstimate(flops=2 * rows * weight.size, transcendentals=0, bytes_accessed=0),
        name="out_project",
    )(scalars, *first, *last, weight)


def swap(x, axis):
    return lax.ppermute(x, axis, [(i, i ^ 1) for i in range(lax.axis_size(axis))])


def onward(x):
    n = lax.axis_size("sp")
    return lax.ppermute(x, "sp", [(i, i + 2) for i in range(n - 2)])


def body(tokens, query_weight, key_weight, value_weight, output_weight):
    half, depth = tokens.shape
    rows = 2 * half
    group = 2 * rows
    nq = rows // FAR_DILATION
    assert 2 * group == FAR_DILATION * REACH_STEPS
    heads = query_weight.shape[1] // HEAD // 2
    width = heads * HEAD
    flops = 2 * rows * depth * width
    sp, tp = lax.axis_index("sp"), lax.axis_index("tp")
    scalars = jnp.stack([tp, sp % 2, sp // 2, sp]).astype(jnp.int32)
    inverse = THETA_BASE ** (-jnp.arange(HEAD // 2, dtype=F32) / (HEAD // 2))
    inverse = jnp.concatenate([inverse, inverse])[None]
    group0, group1, near0, near1, pair2 = biases(nq)
    shape = jax.ShapeDtypeStruct
    kv = shape((heads, 2, half, HEAD), BF16)
    q_shape, q_half = shape((heads, rows, HEAD), BF16), shape((heads, half, HEAD), BF16)
    table = shape((2, half, HEAD), F32)
    buffers = pltpu.VMEM((4 * heads, half, HEAD), F32)

    partner = swap(tokens, "tp")
    weights = shape((2, depth, width), BF16)
    kv_a, own, w_keep, cosine, sine = call(
        own_keep_kernel, scalars, [tokens, key_weight, value_weight, inverse],
        [kv, shape((half, depth), BF16), weights, table, table],
        [buffers, pltpu.SemaphoreType.DMA((3,))], flops, hbm=(0, 1, 2))
    kv1_a = onward(kv_a)
    kv_b, = call(rest_keep_kernel, scalars, [partner, w_keep, cosine, sine], [kv], [buffers], flops)
    kv1_b = onward(kv_b)
    send_a, = call(functools.partial(send_kernel, part=0), scalars, [own, key_weight, value_weight, cosine, sine],
                   [kv], [buffers],
                   flops)
    kv_ya = swap(send_a, "sp")
    send_b, = call(functools.partial(send_kernel, part=1), scalars, [partner, key_weight, value_weight, cosine, sine],
                   [kv], [buffers],
                   flops)
    kv_yb = swap(send_b, "sp")
    back = shape((heads - RELAYED, 2, half, HEAD), BF16)
    q_a, q_b, q_send, back_own = call(
        q_kernel, scalars, [own, partner, cosine, sine, query_weight], [q_half, q_half, q_shape, back],
        [buffers], 2 * flops)
    q_y = swap(q_send, "sp")
    behind = jnp.stack([back_own.reshape(rows, HEAD), q_y[RELAYED]])
    n = lax.axis_size("sp")
    q_next = lax.ppermute(behind, "sp", [(i, i - 2) for i in range(2, n)])
    kv1_ya = onward(kv_ya)
    kv1_yb = onward(kv_yb)
    kv2_ab = onward(jnp.stack([kv1_a[0], kv1_b[0]]))
    kv2_y = onward(jnp.stack([kv1_ya[0], kv1_yb[0]]))
    packed = shape((rows + 3 * FAR_DILATION, HEAD), BF16)
    packing = [pltpu.VMEM((2, rows, HEAD), BF16), pltpu.VMEM((FAR_DILATION, HEAD), F32)]
    piece_own, piece_diag = call(
        functools.partial(foreign_kernel, head=1), scalars,
        [q_next, kv1_a, kv1_b, kv1_ya, kv1_yb, pair2], [packed, packed],
        [pltpu.VMEM((group, HEAD), BF16)] * 3 + [pltpu.VMEM((group, HEAD), F32)] * 2 + packing, 10 ** 9)
    n = lax.axis_size("sp")
    piece_diag = lax.ppermute(piece_diag, "sp", [(i, (i ^ 1) + 2) for i in range(n - 2)])
    piece_own = onward(piece_own)
    state = shape((heads, group, HEAD), F32)
    kv_scratch = [pltpu.VMEM((heads, group, HEAD), BF16)] * 2
    q, m, l, o = call(
        local_kernel, scalars, [q_a, q_b, q_y, kv_a, kv_b, kv_ya, kv_yb, group0, near0, near1],
        [shape((heads, group, HEAD), BF16), state, state, state],
        kv_scratch + [pltpu.VMEM((heads, 2 * group, 4 * HEAD), F32)], 3 * 10 ** 9)
    m, l, o, state_y = call(
        one_kernel, scalars, [q, m, l, o, kv1_a, kv1_b, kv1_ya, kv1_yb, group1, near1], [state, state, state, packed],
        kv_scratch + [pltpu.VMEM((heads, 2 * group, 2 * HEAD), F32), pltpu.VMEM((heads, group, HEAD), F32)]
        + packing, 10 ** 9, {2: 0, 3: 1, 4: 2})
    state_y = swap(state_y, "sp")
    mixed = shape((rows, HEAD), BF16)
    keep, send = call(
        functools.partial(two_kernel, head=0), scalars, [q, m, l, o, kv2_ab, kv2_y, pair2],
        [mixed, mixed], [pltpu.VMEM((group, HEAD), BF16)] * 2 + [pltpu.VMEM((group, HEAD), F32)] * 2
        + [pltpu.VMEM((2, rows, HEAD), F32)], 10 ** 9)
    keep_tp = swap(keep, "tp")
    from_y = swap(send, "sp")
    first = [keep, from_y, keep_tp, swap(from_y, "tp")]
    last, = call(functools.partial(final_kernel, head=1), scalars, [m, l, o, state_y, piece_own, piece_diag],
                 [shape((2, rows, HEAD), BF16)], [pltpu.VMEM((2, rows, HEAD), F32)], 10 ** 9)
    last_tp = swap(last, "tp")
    return out_project(scalars, first, [last, last_tp], output_weight)


def solution(mesh):
    in_specs = (
        P(("grp", "sp", "tp"), None),
        P(None, "tp"),
        P(None, "tp"),
        P(None, "tp"),
        P(None, "tp"),
    )
    out_specs = P(("grp", "sp"), "tp")

    return jax.shard_map(body, mesh=mesh, in_specs=in_specs, out_specs=out_specs, check_vma=False)
```

```python
import functools

import jax
import jax.numpy as jnp
import numpy as np
from jax import lax
from jax.experimental import pallas as pl
from jax.experimental.pallas import tpu as pltpu
from jax.sharding import PartitionSpec as P

HEAD = 128
REACH_STEPS = 128
MIDDLE_DILATION = 4
FAR_DILATION = 16
THETA_BASE = 500000.0
TILE = 16
RELAYED = 1
MASKED = -1e30
SCALE = HEAD ** -0.5 * 1.4426950408889634
F32 = jnp.float32
BF16 = jnp.bfloat16


def in_vmem(count):
    return [pl.BlockSpec(memory_space=pltpu.VMEM)] * count


def rotated(val, cos, sin):
    return val * cos + pltpu.roll(val, HEAD // 2, 1) * sin


def place(out_ref, lead, val, buf_ref, slot, first):
    nq_half = val.shape[0] // FAR_DILATION
    buf_ref[slot] = val
    for r in range(FAR_DILATION):
        piece = buf_ref[slot, pl.ds(r, nq_half, stride=FAR_DILATION), :]
        at = r * nq_half if first is None else pl.multiple_of((2 * r + first) * nq_half, TILE)
        out_ref[lead + (pl.ds(at, nq_half), slice(None))] = piece.astype(BF16)


def kv_part(x_ref, w_refs, out_ref, cos_ref, sin_ref, buf_ref, ready=None):
    slot = 0
    for which in (1, 0):
        if ready is not None:
            ready[which].wait()
        acc = jnp.dot(x_ref[...], w_refs[which][...], preferred_element_type=F32)
        for h in range(acc.shape[1] // HEAD):
            val = acc[:, h * HEAD:(h + 1) * HEAD]
            if which == 0:
                val = rotated(val, cos_ref[...], sin_ref[...])
            place(out_ref, (h, which), val, buf_ref, slot, None)
            slot += 1


def weight_copies(wk_hbm, wv_hbm, w_ref, side, sems):
    width = w_ref.shape[2]
    column = pl.multiple_of(side * width, width)
    return [pltpu.make_async_copy(hbm.at[:, pl.ds(column, width)], w_ref.at[which], sems.at[which])
            for which, hbm in enumerate((wk_hbm, wv_hbm))]


def own_keep_kernel(sc_ref, x_hbm, wk_hbm, wv_hbm, inv_ref,
                    out_ref, x_ref, w_ref, cos_ref, sin_ref, buf_ref, sems):
    tp, par, sp = sc_ref[0], sc_ref[1], sc_ref[3]
    half = x_ref.shape[0]
    x_copy = pltpu.make_async_copy(x_hbm, x_ref, sems.at[2])
    copies = weight_copies(wk_hbm, wv_hbm, w_ref, par, sems)
    x_copy.start()
    copies[1].start()
    copies[0].start()
    steps = half // FAR_DILATION
    lane = lax.broadcasted_iota(jnp.int32, (2 * steps, HEAD), 1)
    row = lax.broadcasted_iota(jnp.int32, (2 * steps, HEAD), 0)
    part = jnp.where(row < steps, tp, 1 - tp)
    position = sp * (2 * half) + part * half + (row % steps) * FAR_DILATION
    coarse = position.astype(F32) * inv_ref[...]
    fine = lax.broadcasted_iota(jnp.int32, (FAR_DILATION, HEAD), 0).astype(F32) * inv_ref[...]
    cos_c, sin_c = jnp.cos(coarse)[:, None, :], jnp.sin(coarse)[:, None, :]
    cos_f, sin_f = jnp.cos(fine)[None], jnp.sin(fine)[None]
    sign = jnp.where(lane[:1] < HEAD // 2, -1.0, 1.0)[None]
    cos_ref[...] = (cos_c * cos_f - sin_c * sin_f).reshape(2, half, HEAD)
    sin_ref[...] = ((sin_c * cos_f + cos_c * sin_f) * sign).reshape(2, half, HEAD)
    x_copy.wait()
    kv_part(x_ref, (w_ref.at[0], w_ref.at[1]), out_ref, cos_ref.at[0], sin_ref.at[0], buf_ref, copies)


def middle_kernel(sc_ref, xo_ref, xp_ref, wk_ref, wv_ref, w_ref, cos_ref, sin_ref, send_ref, keep_ref, buf_ref):
    send_kernel(sc_ref, xo_ref, wk_ref, wv_ref, cos_ref, sin_ref, send_ref, buf_ref, part=0)
    half = buf_ref.shape[0] // 2
    kv_part(xp_ref, (w_ref.at[0], w_ref.at[1]), keep_ref, cos_ref.at[1], sin_ref.at[1], buf_ref.at[half:])


def send_kernel(sc_ref, x_ref, wk_ref, wv_ref, cos_ref, sin_ref, out_ref, buf_ref, *, part):
    width = out_ref.shape[0] * HEAD
    column = pl.ds(pl.multiple_of((1 - sc_ref[1]) * width, width), width)
    kv_part(x_ref, (wk_ref.at[:, column], wv_ref.at[:, column]), out_ref, cos_ref.at[part], sin_ref.at[part], buf_ref)


def q_kernel(sc_ref, xo_ref, xp_ref, cos_ref, sin_ref, w_ref, keepa_ref, keepb_ref, send_ref,
             back_ref, buf_ref):
    tp, par = sc_ref[0], sc_ref[1]
    heads = send_ref.shape[0]
    width = heads * HEAD
    slot = 0
    for side in (1, 0):
        w = w_ref[:, pl.ds(pl.multiple_of((1 - par if side else par) * width, width), width)]
        for part, x_ref in enumerate((xo_ref, xp_ref)):
            acc = jnp.dot(x_ref[...], w, preferred_element_type=F32)
            for h in range(heads):
                val = rotated(acc[:, h * HEAD:(h + 1) * HEAD], cos_ref[part], sin_ref[part])
                if side:
                    place(send_ref, (h,), val, buf_ref, slot, tp if part == 0 else 1 - tp)
                else:
                    place((keepa_ref, keepb_ref)[part], (h,), val, buf_ref, slot, None)
                if h >= RELAYED and not side:
                    place(back_ref, (h - RELAYED, part), val, buf_ref, slot, None)
                slot += 1


def call(kernel, scalars, inputs, outputs, scratch, flops, aliases={}, limit=28, hbm=()):
    spaces = [pltpu.HBM if i in hbm else pltpu.VMEM for i in range(len(inputs))]
    return pl.pallas_call(
        kernel,
        in_specs=[pl.BlockSpec(memory_space=pltpu.SMEM)] + [pl.BlockSpec(memory_space=m) for m in spaces],
        out_specs=in_vmem(len(outputs)),
        out_shape=outputs,
        scratch_shapes=scratch,
        input_output_aliases=aliases,
        compiler_params=pltpu.CompilerParams(vmem_limit_bytes=limit * 2 ** 20),
        cost_estimate=pl.CostEstimate(flops=flops, transcendentals=0, bytes_accessed=0),
    )(scalars, *[pltpu.with_memory_space_constraint(x, pltpu.HBM) if i in hbm else x for i, x in enumerate(inputs)])


def gather(dst_ref, nq, sources):
    for r in range(FAR_DILATION):
        for source, block, half in sources:
            rows = nq if half is None else nq // 2
            start = 0 if half is None else half * (nq // 2)
            at = pl.multiple_of(r * 2 * nq + block * nq + start, TILE)
            dst_ref[pl.ds(at, rows), :] = source[r * rows:(r + 1) * rows, :]


def gather_kv(k_ref, v_ref, refs, nq, tp, par):
    places = ((par, tp), (par, 1 - tp), (1 - par, tp), (1 - par, 1 - tp))
    for which, dst_ref in enumerate((k_ref, v_ref)):
        gather(dst_ref, nq, [(ref.at[which], block, half) for ref, (block, half) in zip(refs, places)])


def scores_of(q, k):
    return lax.dot_general(q, k, (((1,), (1,)), ((), ())), preferred_element_type=F32)


def take(ref, rows):
    parts = [ref[a:a + n, :] for a, n in rows]
    return parts[0] if len(parts) == 1 else jnp.concatenate(parts, axis=0)


def put(ref, rows, value):
    at = 0
    for a, n in rows:
        ref[a:a + n, :] = value[at:at + n]
        at += n


def widened(stat, columns):
    return jnp.concatenate([stat] * (columns // HEAD), axis=1) if columns > HEAD else stat


def scored(item, q_ref, k_ref, s_ref, m_ref, fresh):
    rows, keys, bias, at = item
    if rows[0][1] < TILE:
        s = scores_of(take(q_ref, [(a, TILE) for a, _ in rows]), take(k_ref, keys))
        s = s.reshape(len(rows), TILE, s.shape[1])[:, :rows[0][1]].reshape(length(rows), s.shape[1])
    else:
        s = scores_of(take(q_ref, rows), take(k_ref, keys))
    if bias is not None:
        s = s + bias
    n, columns = s.shape
    s_ref[at:at + n, :columns] = s
    top = jnp.broadcast_to(jnp.max(s, axis=-1, keepdims=True), (n, HEAD))
    put(m_ref, rows, top if fresh else jnp.maximum(take(m_ref, rows), top))


def weighed(item, v_ref, s_ref, m_ref, columns):
    rows, keys, _, at = item
    n = sum(c for _, c in rows)
    p = jnp.exp2((s_ref[at:at + n, :columns] - widened(take(m_ref, rows), columns)) * SCALE).astype(BF16)
    v = take(v_ref, keys)
    return jnp.dot(p, jnp.concatenate([v, jnp.ones_like(v)], axis=1), preferred_element_type=F32)


def length(rows):
    return sum(n for _, n in rows)


def group_rows(r4, nq):
    return [((r4 + MIDDLE_DILATION * j) * 2 * nq, 2 * nq) for j in range(FAR_DILATION // MIDDLE_DILATION)]


def near_rows(c, nq):
    return [(r * 2 * nq + c * TILE, TILE) for r in range(FAR_DILATION)]


def upper_rows(c, nq):
    return [(a, REACH_STEPS // FAR_DILATION) for a, _ in near_rows(c, nq)]


def pair_rows(i, nq):
    return [(i * 4 * nq, 4 * nq)]


def near_of(tq, tk):
    return (tq - tk >= 0) & (tq - tk <= REACH_STEPS)


def every(tq, tk, step):
    return (tq % step == tk % step) & (tq - tk >= 0) & (tq - tk <= REACH_STEPS * step)


def bias_of(count):
    return np.where(count > 0, np.log2(np.maximum(count, 1)) / SCALE, MASKED).astype(np.float32)


def biases(nq):
    group = 2 * nq * FAR_DILATION
    j = np.arange(FAR_DILATION // MIDDLE_DILATION)[:, None]
    t = (np.arange(2 * nq)[None, :] * FAR_DILATION + j * MIDDLE_DILATION).reshape(-1)
    tq, tk = t[:, None], t[None, :]
    both = lambda tq, tk: every(tq, tk, MIDDLE_DILATION).astype(int) + every(tq, tk, FAR_DILATION)
    group0, group1 = both(tq, tk), both(tq + group, tk)
    r = np.arange(FAR_DILATION)[:, None]
    t = (np.arange(TILE)[None, :] * FAR_DILATION + r).reshape(-1)
    tq, tk = t[:, None], t[None, :]
    near0, near1 = near_of(tq, tk), near_of(tq + TILE * FAR_DILATION, tk)
    upper = near1.reshape(FAR_DILATION, TILE, -1)[:, :REACH_STEPS // FAR_DILATION].reshape(-1, near1.shape[1])
    r = np.arange(2)[:, None]
    t = (np.arange(2 * nq)[None, :] * FAR_DILATION + r).reshape(-1)
    pair2 = every(t[:, None] + 2 * group, t[None, :], FAR_DILATION)
    return [bias_of(np.asarray(x, int)) for x in (group0, group1, near0, near1, upper, pair2)]


def local_kernel(sc_ref, qa_ref, qb_ref, qy_ref, kva_ref, kvb_ref, kvya_ref, kvyb_ref, group_ref, near0_ref, near1_ref,
                 q_ref, m_ref, l_ref, o_ref, k_s, v_s, s_s):
    tp, par = sc_ref[0], sc_ref[1]
    nq = qy_ref.shape[1] // FAR_DILATION
    for h in range(q_ref.shape[0]):
        q, m, l, o, k, v, sh = (x.at[h] for x in (q_ref, m_ref, l_ref, o_ref, k_s, v_s, s_s))
        gather(q, nq, [(qa_ref.at[h], par, tp), (qb_ref.at[h], par, 1 - tp), (qy_ref.at[h], 1 - par, None)])
        gather_kv(k, v, [x.at[h] for x in (kva_ref, kvb_ref, kvya_ref, kvyb_ref)], nq, tp, par)
        at = 0
        items = []
        for r4 in range(MIDDLE_DILATION):
            rows = group_rows(r4, nq)
            items.append((rows, rows, group_ref[...], at))
            scored(items[-1], q, k, sh, m, True)
            at += length(rows)
        for c in range(2 * nq // TILE):
            rows = near_rows(c, nq)
            items.append((rows, rows, near0_ref[...], at))
            scored(items[-1], q, k, sh, m, False)
            at += length(rows)
            if c:
                items.append((upper_rows(c, nq), near_rows(c - 1, nq), near1_ref[...], at))
                scored(items[-1], q, k, sh, m, False)
                at += length(items[-1][0])
        for i, item in enumerate(items):
            ol = weighed(item, v, sh, m, length(item[1]))
            if i < MIDDLE_DILATION:
                put(o, item[0], ol[:, :HEAD])
                put(l, item[0], ol[:, HEAD:])
            else:
                put(o, item[0], take(o, item[0]) + ol[:, :HEAD])
                put(l, item[0], take(l, item[0]) + ol[:, HEAD:])


def one_kernel(sc_ref, q_ref, m_in, l_in, o_in, kva_ref, kvb_ref, kvya_ref, kvyb_ref, group_ref, near_ref,
               m_ref, l_ref, o_ref, state_ref, k_s, v_s, s_s, n_s, piece_s, stat_s):
    tp, par = sc_ref[0], sc_ref[1]
    nq = kvya_ref.shape[2] // FAR_DILATION * 2

    @pl.when(sc_ref[2] >= 1)
    def _():
        for h in range(q_ref.shape[0]):
            q, mi, li, oi, m, l, o, k, v, sh, n = (x.at[h] for x in (
                q_ref, m_in, l_in, o_in, m_ref, l_ref, o_ref, k_s, v_s, s_s, n_s))
            gather_kv(k, v, [x.at[h] for x in (kva_ref, kvb_ref, kvya_ref, kvyb_ref)], nq, tp, par)
            near = (near_rows(0, nq), near_rows(2 * nq // TILE - 1, nq), near_ref[...], 0)
            at = length(near[0])
            items = []
            for r4 in range(MIDDLE_DILATION):
                rows = group_rows(r4, nq)
                items.append((rows, rows, group_ref[...], at))
                scored(items[-1], q, k, sh, n, True)
                at += length(rows)
            scored(near, q, k, sh, n, False)
            for item in items:
                rows = item[0]
                old = take(mi, rows)
                new = jnp.maximum(old, take(n, rows))
                keep = jnp.exp2((old - new) * SCALE)
                put(m, rows, new)
                ol = weighed(item, v, sh, m, length(item[1]))
                put(o, rows, take(oi, rows) * keep + ol[:, :HEAD])
                put(l, rows, take(li, rows) * keep + ol[:, HEAD:])
            ol = weighed(near, v, sh, m, length(near[1]))
            put(o, near[0], take(o, near[0]) + ol[:, :HEAD])
            put(l, near[0], take(l, near[0]) + ol[:, HEAD:])

    for i in range(FAR_DILATION // 2):
        rows = pair_rows(i, nq)
        m, l, o = (take(x.at[RELAYED], rows) for x in (m_ref, l_ref, o_ref))
        pack_rows(piece_s, stat_s, i, o / l, m, l)
    pack_out(state_ref, piece_s, stat_s, 1 - par)


def two_kernel(sc_ref, q_ref, m_ref, l_ref, o_ref, kvo_ref, kvy_ref, pair_ref,
               keep_ref, send_ref, k_s, v_s, s_s, n_s, mix_s, *, head):
    tp, par = sc_ref[0], sc_ref[1]
    nq = kvy_ref.shape[2] // FAR_DILATION * 2
    q, m, l, o = (x.at[head] for x in (q_ref, m_ref, l_ref, o_ref))
    pairs = [pair_rows(i, nq) for i in range(FAR_DILATION // 2)]

    def settle(i, val):
        for part in range(4):
            r, block = 2 * i + part // 2, part % 2
            mix_s[block, pl.ds(r, nq, stride=FAR_DILATION), :] = val[part * nq:(part + 1) * nq]

    @pl.when(sc_ref[2] >= 2)
    def _():
        gather_kv(k_s, v_s, [kvo_ref.at[0], kvo_ref.at[1], kvy_ref.at[0], kvy_ref.at[1]], nq, tp, par)
        items = [(rows, rows, pair_ref[...], i * length(rows)) for i, rows in enumerate(pairs)]
        for item in items:
            put(n_s, item[0], take(m, item[0]))
            scored(item, q, k_s, s_s, n_s, False)
        for i, item in enumerate(items):
            rows = item[0]
            ol = weighed(item, v_s, s_s, n_s, length(rows))
            keep = jnp.exp2((take(m, rows) - take(n_s, rows)) * SCALE)
            settle(i, (take(o, rows) * keep + ol[:, :HEAD]) / (take(l, rows) * keep + ol[:, HEAD:]))

    @pl.when(sc_ref[2] < 2)
    def _():
        for i, rows in enumerate(pairs):
            settle(i, take(o, rows) / take(l, rows))

    keep_ref[...] = mix_s[pl.ds(par, 1)][0].astype(BF16)
    send_ref[...] = mix_s[pl.ds(1 - par, 1)][0].astype(BF16)


def diagonal(n):
    return lax.broadcasted_iota(jnp.int32, (n, n), 0) == lax.broadcasted_iota(jnp.int32, (n, n), 1)


def pack_rows(piece_s, stat_s, i, value, top, total):
    nq = value.shape[0] // 4
    eye = diagonal(HEAD)
    for part in range(4):
        r, block = 2 * i + part // 2, part % 2
        piece_s[block, r * nq:(r + 1) * nq, :] = value[part * nq:(part + 1) * nq].astype(BF16)
    for which, stat in enumerate((top, total)):
        at = which * (FAR_DILATION // 2) + i
        stat_s[at:at + 1, :] = jnp.sum(jnp.where(eye, stat, 0.0), axis=0, keepdims=True)


def pack_out(out_ref, piece_s, stat_s, block):
    rows, count = piece_s.shape[1], stat_s.shape[0]
    out_ref[:rows, :] = piece_s[pl.ds(block, 1)][0]
    rest = stat_s[...]
    for term in range(3):
        low = rest.astype(BF16)
        out_ref[rows + term * count:rows + (term + 1) * count, :] = low
        rest = rest - low.astype(F32)


def unpacked_stats(ref, rows):
    return sum(ref[rows + t * FAR_DILATION:rows + (t + 1) * FAR_DILATION, :].astype(F32) for t in range(3))


def foreign_kernel(sc_ref, qn_ref, kva_ref, kvb_ref, kvya_ref, kvyb_ref, pair_ref,
                   own_ref, diag_ref, q_s, k_s, v_s, s_s, n_s, piece_s, stat_s, *, head):
    tp, par = sc_ref[0], sc_ref[1]
    nq = kvya_ref.shape[2] // FAR_DILATION * 2
    half = kvya_ref.shape[2]
    gather(q_s, nq, [(qn_ref.at[0, :half], par, tp), (qn_ref.at[0, half:], par, 1 - tp), (qn_ref.at[1], 1 - par, None)])
    gather_kv(k_s, v_s, [x.at[head] for x in (kva_ref, kvb_ref, kvya_ref, kvyb_ref)], nq, tp, par)
    pairs = [pair_rows(i, nq) for i in range(FAR_DILATION // 2)]
    items = [(rows, rows, pair_ref[...], i * length(rows)) for i, rows in enumerate(pairs)]
    for item in items:
        scored(item, q_s, k_s, s_s, n_s, True)
    for i, item in enumerate(items):
        ol = weighed(item, v_s, s_s, n_s, length(item[0]))
        total = ol[:, HEAD:]
        pack_rows(piece_s, stat_s, i, ol[:, :HEAD] / total, take(n_s, item[0]), total)
    pack_out(own_ref, piece_s, stat_s, par)
    pack_out(diag_ref, piece_s, stat_s, 1 - par)


def final_kernel(sc_ref, m_ref, l_ref, o_ref, state_ref, own_ref, diag_ref, out_ref, mix_s, *, head):
    par = sc_ref[1]
    m, l, o = (x.at[head] for x in (m_ref, l_ref, o_ref))
    rows = out_ref.shape[1]
    nq = rows // FAR_DILATION
    count = FAR_DILATION // 2
    far = sc_ref[2] >= 2
    eye = diagonal(HEAD)

    def columns(ref):
        stats = unpacked_stats(ref, rows)
        result = []
        for i in range(2 * count):
            spread = jnp.sum(jnp.where(eye, stats[i:i + 1, :], 0.0), axis=1, keepdims=True)
            result.append(jnp.broadcast_to(spread, (HEAD, HEAD)))
        return result

    def rows_of(result, which, r):
        column = result[which * count + r // 2]
        at = (r % 2) * 2 * nq
        return jnp.where(par == 0, column[at:at + nq], column[at + nq:at + 2 * nq])

    def joined(top, total, numerator, ref, result, r):
        top2, total2 = rows_of(result, 0, r), rows_of(result, 1, r)
        top2 = jnp.where(far, top2, MASKED)
        new = jnp.maximum(top, top2)
        keep = jnp.exp2((top - new) * SCALE)
        add = jnp.where(far, jnp.exp2((top2 - new) * SCALE) * total2, 0.0)
        part = jnp.where(far, ref[r * nq:(r + 1) * nq, :].astype(F32), 0.0)
        return (numerator * keep + part * add) / (total * keep + add)

    own_stats, diag_stats, state_stats = columns(own_ref), columns(diag_ref), columns(state_ref)
    for r in range(FAR_DILATION):
        here = pl.ds(pl.multiple_of(r * 2 * nq + par * nq, TILE), nq)
        mix_s[0, pl.ds(r, nq, stride=FAR_DILATION), :] = joined(
            m[here, :], l[here, :], o[here, :], own_ref, own_stats, r)
        top, total = rows_of(state_stats, 0, r), rows_of(state_stats, 1, r)
        mix_s[1, pl.ds(r, nq, stride=FAR_DILATION), :] = joined(
            top, total, state_ref[r * nq:(r + 1) * nq, :].astype(F32) * total, diag_ref, diag_stats, r)
    out_ref[...] = mix_s[...].astype(BF16)


def out_kernel(sc_ref, a_ref, b_ref, c_ref, d_ref, own_ref, tp_ref, w_ref, o_ref):
    tp, par = sc_ref[0], sc_ref[1]
    block = o_ref.shape[1]
    heads = w_ref.shape[0] // HEAD // 4
    column = pl.multiple_of(pl.program_id(0) * block, block)
    order = (2 * tp + par, 2 * tp + 1 - par, 2 * (1 - tp) + par, 2 * (1 - tp) + 1 - par)
    x_refs = (own_ref.at[0], own_ref.at[1], tp_ref.at[0], tp_ref.at[1], a_ref, b_ref, c_ref, d_ref)
    x = jnp.concatenate([x_ref[...] for x_ref in x_refs], axis=1)
    w = jnp.concatenate([w_ref[pl.ds(pl.multiple_of((i * heads + head) * HEAD, HEAD), HEAD), pl.ds(column, block)]
                         for head in (1, 0) for i in order], axis=0)
    o_ref[...] = jnp.dot(x, w, preferred_element_type=F32).astype(BF16)


def out_project(scalars, first, last, weight):
    rows, columns = first[0].shape[0], weight.shape[1]
    steps = 2
    return pl.pallas_call(
        out_kernel,
        grid=(steps,),
        in_specs=[pl.BlockSpec(memory_space=pltpu.SMEM)] + in_vmem(7),
        out_specs=pl.BlockSpec((rows, columns // steps), lambda j: (0, j)),
        out_shape=jax.ShapeDtypeStruct((rows, columns), BF16),
        compiler_params=pltpu.CompilerParams(vmem_limit_bytes=16 * 2 ** 20),
        cost_estimate=pl.CostEstimate(flops=2 * rows * weight.size, transcendentals=0, bytes_accessed=0),
        name="out_project",
    )(scalars, *first, *last, weight)


def swap(x, axis):
    return lax.ppermute(x, axis, [(i, i ^ 1) for i in range(lax.axis_size(axis))])


def onward(x):
    n = lax.axis_size("sp")
    return lax.ppermute(x, "sp", [(i, i + 2) for i in range(n - 2)])


def body(tokens, query_weight, key_weight, value_weight, output_weight):
    half, depth = tokens.shape
    rows = 2 * half
    group = 2 * rows
    nq = rows // FAR_DILATION
    assert 2 * group == FAR_DILATION * REACH_STEPS
    heads = query_weight.shape[1] // HEAD // 2
    width = heads * HEAD
    flops = 2 * rows * depth * width
    sp, tp = lax.axis_index("sp"), lax.axis_index("tp")
    scalars = jnp.stack([tp, sp % 2, sp // 2, sp]).astype(jnp.int32)
    inverse = THETA_BASE ** (-jnp.arange(HEAD // 2, dtype=F32) / (HEAD // 2))
    inverse = jnp.concatenate([inverse, inverse])[None]
    group0, group1, near0, near1, upper, pair2 = biases(nq)
    shape = jax.ShapeDtypeStruct
    kv = shape((heads, 2, half, HEAD), BF16)
    q_shape, q_half = shape((heads, rows, HEAD), BF16), shape((heads, half, HEAD), BF16)
    table = shape((2, half, HEAD), F32)
    buffers = pltpu.VMEM((4 * heads, half, HEAD), F32)

    partner = swap(tokens, "tp")
    weights = shape((2, depth, width), BF16)
    kv_a, own, w_keep, cosine, sine = call(
        own_keep_kernel, scalars, [tokens, key_weight, value_weight, inverse],
        [kv, shape((half, depth), BF16), weights, table, table],
        [buffers, pltpu.SemaphoreType.DMA((3,))], flops, hbm=(0, 1, 2))
    kv1_a = onward(kv_a)
    key_weight, value_weight, own = lax.optimization_barrier((key_weight, value_weight, own))
    send_a, kv_b = call(
        middle_kernel, scalars, [own, partner, key_weight, value_weight, w_keep, cosine, sine], [kv, kv], [buffers],
        2 * flops)
    kv1_b = onward(kv_b)
    kv_ya = swap(send_a, "sp")
    send_b, = call(functools.partial(send_kernel, part=1), scalars, [partner, key_weight, value_weight, cosine, sine],
                   [kv], [buffers],
                   flops)
    kv_yb = swap(send_b, "sp")
    back = shape((heads - RELAYED, 2, half, HEAD), BF16)
    q_a, q_b, q_send, back_own = call(
        q_kernel, scalars, [own, partner, cosine, sine, query_weight], [q_half, q_half, q_shape, back],
        [buffers], 2 * flops)
    q_y = swap(q_send, "sp")
    behind = jnp.stack([back_own.reshape(rows, HEAD), q_y[RELAYED]])
    n = lax.axis_size("sp")
    q_next = lax.ppermute(behind, "sp", [(i, i - 2) for i in range(2, n)])
    kv1_ya = onward(kv_ya)
    kv1_yb = onward(kv_yb)
    kv2_ab = onward(jnp.stack([kv1_a[0], kv1_b[0]]))
    kv2_y = onward(jnp.stack([kv1_ya[0], kv1_yb[0]]))
    packed = shape((rows + 3 * FAR_DILATION, HEAD), BF16)
    packing = [pltpu.VMEM((2, rows, HEAD), BF16), pltpu.VMEM((FAR_DILATION, HEAD), F32)]
    piece_own, piece_diag = call(
        functools.partial(foreign_kernel, head=1), scalars,
        [q_next, kv1_a, kv1_b, kv1_ya, kv1_yb, pair2], [packed, packed],
        [pltpu.VMEM((group, HEAD), BF16)] * 3 + [pltpu.VMEM((group, HEAD), F32)] * 2 + packing, 10 ** 9)
    n = lax.axis_size("sp")
    piece_diag = lax.ppermute(piece_diag, "sp", [(i, (i ^ 1) + 2) for i in range(n - 2)])
    piece_own = onward(piece_own)
    state = shape((heads, group, HEAD), F32)
    kv_scratch = [pltpu.VMEM((heads, group, HEAD), BF16)] * 2
    q, m, l, o = call(
        local_kernel, scalars, [q_a, q_b, q_y, kv_a, kv_b, kv_ya, kv_yb, group0, near0, upper],
        [shape((heads, group, HEAD), BF16), state, state, state],
        kv_scratch + [pltpu.VMEM((heads, 3 * group, 2 * HEAD), F32)], 3 * 10 ** 9)
    m, l, o, state_y = call(
        one_kernel, scalars, [q, m, l, o, kv1_a, kv1_b, kv1_ya, kv1_yb, group1, near1], [state, state, state, packed],
        kv_scratch + [pltpu.VMEM((heads, 2 * group, 2 * HEAD), F32), pltpu.VMEM((heads, group, HEAD), F32)]
        + packing, 10 ** 9, {2: 0, 3: 1, 4: 2})
    state_y = swap(state_y, "sp")
    mixed = shape((rows, HEAD), BF16)
    keep, send = call(
        functools.partial(two_kernel, head=0), scalars, [q, m, l, o, kv2_ab, kv2_y, pair2],
        [mixed, mixed], [pltpu.VMEM((group, HEAD), BF16)] * 2 + [pltpu.VMEM((group, HEAD), F32)] * 2
        + [pltpu.VMEM((2, rows, HEAD), F32)], 10 ** 9)
    keep_tp = swap(keep, "tp")
    from_y = swap(send, "sp")
    first = [keep, from_y, keep_tp, swap(from_y, "tp")]
    last, = call(functools.partial(final_kernel, head=1), scalars, [m, l, o, state_y, piece_own, piece_diag],
                 [shape((2, rows, HEAD), BF16)], [pltpu.VMEM((2, rows, HEAD), F32)], 10 ** 9)
    last_tp = swap(last, "tp")
    return out_project(scalars, first, [last, last_tp], output_weight)


def solution(mesh):
    in_specs = (
        P(("grp", "sp", "tp"), None),
        P(None, "tp"),
        P(None, "tp"),
        P(None, "tp"),
        P(None, "tp"),
    )
    out_specs = P(("grp", "sp"), "tp")

    return jax.shard_map(body, mesh=mesh, in_specs=in_specs, out_specs=out_specs, check_vma=False)
```

```python
import functools

import jax
import jax.numpy as jnp
import numpy as np
from jax import lax
from jax.experimental import pallas as pl
from jax.experimental.pallas import tpu as pltpu
from jax.sharding import PartitionSpec as P

HEAD = 128
REACH_STEPS = 128
MIDDLE_DILATION = 4
FAR_DILATION = 16
THETA_BASE = 500000.0
TILE = 16
RELAYED = 1
MASKED = -1e30
SCALE = HEAD ** -0.5 * 1.4426950408889634
F32 = jnp.float32
BF16 = jnp.bfloat16


def in_vmem(count):
    return [pl.BlockSpec(memory_space=pltpu.VMEM)] * count


def rotated(val, cos, sin):
    return val * cos + pltpu.roll(val, HEAD // 2, 1) * sin


def place(out_ref, lead, val, buf_ref, slot, first):
    nq_half = val.shape[0] // FAR_DILATION
    buf_ref[slot] = val
    for r in range(FAR_DILATION):
        piece = buf_ref[slot, pl.ds(r, nq_half, stride=FAR_DILATION), :]
        at = r * nq_half if first is None else pl.multiple_of((2 * r + first) * nq_half, TILE)
        out_ref[lead + (pl.ds(at, nq_half), slice(None))] = piece.astype(BF16)


def kv_finish(acc, which, out_ref, cos_ref, sin_ref, buf_ref):
    heads = acc.shape[1] // HEAD
    for h in range(heads):
        val = acc[:, h * HEAD:(h + 1) * HEAD]
        if which == 0:
            val = rotated(val, cos_ref[...], sin_ref[...])
        place(out_ref, (h, which), val, buf_ref, (1 - which) * heads + h, None)


def kv_part(x_ref, w_refs, out_ref, cos_ref, sin_ref, buf_ref):
    for which in (1, 0):
        acc = jnp.dot(x_ref[...], w_refs[which][...], preferred_element_type=F32)
        kv_finish(acc, which, out_ref, cos_ref, sin_ref, buf_ref)


def own_keep_kernel(sc_ref, x_hbm, wk_hbm, wv_hbm, inv_ref,
                    out_ref, x_ref, w_ref, cos_ref, sin_ref, buf_ref, acc_ref, sems):
    tp, par, sp = sc_ref[0], sc_ref[1], sc_ref[3]
    half = x_ref.shape[0]
    depth, width = w_ref.shape[1:]
    column = pl.ds(pl.multiple_of(par * width, width), width)
    cuts = [pl.ds(i * depth // 2, depth // 2) for i in range(2)]
    copies = []
    for i, cut in enumerate(cuts):
        copies.append([
            pltpu.make_async_copy(wk_hbm.at[cut, column], w_ref.at[0, cut], sems.at[i, 0]),
            pltpu.make_async_copy(wv_hbm.at[cut, column], w_ref.at[1, cut], sems.at[i, 1]),
            pltpu.make_async_copy(x_hbm.at[:, cut], x_ref.at[:, cut], sems.at[i, 2])])
    for part in copies:
        for i in (2, 1, 0):
            part[i].start()
    steps = half // FAR_DILATION
    lane = lax.broadcasted_iota(jnp.int32, (2 * steps, HEAD), 1)
    row = lax.broadcasted_iota(jnp.int32, (2 * steps, HEAD), 0)
    part = jnp.where(row < steps, tp, 1 - tp)
    position = sp * (2 * half) + part * half + (row % steps) * FAR_DILATION
    coarse = position.astype(F32) * inv_ref[...]
    fine = lax.broadcasted_iota(jnp.int32, (FAR_DILATION, HEAD), 0).astype(F32) * inv_ref[...]
    cos_c, sin_c = jnp.cos(coarse)[:, None, :], jnp.sin(coarse)[:, None, :]
    cos_f, sin_f = jnp.cos(fine)[None], jnp.sin(fine)[None]
    sign = jnp.where(lane[:1] < HEAD // 2, -1.0, 1.0)[None]
    cos_ref[...] = (cos_c * cos_f - sin_c * sin_f).reshape(2, half, HEAD)
    sin_ref[...] = ((sin_c * cos_f + cos_c * sin_f) * sign).reshape(2, half, HEAD)
    for i, cut in enumerate(cuts):
        copies[i][2].wait()
        for which in (1, 0):
            copies[i][which].wait()
            acc = jnp.dot(x_ref[:, cut], w_ref[which, cut], preferred_element_type=F32)
            if i == 0:
                acc_ref[which] = acc
            else:
                kv_finish(acc_ref[which] + acc, which, out_ref, cos_ref.at[0], sin_ref.at[0], buf_ref)


def middle_kernel(sc_ref, xo_ref, xp_ref, wk_ref, wv_ref, w_ref, cos_ref, sin_ref, send_ref, keep_ref, buf_ref):
    send_kernel(sc_ref, xo_ref, wk_ref, wv_ref, cos_ref, sin_ref, send_ref, buf_ref, part=0)
    half = buf_ref.shape[0] // 2
    kv_part(xp_ref, (w_ref.at[0], w_ref.at[1]), keep_ref, cos_ref.at[1], sin_ref.at[1], buf_ref.at[half:])


def send_kernel(sc_ref, x_ref, wk_ref, wv_ref, cos_ref, sin_ref, out_ref, buf_ref, *, part):
    width = out_ref.shape[0] * HEAD
    column = pl.ds(pl.multiple_of((1 - sc_ref[1]) * width, width), width)
    kv_part(x_ref, (wk_ref.at[:, column], wv_ref.at[:, column]), out_ref, cos_ref.at[part], sin_ref.at[part], buf_ref)


def q_kernel(sc_ref, xo_ref, xp_ref, cos_ref, sin_ref, w_ref, keepa_ref, keepb_ref, send_ref,
             back_ref, buf_ref):
    tp, par = sc_ref[0], sc_ref[1]
    heads = send_ref.shape[0]
    width = heads * HEAD
    slot = 0
    for side in (1, 0):
        w = w_ref[:, pl.ds(pl.multiple_of((1 - par if side else par) * width, width), width)]
        for part, x_ref in enumerate((xo_ref, xp_ref)):
            acc = jnp.dot(x_ref[...], w, preferred_element_type=F32)
            for h in range(heads):
                val = rotated(acc[:, h * HEAD:(h + 1) * HEAD], cos_ref[part], sin_ref[part])
                if side:
                    place(send_ref, (h,), val, buf_ref, slot, tp if part == 0 else 1 - tp)
                else:
                    place((keepa_ref, keepb_ref)[part], (h,), val, buf_ref, slot, None)
                if h >= RELAYED and not side:
                    place(back_ref, (h - RELAYED, part), val, buf_ref, slot, None)
                slot += 1


def call(kernel, scalars, inputs, outputs, scratch, flops, aliases={}, limit=28, hbm=()):
    spaces = [pltpu.HBM if i in hbm else pltpu.VMEM for i in range(len(inputs))]
    return pl.pallas_call(
        kernel,
        in_specs=[pl.BlockSpec(memory_space=pltpu.SMEM)] + [pl.BlockSpec(memory_space=m) for m in spaces],
        out_specs=in_vmem(len(outputs)),
        out_shape=outputs,
        scratch_shapes=scratch,
        input_output_aliases=aliases,
        compiler_params=pltpu.CompilerParams(vmem_limit_bytes=limit * 2 ** 20),
        cost_estimate=pl.CostEstimate(flops=flops, transcendentals=0, bytes_accessed=0),
    )(scalars, *[pltpu.with_memory_space_constraint(x, pltpu.HBM) if i in hbm else x for i, x in enumerate(inputs)])


def gather(dst_ref, nq, sources):
    for r in range(FAR_DILATION):
        for source, block, half in sources:
            rows = nq if half is None else nq // 2
            start = 0 if half is None else half * (nq // 2)
            at = pl.multiple_of(r * 2 * nq + block * nq + start, TILE)
            dst_ref[pl.ds(at, rows), :] = source[r * rows:(r + 1) * rows, :]


def gather_kv(k_ref, v_ref, refs, nq, tp, par):
    places = ((par, tp), (par, 1 - tp), (1 - par, tp), (1 - par, 1 - tp))
    for which, dst_ref in enumerate((k_ref, v_ref)):
        gather(dst_ref, nq, [(ref.at[which], block, half) for ref, (block, half) in zip(refs, places)])


def scores_of(q, k):
    return lax.dot_general(q, k, (((1,), (1,)), ((), ())), preferred_element_type=F32)


def take(ref, rows):
    parts = [ref[a:a + n, :] for a, n in rows]
    return parts[0] if len(parts) == 1 else jnp.concatenate(parts, axis=0)


def put(ref, rows, value):
    at = 0
    for a, n in rows:
        ref[a:a + n, :] = value[at:at + n]
        at += n


def widened(stat, columns):
    return jnp.concatenate([stat] * (columns // HEAD), axis=1) if columns > HEAD else stat


def scored(item, q_ref, k_ref, s_ref, m_ref, fresh):
    rows, keys, bias, at = item
    if rows[0][1] < TILE:
        s = scores_of(take(q_ref, [(a, TILE) for a, _ in rows]), take(k_ref, keys))
        s = s.reshape(len(rows), TILE, s.shape[1])[:, :rows[0][1]].reshape(length(rows), s.shape[1])
    else:
        s = scores_of(take(q_ref, rows), take(k_ref, keys))
    if bias is not None:
        s = s + bias
    n, columns = s.shape
    s_ref[at:at + n, :columns] = s
    top = jnp.broadcast_to(jnp.max(s, axis=-1, keepdims=True), (n, HEAD))
    put(m_ref, rows, top if fresh else jnp.maximum(take(m_ref, rows), top))


def weighed(item, v_ref, s_ref, m_ref, columns):
    rows, keys, _, at = item
    n = sum(c for _, c in rows)
    p = jnp.exp2((s_ref[at:at + n, :columns] - widened(take(m_ref, rows), columns)) * SCALE).astype(BF16)
    v = take(v_ref, keys)
    return jnp.dot(p, jnp.concatenate([v, jnp.ones_like(v)], axis=1), preferred_element_type=F32)


def length(rows):
    return sum(n for _, n in rows)


def group_rows(r4, nq):
    return [((r4 + MIDDLE_DILATION * j) * 2 * nq, 2 * nq) for j in range(FAR_DILATION // MIDDLE_DILATION)]


def near_rows(c, nq):
    return [(r * 2 * nq + c * TILE, TILE) for r in range(FAR_DILATION)]


def upper_rows(c, nq):
    return [(a, REACH_STEPS // FAR_DILATION) for a, _ in near_rows(c, nq)]


def pair_rows(i, nq):
    return [(i * 4 * nq, 4 * nq)]


def near_of(tq, tk):
    return (tq - tk >= 0) & (tq - tk <= REACH_STEPS)


def every(tq, tk, step):
    return (tq % step == tk % step) & (tq - tk >= 0) & (tq - tk <= REACH_STEPS * step)


def bias_of(count):
    return np.where(count > 0, np.log2(np.maximum(count, 1)) / SCALE, MASKED).astype(np.float32)


def biases(nq):
    group = 2 * nq * FAR_DILATION
    j = np.arange(FAR_DILATION // MIDDLE_DILATION)[:, None]
    t = (np.arange(2 * nq)[None, :] * FAR_DILATION + j * MIDDLE_DILATION).reshape(-1)
    tq, tk = t[:, None], t[None, :]
    both = lambda tq, tk: every(tq, tk, MIDDLE_DILATION).astype(int) + every(tq, tk, FAR_DILATION)
    group0, group1 = both(tq, tk), both(tq + group, tk)
    r = np.arange(FAR_DILATION)[:, None]
    t = (np.arange(TILE)[None, :] * FAR_DILATION + r).reshape(-1)
    tq, tk = t[:, None], t[None, :]
    near0, near1 = near_of(tq, tk), near_of(tq + TILE * FAR_DILATION, tk)
    upper = near1.reshape(FAR_DILATION, TILE, -1)[:, :REACH_STEPS // FAR_DILATION].reshape(-1, near1.shape[1])
    r = np.arange(2)[:, None]
    t = (np.arange(2 * nq)[None, :] * FAR_DILATION + r).reshape(-1)
    pair2 = every(t[:, None] + 2 * group, t[None, :], FAR_DILATION)
    return [bias_of(np.asarray(x, int)) for x in (group0, group1, near0, near1, upper, pair2)]


def local_kernel(sc_ref, qa_ref, qb_ref, qy_ref, kva_ref, kvb_ref, kvya_ref, kvyb_ref, group_ref, near0_ref, near1_ref,
                 q_ref, m_ref, l_ref, o_ref, k_s, v_s, s_s):
    tp, par = sc_ref[0], sc_ref[1]
    nq = qy_ref.shape[1] // FAR_DILATION
    for h in range(q_ref.shape[0]):
        q, m, l, o, k, v, sh = (x.at[h] for x in (q_ref, m_ref, l_ref, o_ref, k_s, v_s, s_s))
        gather(q, nq, [(qa_ref.at[h], par, tp), (qb_ref.at[h], par, 1 - tp), (qy_ref.at[h], 1 - par, None)])
        gather_kv(k, v, [x.at[h] for x in (kva_ref, kvb_ref, kvya_ref, kvyb_ref)], nq, tp, par)
        at = 0
        items = []
        for r4 in range(MIDDLE_DILATION):
            rows = group_rows(r4, nq)
            items.append((rows, rows, group_ref[...], at))
            scored(items[-1], q, k, sh, m, True)
            at += length(rows)
        for c in range(2 * nq // TILE):
            rows = near_rows(c, nq)
            items.append((rows, rows, near0_ref[...], at))
            scored(items[-1], q, k, sh, m, False)
            at += length(rows)
            if c:
                items.append((upper_rows(c, nq), near_rows(c - 1, nq), near1_ref[...], at))
                scored(items[-1], q, k, sh, m, False)
                at += length(items[-1][0])
        for i, item in enumerate(items):
            ol = weighed(item, v, sh, m, length(item[1]))
            if i < MIDDLE_DILATION:
                put(o, item[0], ol[:, :HEAD])
                put(l, item[0], ol[:, HEAD:])
            else:
                put(o, item[0], take(o, item[0]) + ol[:, :HEAD])
                put(l, item[0], take(l, item[0]) + ol[:, HEAD:])


def one_kernel(sc_ref, q_ref, m_in, l_in, o_in, kva_ref, kvb_ref, kvya_ref, kvyb_ref, group_ref, near_ref,
               m_ref, l_ref, o_ref, state_ref, k_s, v_s, s_s, n_s, piece_s, stat_s):
    tp, par = sc_ref[0], sc_ref[1]
    nq = kvya_ref.shape[2] // FAR_DILATION * 2

    @pl.when(sc_ref[2] >= 1)
    def _():
        for h in range(q_ref.shape[0]):
            q, mi, li, oi, m, l, o, k, v, sh, n = (x.at[h] for x in (
                q_ref, m_in, l_in, o_in, m_ref, l_ref, o_ref, k_s, v_s, s_s, n_s))
            gather_kv(k, v, [x.at[h] for x in (kva_ref, kvb_ref, kvya_ref, kvyb_ref)], nq, tp, par)
            near = (near_rows(0, nq), near_rows(2 * nq // TILE - 1, nq), near_ref[...], 0)
            at = length(near[0])
            items = []
            for r4 in range(MIDDLE_DILATION):
                rows = group_rows(r4, nq)
                items.append((rows, rows, group_ref[...], at))
                scored(items[-1], q, k, sh, n, True)
                at += length(rows)
            scored(near, q, k, sh, n, False)
            for item in items:
                rows = item[0]
                old = take(mi, rows)
                new = jnp.maximum(old, take(n, rows))
                keep = jnp.exp2((old - new) * SCALE)
                put(m, rows, new)
                ol = weighed(item, v, sh, m, length(item[1]))
                put(o, rows, take(oi, rows) * keep + ol[:, :HEAD])
                put(l, rows, take(li, rows) * keep + ol[:, HEAD:])
            ol = weighed(near, v, sh, m, length(near[1]))
            put(o, near[0], take(o, near[0]) + ol[:, :HEAD])
            put(l, near[0], take(l, near[0]) + ol[:, HEAD:])

    for i in range(FAR_DILATION // 2):
        rows = pair_rows(i, nq)
        m, l, o = (take(x.at[RELAYED], rows) for x in (m_ref, l_ref, o_ref))
        pack_rows(piece_s, stat_s, i, o / l, m, l)
    pack_out(state_ref, piece_s, stat_s, 1 - par)


def two_kernel(sc_ref, q_ref, m_ref, l_ref, o_ref, kvo_ref, kvy_ref, pair_ref,
               keep_ref, send_ref, k_s, v_s, s_s, n_s, mix_s, *, head):
    tp, par = sc_ref[0], sc_ref[1]
    nq = kvy_ref.shape[2] // FAR_DILATION * 2
    q, m, l, o = (x.at[head] for x in (q_ref, m_ref, l_ref, o_ref))
    pairs = [pair_rows(i, nq) for i in range(FAR_DILATION // 2)]

    def settle(i, val):
        for part in range(4):
            r, block = 2 * i + part // 2, part % 2
            mix_s[block, pl.ds(r, nq, stride=FAR_DILATION), :] = val[part * nq:(part + 1) * nq]

    @pl.when(sc_ref[2] >= 2)
    def _():
        gather_kv(k_s, v_s, [kvo_ref.at[0], kvo_ref.at[1], kvy_ref.at[0], kvy_ref.at[1]], nq, tp, par)
        items = [(rows, rows, pair_ref[...], i * length(rows)) for i, rows in enumerate(pairs)]
        for item in items:
            put(n_s, item[0], take(m, item[0]))
            scored(item, q, k_s, s_s, n_s, False)
        for i, item in enumerate(items):
            rows = item[0]
            ol = weighed(item, v_s, s_s, n_s, length(rows))
            keep = jnp.exp2((take(m, rows) - take(n_s, rows)) * SCALE)
            settle(i, (take(o, rows) * keep + ol[:, :HEAD]) / (take(l, rows) * keep + ol[:, HEAD:]))

    @pl.when(sc_ref[2] < 2)
    def _():
        for i, rows in enumerate(pairs):
            settle(i, take(o, rows) / take(l, rows))

    keep_ref[...] = mix_s[pl.ds(par, 1)][0].astype(BF16)
    send_ref[...] = mix_s[pl.ds(1 - par, 1)][0].astype(BF16)


def diagonal(n):
    return lax.broadcasted_iota(jnp.int32, (n, n), 0) == lax.broadcasted_iota(jnp.int32, (n, n), 1)


def pack_rows(piece_s, stat_s, i, value, top, total):
    nq = value.shape[0] // 4
    eye = diagonal(HEAD)
    for part in range(4):
        r, block = 2 * i + part // 2, part % 2
        piece_s[block, r * nq:(r + 1) * nq, :] = value[part * nq:(part + 1) * nq].astype(BF16)
    for which, stat in enumerate((top, total)):
        at = which * (FAR_DILATION // 2) + i
        stat_s[at:at + 1, :] = jnp.sum(jnp.where(eye, stat, 0.0), axis=0, keepdims=True)


def pack_out(out_ref, piece_s, stat_s, block):
    rows, count = piece_s.shape[1], stat_s.shape[0]
    out_ref[:rows, :] = piece_s[pl.ds(block, 1)][0]
    rest = stat_s[...]
    for term in range(3):
        low = rest.astype(BF16)
        out_ref[rows + term * count:rows + (term + 1) * count, :] = low
        rest = rest - low.astype(F32)


def unpacked_stats(ref, rows):
    return sum(ref[rows + t * FAR_DILATION:rows + (t + 1) * FAR_DILATION, :].astype(F32) for t in range(3))


def foreign_kernel(sc_ref, qn_ref, kva_ref, kvb_ref, kvya_ref, kvyb_ref, pair_ref,
                   own_ref, diag_ref, q_s, k_s, v_s, s_s, n_s, piece_s, stat_s, *, head):
    tp, par = sc_ref[0], sc_ref[1]
    nq = kvya_ref.shape[2] // FAR_DILATION * 2
    half = kvya_ref.shape[2]
    gather(q_s, nq, [(qn_ref.at[0, :half], par, tp), (qn_ref.at[0, half:], par, 1 - tp), (qn_ref.at[1], 1 - par, None)])
    gather_kv(k_s, v_s, [x.at[head] for x in (kva_ref, kvb_ref, kvya_ref, kvyb_ref)], nq, tp, par)
    pairs = [pair_rows(i, nq) for i in range(FAR_DILATION // 2)]
    items = [(rows, rows, pair_ref[...], i * length(rows)) for i, rows in enumerate(pairs)]
    for item in items:
        scored(item, q_s, k_s, s_s, n_s, True)
    for i, item in enumerate(items):
        ol = weighed(item, v_s, s_s, n_s, length(item[0]))
        total = ol[:, HEAD:]
        pack_rows(piece_s, stat_s, i, ol[:, :HEAD] / total, take(n_s, item[0]), total)
    pack_out(own_ref, piece_s, stat_s, par)
    pack_out(diag_ref, piece_s, stat_s, 1 - par)


def final_kernel(sc_ref, m_ref, l_ref, o_ref, state_ref, own_ref, diag_ref, out_ref, mix_s, *, head):
    par = sc_ref[1]
    m, l, o = (x.at[head] for x in (m_ref, l_ref, o_ref))
    rows = out_ref.shape[1]
    nq = rows // FAR_DILATION
    count = FAR_DILATION // 2
    far = sc_ref[2] >= 2
    eye = diagonal(HEAD)

    def columns(ref):
        stats = unpacked_stats(ref, rows)
        result = []
        for i in range(2 * count):
            spread = jnp.sum(jnp.where(eye, stats[i:i + 1, :], 0.0), axis=1, keepdims=True)
            result.append(jnp.broadcast_to(spread, (HEAD, HEAD)))
        return result

    def rows_of(result, which, r):
        column = result[which * count + r // 2]
        at = (r % 2) * 2 * nq
        return jnp.where(par == 0, column[at:at + nq], column[at + nq:at + 2 * nq])

    def joined(top, total, numerator, ref, result, r):
        top2, total2 = rows_of(result, 0, r), rows_of(result, 1, r)
        top2 = jnp.where(far, top2, MASKED)
        new = jnp.maximum(top, top2)
        keep = jnp.exp2((top - new) * SCALE)
        add = jnp.where(far, jnp.exp2((top2 - new) * SCALE) * total2, 0.0)
        part = jnp.where(far, ref[r * nq:(r + 1) * nq, :].astype(F32), 0.0)
        return (numerator * keep + part * add) / (total * keep + add)

    own_stats, diag_stats, state_stats = columns(own_ref), columns(diag_ref), columns(state_ref)
    for r in range(FAR_DILATION):
        here = pl.ds(pl.multiple_of(r * 2 * nq + par * nq, TILE), nq)
        mix_s[0, pl.ds(r, nq, stride=FAR_DILATION), :] = joined(
            m[here, :], l[here, :], o[here, :], own_ref, own_stats, r)
        top, total = rows_of(state_stats, 0, r), rows_of(state_stats, 1, r)
        mix_s[1, pl.ds(r, nq, stride=FAR_DILATION), :] = joined(
            top, total, state_ref[r * nq:(r + 1) * nq, :].astype(F32) * total, diag_ref, diag_stats, r)
    out_ref[...] = mix_s[...].astype(BF16)


def out_kernel(sc_ref, a_ref, b_ref, c_ref, d_ref, own_ref, tp_ref, w_ref, o_ref):
    tp, par = sc_ref[0], sc_ref[1]
    block = o_ref.shape[1]
    heads = w_ref.shape[0] // HEAD // 4
    column = pl.multiple_of(pl.program_id(0) * block, block)
    order = (2 * tp + par, 2 * tp + 1 - par, 2 * (1 - tp) + par, 2 * (1 - tp) + 1 - par)
    x_refs = (own_ref.at[0], own_ref.at[1], tp_ref.at[0], tp_ref.at[1], a_ref, b_ref, c_ref, d_ref)
    x = jnp.concatenate([x_ref[...] for x_ref in x_refs], axis=1)
    w = jnp.concatenate([w_ref[pl.ds(pl.multiple_of((i * heads + head) * HEAD, HEAD), HEAD), pl.ds(column, block)]
                         for head in (1, 0) for i in order], axis=0)
    o_ref[...] = jnp.dot(x, w, preferred_element_type=F32).astype(BF16)


def out_project(scalars, first, last, weight):
    rows, columns = first[0].shape[0], weight.shape[1]
    steps = 2
    return pl.pallas_call(
        out_kernel,
        grid=(steps,),
        in_specs=[pl.BlockSpec(memory_space=pltpu.SMEM)] + in_vmem(7),
        out_specs=pl.BlockSpec((rows, columns // steps), lambda j: (0, j)),
        out_shape=jax.ShapeDtypeStruct((rows, columns), BF16),
        compiler_params=pltpu.CompilerParams(vmem_limit_bytes=16 * 2 ** 20),
        cost_estimate=pl.CostEstimate(flops=2 * rows * weight.size, transcendentals=0, bytes_accessed=0),
        name="out_project",
    )(scalars, *first, *last, weight)


def swap(x, axis):
    return lax.ppermute(x, axis, [(i, i ^ 1) for i in range(lax.axis_size(axis))])


def onward(x):
    n = lax.axis_size("sp")
    return lax.ppermute(x, "sp", [(i, i + 2) for i in range(n - 2)])


def body(tokens, query_weight, key_weight, value_weight, output_weight):
    half, depth = tokens.shape
    rows = 2 * half
    group = 2 * rows
    nq = rows // FAR_DILATION
    assert 2 * group == FAR_DILATION * REACH_STEPS
    heads = query_weight.shape[1] // HEAD // 2
    width = heads * HEAD
    flops = 2 * rows * depth * width
    sp, tp = lax.axis_index("sp"), lax.axis_index("tp")
    scalars = jnp.stack([tp, sp % 2, sp // 2, sp]).astype(jnp.int32)
    inverse = THETA_BASE ** (-jnp.arange(HEAD // 2, dtype=F32) / (HEAD // 2))
    inverse = jnp.concatenate([inverse, inverse])[None]
    group0, group1, near0, near1, upper, pair2 = biases(nq)
    shape = jax.ShapeDtypeStruct
    kv = shape((heads, 2, half, HEAD), BF16)
    q_shape, q_half = shape((heads, rows, HEAD), BF16), shape((heads, half, HEAD), BF16)
    table = shape((2, half, HEAD), F32)
    buffers = pltpu.VMEM((4 * heads, half, HEAD), F32)

    partner = swap(tokens, "tp")
    weights = shape((2, depth, width), BF16)
    kv_a, own, w_keep, cosine, sine = call(
        own_keep_kernel, scalars, [tokens, key_weight, value_weight, inverse],
        [kv, shape((half, depth), BF16), weights, table, table],
        [buffers, pltpu.VMEM((2, half, width), F32), pltpu.SemaphoreType.DMA((2, 3))], flops, hbm=(0, 1, 2))
    kv1_a = onward(kv_a)
    key_weight, value_weight, own = lax.optimization_barrier((key_weight, value_weight, own))
    send_a, kv_b = call(
        middle_kernel, scalars, [own, partner, key_weight, value_weight, w_keep, cosine, sine], [kv, kv], [buffers],
        2 * flops)
    kv1_b = onward(kv_b)
    kv_ya = swap(send_a, "sp")
    send_b, = call(functools.partial(send_kernel, part=1), scalars, [partner, key_weight, value_weight, cosine, sine],
                   [kv], [buffers],
                   flops)
    kv_yb = swap(send_b, "sp")
    back = shape((heads - RELAYED, 2, half, HEAD), BF16)
    q_a, q_b, q_send, back_own = call(
        q_kernel, scalars, [own, partner, cosine, sine, query_weight], [q_half, q_half, q_shape, back],
        [buffers], 2 * flops)
    q_y = swap(q_send, "sp")
    behind = jnp.stack([back_own.reshape(rows, HEAD), q_y[RELAYED]])
    n = lax.axis_size("sp")
    q_next = lax.ppermute(behind, "sp", [(i, i - 2) for i in range(2, n)])
    kv1_ya = onward(kv_ya)
    kv1_yb = onward(kv_yb)
    kv2_ab = onward(jnp.stack([kv1_a[0], kv1_b[0]]))
    kv2_y = onward(jnp.stack([kv1_ya[0], kv1_yb[0]]))
    packed = shape((rows + 3 * FAR_DILATION, HEAD), BF16)
    packing = [pltpu.VMEM((2, rows, HEAD), BF16), pltpu.VMEM((FAR_DILATION, HEAD), F32)]
    piece_own, piece_diag = call(
        functools.partial(foreign_kernel, head=1), scalars,
        [q_next, kv1_a, kv1_b, kv1_ya, kv1_yb, pair2], [packed, packed],
        [pltpu.VMEM((group, HEAD), BF16)] * 3 + [pltpu.VMEM((group, HEAD), F32)] * 2 + packing, 10 ** 9)
    n = lax.axis_size("sp")
    piece_diag = lax.ppermute(piece_diag, "sp", [(i, (i ^ 1) + 2) for i in range(n - 2)])
    piece_own = onward(piece_own)
    state = shape((heads, group, HEAD), F32)
    kv_scratch = [pltpu.VMEM((heads, group, HEAD), BF16)] * 2
    q, m, l, o = call(
        local_kernel, scalars, [q_a, q_b, q_y, kv_a, kv_b, kv_ya, kv_yb, group0, near0, upper],
        [shape((heads, group, HEAD), BF16), state, state, state],
        kv_scratch + [pltpu.VMEM((heads, 3 * group, 2 * HEAD), F32)], 3 * 10 ** 9)
    m, l, o, state_y = call(
        one_kernel, scalars, [q, m, l, o, kv1_a, kv1_b, kv1_ya, kv1_yb, group1, near1], [state, state, state, packed],
        kv_scratch + [pltpu.VMEM((heads, 2 * group, 2 * HEAD), F32), pltpu.VMEM((heads, group, HEAD), F32)]
        + packing, 10 ** 9, {2: 0, 3: 1, 4: 2})
    state_y = swap(state_y, "sp")
    mixed = shape((rows, HEAD), BF16)
    keep, send = call(
        functools.partial(two_kernel, head=0), scalars, [q, m, l, o, kv2_ab, kv2_y, pair2],
        [mixed, mixed], [pltpu.VMEM((group, HEAD), BF16)] * 2 + [pltpu.VMEM((group, HEAD), F32)] * 2
        + [pltpu.VMEM((2, rows, HEAD), F32)], 10 ** 9)
    keep_tp = swap(keep, "tp")
    from_y = swap(send, "sp")
    first = [keep, from_y, keep_tp, swap(from_y, "tp")]
    last, = call(functools.partial(final_kernel, head=1), scalars, [m, l, o, state_y, piece_own, piece_diag],
                 [shape((2, rows, HEAD), BF16)], [pltpu.VMEM((2, rows, HEAD), F32)], 10 ** 9)
    last_tp = swap(last, "tp")
    return out_project(scalars, first, [last, last_tp], output_weight)


def solution(mesh):
    in_specs = (
        P(("grp", "sp", "tp"), None),
        P(None, "tp"),
        P(None, "tp"),
        P(None, "tp"),
        P(None, "tp"),
    )
    out_specs = P(("grp", "sp"), "tp")

    return jax.shard_map(body, mesh=mesh, in_specs=in_specs, out_specs=out_specs, check_vma=False)
```

```python
import functools

import jax
import jax.numpy as jnp
import numpy as np
from jax import lax
from jax.experimental import pallas as pl
from jax.experimental.pallas import tpu as pltpu
from jax.sharding import PartitionSpec as P

HEAD = 128
REACH_STEPS = 128
MIDDLE_DILATION = 4
FAR_DILATION = 16
THETA_BASE = 500000.0
TILE = 16
RELAYED = 1
MASKED = -1e30
SCALE = HEAD ** -0.5 * 1.4426950408889634
F32 = jnp.float32
BF16 = jnp.bfloat16


def in_vmem(count):
    return [pl.BlockSpec(memory_space=pltpu.VMEM)] * count


def rotated(val, cos, sin):
    return val * cos + pltpu.roll(val, HEAD // 2, 1) * sin


def place(out_ref, lead, val, buf_ref, slot, first):
    nq_half = val.shape[0] // FAR_DILATION
    buf_ref[slot] = val
    for r in range(FAR_DILATION):
        piece = buf_ref[slot, pl.ds(r, nq_half, stride=FAR_DILATION), :]
        at = r * nq_half if first is None else pl.multiple_of((2 * r + first) * nq_half, TILE)
        out_ref[lead + (pl.ds(at, nq_half), slice(None))] = piece.astype(BF16)


def kv_finish(acc, which, out_ref, cos_ref, sin_ref, buf_ref):
    heads = acc.shape[1] // HEAD
    for h in range(heads):
        val = acc[:, h * HEAD:(h + 1) * HEAD]
        if which == 0:
            val = rotated(val, cos_ref[...], sin_ref[...])
        place(out_ref, (h, which), val, buf_ref, (1 - which) * heads + h, None)


def kv_part(x_ref, w_refs, out_ref, cos_ref, sin_ref, buf_ref):
    for which in (1, 0):
        acc = jnp.dot(x_ref[...], w_refs[which][...], preferred_element_type=F32)
        kv_finish(acc, which, out_ref, cos_ref, sin_ref, buf_ref)


def own_keep_kernel(sc_ref, x_hbm, wk_hbm, wv_hbm, inv_ref,
                    out_ref, x_ref, w_ref, cos_ref, sin_ref, buf_ref, acc_ref, sems):
    tp, par, sp = sc_ref[0], sc_ref[1], sc_ref[3]
    half = x_ref.shape[0]
    depth, width = w_ref.shape[1:]
    column = pl.ds(pl.multiple_of(par * width, width), width)
    cuts = [pl.ds(i * depth // 2, depth // 2) for i in range(2)]
    copies = []
    for i, cut in enumerate(cuts):
        copies.append([
            pltpu.make_async_copy(wk_hbm.at[cut, column], w_ref.at[0, cut], sems.at[i, 0]),
            pltpu.make_async_copy(wv_hbm.at[cut, column], w_ref.at[1, cut], sems.at[i, 1]),
            pltpu.make_async_copy(x_hbm.at[:, cut], x_ref.at[:, cut], sems.at[i, 2])])
    for part in copies:
        for i in (2, 1, 0):
            part[i].start()
    steps = half // FAR_DILATION
    lane = lax.broadcasted_iota(jnp.int32, (2 * steps, HEAD), 1)
    row = lax.broadcasted_iota(jnp.int32, (2 * steps, HEAD), 0)
    part = jnp.where(row < steps, tp, 1 - tp)
    position = sp * (2 * half) + part * half + (row % steps) * FAR_DILATION
    coarse = position.astype(F32) * inv_ref[...]
    fine = lax.broadcasted_iota(jnp.int32, (FAR_DILATION, HEAD), 0).astype(F32) * inv_ref[...]
    cos_c, sin_c = jnp.cos(coarse)[:, None, :], jnp.sin(coarse)[:, None, :]
    cos_f, sin_f = jnp.cos(fine)[None], jnp.sin(fine)[None]
    sign = jnp.where(lane[:1] < HEAD // 2, -1.0, 1.0)[None]
    cos_ref[...] = (cos_c * cos_f - sin_c * sin_f).reshape(2, half, HEAD)
    sin_ref[...] = ((sin_c * cos_f + cos_c * sin_f) * sign).reshape(2, half, HEAD)
    for i, cut in enumerate(cuts):
        copies[i][2].wait()
        for which in (1, 0):
            copies[i][which].wait()
            acc = jnp.dot(x_ref[:, cut], w_ref[which, cut], preferred_element_type=F32)
            if i == 0:
                acc_ref[which] = acc
            else:
                kv_finish(acc_ref[which] + acc, which, out_ref, cos_ref.at[0], sin_ref.at[0], buf_ref)


def middle_kernel(sc_ref, xo_ref, xp_ref, wk_ref, wv_ref, w_ref, cos_ref, sin_ref, send_ref, keep_ref, buf_ref):
    send_kernel(sc_ref, xo_ref, wk_ref, wv_ref, cos_ref, sin_ref, send_ref, buf_ref, part=0)
    half = buf_ref.shape[0] // 2
    kv_part(xp_ref, (w_ref.at[0], w_ref.at[1]), keep_ref, cos_ref.at[1], sin_ref.at[1], buf_ref.at[half:])


def send_kernel(sc_ref, x_ref, wk_ref, wv_ref, cos_ref, sin_ref, out_ref, buf_ref, *, part):
    width = out_ref.shape[0] * HEAD
    column = pl.ds(pl.multiple_of((1 - sc_ref[1]) * width, width), width)
    kv_part(x_ref, (wk_ref.at[:, column], wv_ref.at[:, column]), out_ref, cos_ref.at[part], sin_ref.at[part], buf_ref)


def q_kernel(sc_ref, xo_ref, xp_ref, cos_ref, sin_ref, w_ref, keepa_ref, keepb_ref, send0_ref, send1_ref,
             back_ref, buf_ref):
    tp, par = sc_ref[0], sc_ref[1]
    heads = keepa_ref.shape[0]
    width = heads * HEAD
    slot = 0
    for side in (1, 0):
        w = w_ref[:, pl.ds(pl.multiple_of((1 - par if side else par) * width, width), width)]
        for part, x_ref in enumerate((xo_ref, xp_ref)):
            acc = jnp.dot(x_ref[...], w, preferred_element_type=F32)
            for h in range(heads):
                val = rotated(acc[:, h * HEAD:(h + 1) * HEAD], cos_ref[part], sin_ref[part])
                if side:
                    place((send0_ref, send1_ref)[h], (), val, buf_ref, slot, tp if part == 0 else 1 - tp)
                else:
                    place((keepa_ref, keepb_ref)[part], (h,), val, buf_ref, slot, None)
                if h >= RELAYED and not side:
                    place(back_ref, (h - RELAYED, part), val, buf_ref, slot, None)
                slot += 1


def call(kernel, scalars, inputs, outputs, scratch, flops, aliases={}, limit=28, hbm=()):
    spaces = [pltpu.HBM if i in hbm else pltpu.VMEM for i in range(len(inputs))]
    return pl.pallas_call(
        kernel,
        in_specs=[pl.BlockSpec(memory_space=pltpu.SMEM)] + [pl.BlockSpec(memory_space=m) for m in spaces],
        out_specs=in_vmem(len(outputs)),
        out_shape=outputs,
        scratch_shapes=scratch,
        input_output_aliases=aliases,
        compiler_params=pltpu.CompilerParams(vmem_limit_bytes=limit * 2 ** 20),
        cost_estimate=pl.CostEstimate(flops=flops, transcendentals=0, bytes_accessed=0),
    )(scalars, *[pltpu.with_memory_space_constraint(x, pltpu.HBM) if i in hbm else x for i, x in enumerate(inputs)])


def gather(dst_ref, nq, sources):
    for r in range(FAR_DILATION):
        for source, block, half in sources:
            rows = nq if half is None else nq // 2
            start = 0 if half is None else half * (nq // 2)
            at = pl.multiple_of(r * 2 * nq + block * nq + start, TILE)
            dst_ref[pl.ds(at, rows), :] = source[r * rows:(r + 1) * rows, :]


def gather_kv(k_ref, v_ref, refs, nq, tp, par):
    places = ((par, tp), (par, 1 - tp), (1 - par, tp), (1 - par, 1 - tp))
    for which, dst_ref in enumerate((k_ref, v_ref)):
        gather(dst_ref, nq, [(ref.at[which], block, half) for ref, (block, half) in zip(refs, places)])


def scores_of(q, k):
    return lax.dot_general(q, k, (((1,), (1,)), ((), ())), preferred_element_type=F32)


def take(ref, rows):
    parts = [ref[a:a + n, :] for a, n in rows]
    return parts[0] if len(parts) == 1 else jnp.concatenate(parts, axis=0)


def put(ref, rows, value):
    at = 0
    for a, n in rows:
        ref[a:a + n, :] = value[at:at + n]
        at += n


def widened(stat, columns):
    return jnp.concatenate([stat] * (columns // HEAD), axis=1) if columns > HEAD else stat


def scored(item, q_ref, k_ref, s_ref, m_ref, fresh):
    rows, keys, bias, at = item
    if rows[0][1] < TILE:
        s = scores_of(take(q_ref, [(a, TILE) for a, _ in rows]), take(k_ref, keys))
        s = s.reshape(len(rows), TILE, s.shape[1])[:, :rows[0][1]].reshape(length(rows), s.shape[1])
    else:
        s = scores_of(take(q_ref, rows), take(k_ref, keys))
    if bias is not None:
        s = s + bias
    n, columns = s.shape
    s_ref[at:at + n, :columns] = s
    top = jnp.broadcast_to(jnp.max(s, axis=-1, keepdims=True), (n, HEAD))
    put(m_ref, rows, top if fresh else jnp.maximum(take(m_ref, rows), top))


def weighed(item, v_ref, s_ref, m_ref, columns):
    rows, keys, _, at = item
    n = sum(c for _, c in rows)
    p = jnp.exp2((s_ref[at:at + n, :columns] - widened(take(m_ref, rows), columns)) * SCALE).astype(BF16)
    v = take(v_ref, keys)
    return jnp.dot(p, jnp.concatenate([v, jnp.ones_like(v)], axis=1), preferred_element_type=F32)


def length(rows):
    return sum(n for _, n in rows)


def group_rows(r4, nq):
    return [((r4 + MIDDLE_DILATION * j) * 2 * nq, 2 * nq) for j in range(FAR_DILATION // MIDDLE_DILATION)]


def near_rows(c, nq):
    return [(r * 2 * nq + c * TILE, TILE) for r in range(FAR_DILATION)]


def upper_rows(c, nq):
    return [(a, REACH_STEPS // FAR_DILATION) for a, _ in near_rows(c, nq)]


def pair_rows(i, nq):
    return [(i * 4 * nq, 4 * nq)]


def near_of(tq, tk):
    return (tq - tk >= 0) & (tq - tk <= REACH_STEPS)


def every(tq, tk, step):
    return (tq % step == tk % step) & (tq - tk >= 0) & (tq - tk <= REACH_STEPS * step)


def bias_of(count):
    return np.where(count > 0, np.log2(np.maximum(count, 1)) / SCALE, MASKED).astype(np.float32)


def biases(nq):
    group = 2 * nq * FAR_DILATION
    j = np.arange(FAR_DILATION // MIDDLE_DILATION)[:, None]
    t = (np.arange(2 * nq)[None, :] * FAR_DILATION + j * MIDDLE_DILATION).reshape(-1)
    tq, tk = t[:, None], t[None, :]
    both = lambda tq, tk: every(tq, tk, MIDDLE_DILATION).astype(int) + every(tq, tk, FAR_DILATION)
    group0, group1 = both(tq, tk), both(tq + group, tk)
    r = np.arange(FAR_DILATION)[:, None]
    t = (np.arange(TILE)[None, :] * FAR_DILATION + r).reshape(-1)
    tq, tk = t[:, None], t[None, :]
    near0, near1 = near_of(tq, tk), near_of(tq + TILE * FAR_DILATION, tk)
    upper = near1.reshape(FAR_DILATION, TILE, -1)[:, :REACH_STEPS // FAR_DILATION].reshape(-1, near1.shape[1])
    r = np.arange(2)[:, None]
    t = (np.arange(2 * nq)[None, :] * FAR_DILATION + r).reshape(-1)
    pair2 = every(t[:, None] + 2 * group, t[None, :], FAR_DILATION)
    return [bias_of(np.asarray(x, int)) for x in (group0, group1, near0, near1, upper, pair2)]


def local_kernel(sc_ref, qa_ref, qb_ref, qy0_ref, qy1_ref, kva_ref, kvb_ref, kvya_ref, kvyb_ref, group_ref, near0_ref, near1_ref,
                 q_ref, m_ref, l_ref, o_ref, k_s, v_s, s_s):
    tp, par = sc_ref[0], sc_ref[1]
    nq = qy0_ref.shape[0] // FAR_DILATION
    for h in range(q_ref.shape[0]):
        q, m, l, o, k, v, sh = (x.at[h] for x in (q_ref, m_ref, l_ref, o_ref, k_s, v_s, s_s))
        gather(q, nq, [(qa_ref.at[h], par, tp), (qb_ref.at[h], par, 1 - tp), ((qy0_ref, qy1_ref)[h], 1 - par, None)])
        gather_kv(k, v, [x.at[h] for x in (kva_ref, kvb_ref, kvya_ref, kvyb_ref)], nq, tp, par)
        at = 0
        items = []
        for r4 in range(MIDDLE_DILATION):
            rows = group_rows(r4, nq)
            items.append((rows, rows, group_ref[...], at))
            scored(items[-1], q, k, sh, m, True)
            at += length(rows)
        for c in range(2 * nq // TILE):
            rows = near_rows(c, nq)
            items.append((rows, rows, near0_ref[...], at))
            scored(items[-1], q, k, sh, m, False)
            at += length(rows)
            if c:
                items.append((upper_rows(c, nq), near_rows(c - 1, nq), near1_ref[...], at))
                scored(items[-1], q, k, sh, m, False)
                at += length(items[-1][0])
        for i, item in enumerate(items):
            ol = weighed(item, v, sh, m, length(item[1]))
            if i < MIDDLE_DILATION:
                put(o, item[0], ol[:, :HEAD])
                put(l, item[0], ol[:, HEAD:])
            else:
                put(o, item[0], take(o, item[0]) + ol[:, :HEAD])
                put(l, item[0], take(l, item[0]) + ol[:, HEAD:])


def one_kernel(sc_ref, q_ref, m_in, l_in, o_in, kva_ref, kvb_ref, kvya_ref, kvyb_ref, group_ref, near_ref,
               m_ref, l_ref, o_ref, state_ref, k_s, v_s, s_s, n_s, piece_s, stat_s):
    tp, par = sc_ref[0], sc_ref[1]
    nq = kvya_ref.shape[2] // FAR_DILATION * 2

    @pl.when(sc_ref[2] >= 1)
    def _():
        for h in range(q_ref.shape[0]):
            q, mi, li, oi, m, l, o, k, v, sh, n = (x.at[h] for x in (
                q_ref, m_in, l_in, o_in, m_ref, l_ref, o_ref, k_s, v_s, s_s, n_s))
            gather_kv(k, v, [x.at[h] for x in (kva_ref, kvb_ref, kvya_ref, kvyb_ref)], nq, tp, par)
            near = (near_rows(0, nq), near_rows(2 * nq // TILE - 1, nq), near_ref[...], 0)
            at = length(near[0])
            items = []
            for r4 in range(MIDDLE_DILATION):
                rows = group_rows(r4, nq)
                items.append((rows, rows, group_ref[...], at))
                scored(items[-1], q, k, sh, n, True)
                at += length(rows)
            scored(near, q, k, sh, n, False)
            for item in items:
                rows = item[0]
                old = take(mi, rows)
                new = jnp.maximum(old, take(n, rows))
                keep = jnp.exp2((old - new) * SCALE)
                put(m, rows, new)
                ol = weighed(item, v, sh, m, length(item[1]))
                put(o, rows, take(oi, rows) * keep + ol[:, :HEAD])
                put(l, rows, take(li, rows) * keep + ol[:, HEAD:])
            ol = weighed(near, v, sh, m, length(near[1]))
            put(o, near[0], take(o, near[0]) + ol[:, :HEAD])
            put(l, near[0], take(l, near[0]) + ol[:, HEAD:])

    for i in range(FAR_DILATION // 2):
        rows = pair_rows(i, nq)
        m, l, o = (take(x.at[RELAYED], rows) for x in (m_ref, l_ref, o_ref))
        pack_rows(piece_s, stat_s, i, o / l, m, l)
    pack_out(state_ref, piece_s, stat_s, 1 - par)


def two_kernel(sc_ref, q_ref, m_ref, l_ref, o_ref, kvo_ref, kvy_ref, pair_ref,
               keep_ref, send_ref, k_s, v_s, s_s, n_s, mix_s, *, head):
    tp, par = sc_ref[0], sc_ref[1]
    nq = kvy_ref.shape[2] // FAR_DILATION * 2
    q, m, l, o = (x.at[head] for x in (q_ref, m_ref, l_ref, o_ref))
    pairs = [pair_rows(i, nq) for i in range(FAR_DILATION // 2)]

    def settle(i, val):
        for part in range(4):
            r, block = 2 * i + part // 2, part % 2
            mix_s[block, pl.ds(r, nq, stride=FAR_DILATION), :] = val[part * nq:(part + 1) * nq]

    @pl.when(sc_ref[2] >= 2)
    def _():
        gather_kv(k_s, v_s, [kvo_ref.at[0], kvo_ref.at[1], kvy_ref.at[0], kvy_ref.at[1]], nq, tp, par)
        items = [(rows, rows, pair_ref[...], i * length(rows)) for i, rows in enumerate(pairs)]
        for item in items:
            put(n_s, item[0], take(m, item[0]))
            scored(item, q, k_s, s_s, n_s, False)
        for i, item in enumerate(items):
            rows = item[0]
            ol = weighed(item, v_s, s_s, n_s, length(rows))
            keep = jnp.exp2((take(m, rows) - take(n_s, rows)) * SCALE)
            settle(i, (take(o, rows) * keep + ol[:, :HEAD]) / (take(l, rows) * keep + ol[:, HEAD:]))

    @pl.when(sc_ref[2] < 2)
    def _():
        for i, rows in enumerate(pairs):
            settle(i, take(o, rows) / take(l, rows))

    keep_ref[...] = mix_s[pl.ds(par, 1)][0].astype(BF16)
    send_ref[...] = mix_s[pl.ds(1 - par, 1)][0].astype(BF16)


def diagonal(n):
    return lax.broadcasted_iota(jnp.int32, (n, n), 0) == lax.broadcasted_iota(jnp.int32, (n, n), 1)


def pack_rows(piece_s, stat_s, i, value, top, total):
    nq = value.shape[0] // 4
    eye = diagonal(HEAD)
    for part in range(4):
        r, block = 2 * i + part // 2, part % 2
        piece_s[block, r * nq:(r + 1) * nq, :] = value[part * nq:(part + 1) * nq].astype(BF16)
    for which, stat in enumerate((top, total)):
        at = which * (FAR_DILATION // 2) + i
        stat_s[at:at + 1, :] = jnp.sum(jnp.where(eye, stat, 0.0), axis=0, keepdims=True)


def pack_out(out_ref, piece_s, stat_s, block):
    rows, count = piece_s.shape[1], stat_s.shape[0]
    out_ref[:rows, :] = piece_s[pl.ds(block, 1)][0]
    rest = stat_s[...]
    for term in range(3):
        low = rest.astype(BF16)
        out_ref[rows + term * count:rows + (term + 1) * count, :] = low
        rest = rest - low.astype(F32)


def unpacked_stats(ref, rows):
    return sum(ref[rows + t * FAR_DILATION:rows + (t + 1) * FAR_DILATION, :].astype(F32) for t in range(3))


def foreign_kernel(sc_ref, qn_ref, kva_ref, kvb_ref, kvya_ref, kvyb_ref, pair_ref,
                   own_ref, diag_ref, q_s, k_s, v_s, s_s, n_s, piece_s, stat_s, *, head):
    tp, par = sc_ref[0], sc_ref[1]
    nq = kvya_ref.shape[2] // FAR_DILATION * 2
    half = kvya_ref.shape[2]
    gather(q_s, nq, [(qn_ref.at[0, :half], par, tp), (qn_ref.at[0, half:], par, 1 - tp), (qn_ref.at[1], 1 - par, None)])
    gather_kv(k_s, v_s, [x.at[head] for x in (kva_ref, kvb_ref, kvya_ref, kvyb_ref)], nq, tp, par)
    pairs = [pair_rows(i, nq) for i in range(FAR_DILATION // 2)]
    items = [(rows, rows, pair_ref[...], i * length(rows)) for i, rows in enumerate(pairs)]
    for item in items:
        scored(item, q_s, k_s, s_s, n_s, True)
    for i, item in enumerate(items):
        ol = weighed(item, v_s, s_s, n_s, length(item[0]))
        total = ol[:, HEAD:]
        pack_rows(piece_s, stat_s, i, ol[:, :HEAD] / total, take(n_s, item[0]), total)
    pack_out(own_ref, piece_s, stat_s, par)
    pack_out(diag_ref, piece_s, stat_s, 1 - par)


def final_kernel(sc_ref, m_ref, l_ref, o_ref, state_ref, own_ref, diag_ref, out_ref, mix_s, *, head):
    par = sc_ref[1]
    m, l, o = (x.at[head] for x in (m_ref, l_ref, o_ref))
    rows = out_ref.shape[1]
    nq = rows // FAR_DILATION
    count = FAR_DILATION // 2
    far = sc_ref[2] >= 2
    eye = diagonal(HEAD)

    def columns(ref):
        stats = unpacked_stats(ref, rows)
        result = []
        for i in range(2 * count):
            spread = jnp.sum(jnp.where(eye, stats[i:i + 1, :], 0.0), axis=1, keepdims=True)
            result.append(jnp.broadcast_to(spread, (HEAD, HEAD)))
        return result

    def rows_of(result, which, r):
        column = result[which * count + r // 2]
        at = (r % 2) * 2 * nq
        return jnp.where(par == 0, column[at:at + nq], column[at + nq:at + 2 * nq])

    def joined(top, total, numerator, ref, result, r):
        top2, total2 = rows_of(result, 0, r), rows_of(result, 1, r)
        top2 = jnp.where(far, top2, MASKED)
        new = jnp.maximum(top, top2)
        keep = jnp.exp2((top - new) * SCALE)
        add = jnp.where(far, jnp.exp2((top2 - new) * SCALE) * total2, 0.0)
        part = jnp.where(far, ref[r * nq:(r + 1) * nq, :].astype(F32), 0.0)
        return (numerator * keep + part * add) / (total * keep + add)

    own_stats, diag_stats, state_stats = columns(own_ref), columns(diag_ref), columns(state_ref)
    for r in range(FAR_DILATION):
        here = pl.ds(pl.multiple_of(r * 2 * nq + par * nq, TILE), nq)
        mix_s[0, pl.ds(r, nq, stride=FAR_DILATION), :] = joined(
            m[here, :], l[here, :], o[here, :], own_ref, own_stats, r)
        top, total = rows_of(state_stats, 0, r), rows_of(state_stats, 1, r)
        mix_s[1, pl.ds(r, nq, stride=FAR_DILATION), :] = joined(
            top, total, state_ref[r * nq:(r + 1) * nq, :].astype(F32) * total, diag_ref, diag_stats, r)
    out_ref[...] = mix_s[...].astype(BF16)


def out_kernel(sc_ref, a_ref, b_ref, c_ref, d_ref, own_ref, tp_ref, w_ref, o_ref):
    tp, par = sc_ref[0], sc_ref[1]
    block = o_ref.shape[1]
    heads = w_ref.shape[0] // HEAD // 4
    column = pl.multiple_of(pl.program_id(0) * block, block)
    order = (2 * tp + par, 2 * tp + 1 - par, 2 * (1 - tp) + par, 2 * (1 - tp) + 1 - par)
    x_refs = (own_ref.at[0], own_ref.at[1], tp_ref.at[0], tp_ref.at[1], a_ref, b_ref, c_ref, d_ref)
    x = jnp.concatenate([x_ref[...] for x_ref in x_refs], axis=1)
    w = jnp.concatenate([w_ref[pl.ds(pl.multiple_of((i * heads + head) * HEAD, HEAD), HEAD), pl.ds(column, block)]
                         for head in (1, 0) for i in order], axis=0)
    o_ref[...] = jnp.dot(x, w, preferred_element_type=F32).astype(BF16)


def out_project(scalars, first, last, weight):
    rows, columns = first[0].shape[0], weight.shape[1]
    steps = 2
    return pl.pallas_call(
        out_kernel,
        grid=(steps,),
        in_specs=[pl.BlockSpec(memory_space=pltpu.SMEM)] + in_vmem(7),
        out_specs=pl.BlockSpec((rows, columns // steps), lambda j: (0, j)),
        out_shape=jax.ShapeDtypeStruct((rows, columns), BF16),
        compiler_params=pltpu.CompilerParams(vmem_limit_bytes=16 * 2 ** 20),
        cost_estimate=pl.CostEstimate(flops=2 * rows * weight.size, transcendentals=0, bytes_accessed=0),
        name="out_project",
    )(scalars, *first, *last, weight)


def swap(x, axis):
    return lax.ppermute(x, axis, [(i, i ^ 1) for i in range(lax.axis_size(axis))])


def onward(x):
    n = lax.axis_size("sp")
    return lax.ppermute(x, "sp", [(i, i + 2) for i in range(n - 2)])


def body(tokens, query_weight, key_weight, value_weight, output_weight):
    half, depth = tokens.shape
    rows = 2 * half
    group = 2 * rows
    nq = rows // FAR_DILATION
    assert 2 * group == FAR_DILATION * REACH_STEPS
    heads = query_weight.shape[1] // HEAD // 2
    width = heads * HEAD
    flops = 2 * rows * depth * width
    sp, tp = lax.axis_index("sp"), lax.axis_index("tp")
    scalars = jnp.stack([tp, sp % 2, sp // 2, sp]).astype(jnp.int32)
    inverse = THETA_BASE ** (-jnp.arange(HEAD // 2, dtype=F32) / (HEAD // 2))
    inverse = jnp.concatenate([inverse, inverse])[None]
    group0, group1, near0, near1, upper, pair2 = biases(nq)
    shape = jax.ShapeDtypeStruct
    kv = shape((heads, 2, half, HEAD), BF16)
    q_shape, q_half = shape((rows, HEAD), BF16), shape((heads, half, HEAD), BF16)
    table = shape((2, half, HEAD), F32)
    buffers = pltpu.VMEM((4 * heads, half, HEAD), F32)

    partner = swap(tokens, "tp")
    weights = shape((2, depth, width), BF16)
    kv_a, own, w_keep, cosine, sine = call(
        own_keep_kernel, scalars, [tokens, key_weight, value_weight, inverse],
        [kv, shape((half, depth), BF16), weights, table, table],
        [buffers, pltpu.VMEM((2, half, width), F32), pltpu.SemaphoreType.DMA((2, 3))], flops, hbm=(0, 1, 2))
    kv1_a = onward(kv_a)
    key_weight, value_weight, own = lax.optimization_barrier((key_weight, value_weight, own))
    send_a, kv_b = call(
        middle_kernel, scalars, [own, partner, key_weight, value_weight, w_keep, cosine, sine], [kv, kv], [buffers],
        2 * flops)
    kv1_b = onward(kv_b)
    kv_ya = swap(send_a, "sp")
    send_b, = call(functools.partial(send_kernel, part=1), scalars, [partner, key_weight, value_weight, cosine, sine],
                   [kv], [buffers],
                   flops)
    kv_yb = swap(send_b, "sp")
    back = shape((heads - RELAYED, 2, half, HEAD), BF16)
    q_a, q_b, q_send0, q_send1, back_own = call(
        q_kernel, scalars, [own, partner, cosine, sine, query_weight], [q_half, q_half, q_shape, q_shape, back],
        [buffers], 2 * flops)
    q_y1 = swap(q_send1, "sp")
    q_y0 = swap(q_send0, "sp")
    behind = jnp.stack([back_own.reshape(rows, HEAD), q_y1])
    n = lax.axis_size("sp")
    q_next = lax.ppermute(behind, "sp", [(i, i - 2) for i in range(2, n)])
    kv1_ya = onward(kv_ya)
    kv1_yb = onward(kv_yb)
    kv2_ab = onward(jnp.stack([kv1_a[0], kv1_b[0]]))
    kv2_y = onward(jnp.stack([kv1_ya[0], kv1_yb[0]]))
    packed = shape((rows + 3 * FAR_DILATION, HEAD), BF16)
    packing = [pltpu.VMEM((2, rows, HEAD), BF16), pltpu.VMEM((FAR_DILATION, HEAD), F32)]
    piece_own, piece_diag = call(
        functools.partial(foreign_kernel, head=1), scalars,
        [q_next, kv1_a, kv1_b, kv1_ya, kv1_yb, pair2], [packed, packed],
        [pltpu.VMEM((group, HEAD), BF16)] * 3 + [pltpu.VMEM((group, HEAD), F32)] * 2 + packing, 10 ** 9)
    n = lax.axis_size("sp")
    piece_diag = lax.ppermute(piece_diag, "sp", [(i, (i ^ 1) + 2) for i in range(n - 2)])
    piece_own = onward(piece_own)
    state = shape((heads, group, HEAD), F32)
    kv_scratch = [pltpu.VMEM((heads, group, HEAD), BF16)] * 2
    q, m, l, o = call(
        local_kernel, scalars, [q_a, q_b, q_y0, q_y1, kv_a, kv_b, kv_ya, kv_yb, group0, near0, upper],
        [shape((heads, group, HEAD), BF16), state, state, state],
        kv_scratch + [pltpu.VMEM((heads, 3 * group, 2 * HEAD), F32)], 3 * 10 ** 9)
    m, l, o, state_y = call(
        one_kernel, scalars, [q, m, l, o, kv1_a, kv1_b, kv1_ya, kv1_yb, group1, near1], [state, state, state, packed],
        kv_scratch + [pltpu.VMEM((heads, 2 * group, 2 * HEAD), F32), pltpu.VMEM((heads, group, HEAD), F32)]
        + packing, 10 ** 9, {2: 0, 3: 1, 4: 2})
    state_y = swap(state_y, "sp")
    mixed = shape((rows, HEAD), BF16)
    keep, send = call(
        functools.partial(two_kernel, head=0), scalars, [q, m, l, o, kv2_ab, kv2_y, pair2],
        [mixed, mixed], [pltpu.VMEM((group, HEAD), BF16)] * 2 + [pltpu.VMEM((group, HEAD), F32)] * 2
        + [pltpu.VMEM((2, rows, HEAD), F32)], 10 ** 9)
    keep_tp = swap(keep, "tp")
    from_y = swap(send, "sp")
    first = [keep, from_y, keep_tp, swap(from_y, "tp")]
    last, = call(functools.partial(final_kernel, head=1), scalars, [m, l, o, state_y, piece_own, piece_diag],
                 [shape((2, rows, HEAD), BF16)], [pltpu.VMEM((2, rows, HEAD), F32)], 10 ** 9)
    last_tp = swap(last, "tp")
    return out_project(scalars, first, [last, last_tp], output_weight)


def solution(mesh):
    in_specs = (
        P(("grp", "sp", "tp"), None),
        P(None, "tp"),
        P(None, "tp"),
        P(None, "tp"),
        P(None, "tp"),
    )
    out_specs = P(("grp", "sp"), "tp")

    return jax.shard_map(body, mesh=mesh, in_specs=in_specs, out_specs=out_specs, check_vma=False)
```

```python
import functools

import jax
import jax.numpy as jnp
import numpy as np
from jax import lax
from jax.experimental import pallas as pl
from jax.experimental.pallas import tpu as pltpu
from jax.sharding import PartitionSpec as P

HEAD = 128
REACH_STEPS = 128
MIDDLE_DILATION = 4
FAR_DILATION = 16
THETA_BASE = 500000.0
TILE = 16
RELAYED = 1
MASKED = -1e30
SCALE = HEAD ** -0.5 * 1.4426950408889634
F32 = jnp.float32
BF16 = jnp.bfloat16


def in_vmem(count):
    return [pl.BlockSpec(memory_space=pltpu.VMEM)] * count


def rotated(val, cos, sin):
    return val * cos + pltpu.roll(val, HEAD // 2, 1) * sin


def place(out_ref, lead, val, buf_ref, slot, first):
    nq_half = val.shape[0] // FAR_DILATION
    buf_ref[slot] = val
    for r in range(FAR_DILATION):
        piece = buf_ref[slot, pl.ds(r, nq_half, stride=FAR_DILATION), :]
        at = r * nq_half if first is None else pl.multiple_of((2 * r + first) * nq_half, TILE)
        out_ref[lead + (pl.ds(at, nq_half), slice(None))] = piece.astype(BF16)


def kv_finish(acc, which, out_ref, cos_ref, sin_ref, buf_ref):
    heads = acc.shape[1] // HEAD
    for h in range(heads):
        val = acc[:, h * HEAD:(h + 1) * HEAD]
        if which == 0:
            val = rotated(val, cos_ref[...], sin_ref[...])
        place(out_ref, (h, which), val, buf_ref, (1 - which) * heads + h, None)


def kv_part(x_ref, w_refs, out_ref, cos_ref, sin_ref, buf_ref):
    for which in (1, 0):
        acc = jnp.dot(x_ref[...], w_refs[which][...], preferred_element_type=F32)
        kv_finish(acc, which, out_ref, cos_ref, sin_ref, buf_ref)


def own_keep_kernel(sc_ref, x_hbm, wk_hbm, wv_hbm, inv_ref,
                    out_ref, x_ref, w_ref, cos_ref, sin_ref, buf_ref, acc_ref, sems):
    tp, par, sp = sc_ref[0], sc_ref[1], sc_ref[3]
    half = x_ref.shape[0]
    depth, width = w_ref.shape[1:]
    column = pl.ds(pl.multiple_of(par * width, width), width)
    cuts = [pl.ds(i * depth // 2, depth // 2) for i in range(2)]
    copies = []
    for i, cut in enumerate(cuts):
        copies.append([
            pltpu.make_async_copy(wk_hbm.at[cut, column], w_ref.at[0, cut], sems.at[i, 0]),
            pltpu.make_async_copy(wv_hbm.at[cut, column], w_ref.at[1, cut], sems.at[i, 1]),
            pltpu.make_async_copy(x_hbm.at[:, cut], x_ref.at[:, cut], sems.at[i, 2])])
    for part in copies:
        for i in (2, 1, 0):
            part[i].start()
    steps = half // FAR_DILATION
    lane = lax.broadcasted_iota(jnp.int32, (2 * steps, HEAD), 1)
    row = lax.broadcasted_iota(jnp.int32, (2 * steps, HEAD), 0)
    part = jnp.where(row < steps, tp, 1 - tp)
    position = sp * (2 * half) + part * half + (row % steps) * FAR_DILATION
    coarse = position.astype(F32) * inv_ref[...]
    fine = lax.broadcasted_iota(jnp.int32, (FAR_DILATION, HEAD), 0).astype(F32) * inv_ref[...]
    cos_c, sin_c = jnp.cos(coarse)[:, None, :], jnp.sin(coarse)[:, None, :]
    cos_f, sin_f = jnp.cos(fine)[None], jnp.sin(fine)[None]
    sign = jnp.where(lane[:1] < HEAD // 2, -1.0, 1.0)[None]
    cos_ref[...] = (cos_c * cos_f - sin_c * sin_f).reshape(2, half, HEAD)
    sin_ref[...] = ((sin_c * cos_f + cos_c * sin_f) * sign).reshape(2, half, HEAD)
    for i, cut in enumerate(cuts):
        copies[i][2].wait()
        for which in (1, 0):
            copies[i][which].wait()
            acc = jnp.dot(x_ref[:, cut], w_ref[which, cut], preferred_element_type=F32)
            if i == 0:
                acc_ref[which] = acc
            else:
                kv_finish(acc_ref[which] + acc, which, out_ref, cos_ref.at[0], sin_ref.at[0], buf_ref)


def middle_kernel(sc_ref, xo_ref, xp_ref, wk_ref, wv_ref, w_ref, cos_ref, sin_ref, send_ref, keep_ref, buf_ref):
    send_kernel(sc_ref, xo_ref, wk_ref, wv_ref, cos_ref, sin_ref, send_ref, buf_ref, part=0)
    half = buf_ref.shape[0] // 2
    kv_part(xp_ref, (w_ref.at[0], w_ref.at[1]), keep_ref, cos_ref.at[1], sin_ref.at[1], buf_ref.at[half:])


def send_kernel(sc_ref, x_ref, wk_ref, wv_ref, cos_ref, sin_ref, out_ref, buf_ref, *, part):
    width = out_ref.shape[0] * HEAD
    column = pl.ds(pl.multiple_of((1 - sc_ref[1]) * width, width), width)
    kv_part(x_ref, (wk_ref.at[:, column], wv_ref.at[:, column]), out_ref, cos_ref.at[part], sin_ref.at[part], buf_ref)


def q_kernel(sc_ref, xo_ref, xp_ref, cos_ref, sin_ref, w_ref, keepa_ref, keepb_ref, send0_ref, send1_ref,
             back_ref, buf_ref):
    tp, par = sc_ref[0], sc_ref[1]
    heads = keepa_ref.shape[0]
    width = heads * HEAD
    slot = 0
    for side in (1, 0):
        w = w_ref[:, pl.ds(pl.multiple_of((1 - par if side else par) * width, width), width)]
        for part, x_ref in enumerate((xo_ref, xp_ref)):
            acc = jnp.dot(x_ref[...], w, preferred_element_type=F32)
            for h in range(heads):
                val = rotated(acc[:, h * HEAD:(h + 1) * HEAD], cos_ref[part], sin_ref[part])
                if side:
                    place((send0_ref, send1_ref)[h], (), val, buf_ref, slot, tp if part == 0 else 1 - tp)
                else:
                    place((keepa_ref, keepb_ref)[part], (h,), val, buf_ref, slot, None)
                if h >= RELAYED and not side:
                    place(back_ref, (h - RELAYED, part), val, buf_ref, slot, None)
                slot += 1


def call(kernel, scalars, inputs, outputs, scratch, flops, aliases={}, limit=28, hbm=()):
    spaces = [pltpu.HBM if i in hbm else pltpu.VMEM for i in range(len(inputs))]
    return pl.pallas_call(
        kernel,
        in_specs=[pl.BlockSpec(memory_space=pltpu.SMEM)] + [pl.BlockSpec(memory_space=m) for m in spaces],
        out_specs=in_vmem(len(outputs)),
        out_shape=outputs,
        scratch_shapes=scratch,
        input_output_aliases=aliases,
        compiler_params=pltpu.CompilerParams(vmem_limit_bytes=limit * 2 ** 20),
        cost_estimate=pl.CostEstimate(flops=flops, transcendentals=0, bytes_accessed=0),
    )(scalars, *[pltpu.with_memory_space_constraint(x, pltpu.HBM) if i in hbm else x for i, x in enumerate(inputs)])


def gather(dst_ref, nq, sources):
    for r in range(FAR_DILATION):
        for source, block, half in sources:
            rows = nq if half is None else nq // 2
            start = 0 if half is None else half * (nq // 2)
            at = pl.multiple_of(r * 2 * nq + block * nq + start, TILE)
            dst_ref[pl.ds(at, rows), :] = source[r * rows:(r + 1) * rows, :]


def gather_kv(k_ref, v_ref, refs, nq, tp, par):
    places = ((par, tp), (par, 1 - tp), (1 - par, tp), (1 - par, 1 - tp))
    for which, dst_ref in enumerate((k_ref, v_ref)):
        gather(dst_ref, nq, [(ref.at[which], block, half) for ref, (block, half) in zip(refs, places)])


def scores_of(q, k):
    return lax.dot_general(q, k, (((1,), (1,)), ((), ())), preferred_element_type=F32)


def take(ref, rows):
    parts = [ref[a:a + n, :] for a, n in rows]
    return parts[0] if len(parts) == 1 else jnp.concatenate(parts, axis=0)


def put(ref, rows, value):
    at = 0
    for a, n in rows:
        ref[a:a + n, :] = value[at:at + n]
        at += n


def widened(stat, columns):
    return jnp.concatenate([stat] * (columns // HEAD), axis=1) if columns > HEAD else stat


def scored(item, q_ref, k_ref, s_ref, m_ref, fresh):
    rows, keys, bias, at = item
    if rows[0][1] < TILE:
        s = scores_of(take(q_ref, [(a, TILE) for a, _ in rows]), take(k_ref, keys))
        s = s.reshape(len(rows), TILE, s.shape[1])[:, :rows[0][1]].reshape(length(rows), s.shape[1])
    else:
        s = scores_of(take(q_ref, rows), take(k_ref, keys))
    if bias is not None:
        s = s + bias
    n, columns = s.shape
    s_ref[at:at + n, :columns] = s
    top = jnp.broadcast_to(jnp.max(s, axis=-1, keepdims=True), (n, HEAD))
    put(m_ref, rows, top if fresh else jnp.maximum(take(m_ref, rows), top))


def weighed(item, v_ref, s_ref, m_ref, columns):
    rows, keys, _, at = item
    n = sum(c for _, c in rows)
    p = jnp.exp2((s_ref[at:at + n, :columns] - widened(take(m_ref, rows), columns)) * SCALE).astype(BF16)
    v = take(v_ref, keys)
    return jnp.dot(p, jnp.concatenate([v, jnp.ones_like(v)], axis=1), preferred_element_type=F32)


def length(rows):
    return sum(n for _, n in rows)


def group_rows(r4, nq):
    return [((r4 + MIDDLE_DILATION * j) * 2 * nq, 2 * nq) for j in range(FAR_DILATION // MIDDLE_DILATION)]


def near_rows(c, nq):
    return [(r * 2 * nq + c * TILE, TILE) for r in range(FAR_DILATION)]


def upper_rows(c, nq):
    return [(a, REACH_STEPS // FAR_DILATION) for a, _ in near_rows(c, nq)]


def pair_rows(i, nq):
    return [(i * 4 * nq, 4 * nq)]


def near_of(tq, tk):
    return (tq - tk >= 0) & (tq - tk <= REACH_STEPS)


def every(tq, tk, step):
    return (tq % step == tk % step) & (tq - tk >= 0) & (tq - tk <= REACH_STEPS * step)


def bias_of(count):
    return np.where(count > 0, np.log2(np.maximum(count, 1)) / SCALE, MASKED).astype(np.float32)


def biases(nq):
    group = 2 * nq * FAR_DILATION
    j = np.arange(FAR_DILATION // MIDDLE_DILATION)[:, None]
    t = (np.arange(2 * nq)[None, :] * FAR_DILATION + j * MIDDLE_DILATION).reshape(-1)
    tq, tk = t[:, None], t[None, :]
    both = lambda tq, tk: every(tq, tk, MIDDLE_DILATION).astype(int) + every(tq, tk, FAR_DILATION)
    group0, group1 = both(tq, tk), both(tq + group, tk)
    r = np.arange(FAR_DILATION)[:, None]
    t = (np.arange(TILE)[None, :] * FAR_DILATION + r).reshape(-1)
    tq, tk = t[:, None], t[None, :]
    near0, near1 = near_of(tq, tk), near_of(tq + TILE * FAR_DILATION, tk)
    upper = near1.reshape(FAR_DILATION, TILE, -1)[:, :REACH_STEPS // FAR_DILATION].reshape(-1, near1.shape[1])
    r = np.arange(2)[:, None]
    t = (np.arange(2 * nq)[None, :] * FAR_DILATION + r).reshape(-1)
    pair2 = every(t[:, None] + 2 * group, t[None, :], FAR_DILATION)
    return [bias_of(np.asarray(x, int)) for x in (group0, group1, near0, near1, upper, pair2)]


def local_kernel(sc_ref, qa_ref, qb_ref, qy0_ref, qy1_ref, kva_ref, kvb_ref, kvya_ref, kvyb_ref, group_ref, near0_ref, near1_ref,
                 q_ref, m_ref, l_ref, o_ref, k_s, v_s, s_s):
    tp, par = sc_ref[0], sc_ref[1]
    nq = qy0_ref.shape[0] // FAR_DILATION
    for h in range(q_ref.shape[0]):
        q, m, l, o, k, v, sh = (x.at[h] for x in (q_ref, m_ref, l_ref, o_ref, k_s, v_s, s_s))
        gather(q, nq, [(qa_ref.at[h], par, tp), (qb_ref.at[h], par, 1 - tp), ((qy0_ref, qy1_ref)[h], 1 - par, None)])
        gather_kv(k, v, [x.at[h] for x in (kva_ref, kvb_ref, kvya_ref, kvyb_ref)], nq, tp, par)
        at = 0
        items = []
        for r4 in range(MIDDLE_DILATION):
            rows = group_rows(r4, nq)
            items.append((rows, rows, group_ref[...], at))
            scored(items[-1], q, k, sh, m, True)
            at += length(rows)
        for c in range(2 * nq // TILE):
            rows = near_rows(c, nq)
            items.append((rows, rows, near0_ref[...], at))
            scored(items[-1], q, k, sh, m, False)
            at += length(rows)
            if c:
                items.append((upper_rows(c, nq), near_rows(c - 1, nq), near1_ref[...], at))
                scored(items[-1], q, k, sh, m, False)
                at += length(items[-1][0])
        for i, item in enumerate(items):
            ol = weighed(item, v, sh, m, length(item[1]))
            if i < MIDDLE_DILATION:
                put(o, item[0], ol[:, :HEAD])
                put(l, item[0], ol[:, HEAD:])
            else:
                put(o, item[0], take(o, item[0]) + ol[:, :HEAD])
                put(l, item[0], take(l, item[0]) + ol[:, HEAD:])


def one_kernel(sc_ref, q_ref, m_in, l_in, o_in, kva_ref, kvb_ref, kvya_ref, kvyb_ref, group_ref, near_ref,
               m_ref, l_ref, o_ref, *refs, head):
    packs = head >= RELAYED
    k, v, sh, n = refs[packs:packs + 4]
    tp, par = sc_ref[0], sc_ref[1]
    nq = kvya_ref.shape[2] // FAR_DILATION * 2

    @pl.when(sc_ref[2] >= 1)
    def _():
        q, mi, li, oi, m, l, o = (x.at[head] for x in (q_ref, m_in, l_in, o_in, m_ref, l_ref, o_ref))
        gather_kv(k, v, [x.at[head] for x in (kva_ref, kvb_ref, kvya_ref, kvyb_ref)], nq, tp, par)
        near = (near_rows(0, nq), near_rows(2 * nq // TILE - 1, nq), near_ref[...], 0)
        at = length(near[0])
        items = []
        for r4 in range(MIDDLE_DILATION):
            rows = group_rows(r4, nq)
            items.append((rows, rows, group_ref[...], at))
            scored(items[-1], q, k, sh, n, True)
            at += length(rows)
        scored(near, q, k, sh, n, False)
        for item in items:
            rows = item[0]
            old = take(mi, rows)
            new = jnp.maximum(old, take(n, rows))
            keep = jnp.exp2((old - new) * SCALE)
            put(m, rows, new)
            ol = weighed(item, v, sh, m, length(item[1]))
            put(o, rows, take(oi, rows) * keep + ol[:, :HEAD])
            put(l, rows, take(li, rows) * keep + ol[:, HEAD:])
        ol = weighed(near, v, sh, m, length(near[1]))
        put(o, near[0], take(o, near[0]) + ol[:, :HEAD])
        put(l, near[0], take(l, near[0]) + ol[:, HEAD:])

    if packs:
        state_ref, piece_s, stat_s = refs[0], *refs[5:]
        for i in range(FAR_DILATION // 2):
            rows = pair_rows(i, nq)
            m, l, o = (take(x.at[head], rows) for x in (m_ref, l_ref, o_ref))
            pack_rows(piece_s, stat_s, i, o / l, m, l)
        pack_out(state_ref, piece_s, stat_s, 1 - par)


def two_kernel(sc_ref, q_ref, m_ref, l_ref, o_ref, kvo_ref, kvy_ref, pair_ref,
               keep_ref, send_ref, k_s, v_s, s_s, n_s, mix_s, *, head):
    tp, par = sc_ref[0], sc_ref[1]
    nq = kvy_ref.shape[2] // FAR_DILATION * 2
    q, m, l, o = (x.at[head] for x in (q_ref, m_ref, l_ref, o_ref))
    pairs = [pair_rows(i, nq) for i in range(FAR_DILATION // 2)]

    def settle(i, val):
        for part in range(4):
            r, block = 2 * i + part // 2, part % 2
            mix_s[block, pl.ds(r, nq, stride=FAR_DILATION), :] = val[part * nq:(part + 1) * nq]

    @pl.when(sc_ref[2] >= 2)
    def _():
        gather_kv(k_s, v_s, [kvo_ref.at[0], kvo_ref.at[1], kvy_ref.at[0], kvy_ref.at[1]], nq, tp, par)
        items = [(rows, rows, pair_ref[...], i * length(rows)) for i, rows in enumerate(pairs)]
        for item in items:
            put(n_s, item[0], take(m, item[0]))
            scored(item, q, k_s, s_s, n_s, False)
        for i, item in enumerate(items):
            rows = item[0]
            ol = weighed(item, v_s, s_s, n_s, length(rows))
            keep = jnp.exp2((take(m, rows) - take(n_s, rows)) * SCALE)
            settle(i, (take(o, rows) * keep + ol[:, :HEAD]) / (take(l, rows) * keep + ol[:, HEAD:]))

    @pl.when(sc_ref[2] < 2)
    def _():
        for i, rows in enumerate(pairs):
            settle(i, take(o, rows) / take(l, rows))

    keep_ref[...] = mix_s[pl.ds(par, 1)][0].astype(BF16)
    send_ref[...] = mix_s[pl.ds(1 - par, 1)][0].astype(BF16)


def diagonal(n):
    return lax.broadcasted_iota(jnp.int32, (n, n), 0) == lax.broadcasted_iota(jnp.int32, (n, n), 1)


def pack_rows(piece_s, stat_s, i, value, top, total):
    nq = value.shape[0] // 4
    eye = diagonal(HEAD)
    for part in range(4):
        r, block = 2 * i + part // 2, part % 2
        piece_s[block, r * nq:(r + 1) * nq, :] = value[part * nq:(part + 1) * nq].astype(BF16)
    for which, stat in enumerate((top, total)):
        at = which * (FAR_DILATION // 2) + i
        stat_s[at:at + 1, :] = jnp.sum(jnp.where(eye, stat, 0.0), axis=0, keepdims=True)


def pack_out(out_ref, piece_s, stat_s, block):
    rows, count = piece_s.shape[1], stat_s.shape[0]
    out_ref[:rows, :] = piece_s[pl.ds(block, 1)][0]
    rest = stat_s[...]
    for term in range(3):
        low = rest.astype(BF16)
        out_ref[rows + term * count:rows + (term + 1) * count, :] = low
        rest = rest - low.astype(F32)


def unpacked_stats(ref, rows):
    return sum(ref[rows + t * FAR_DILATION:rows + (t + 1) * FAR_DILATION, :].astype(F32) for t in range(3))


def foreign_kernel(sc_ref, qn_ref, kva_ref, kvb_ref, kvya_ref, kvyb_ref, pair_ref,
                   own_ref, diag_ref, q_s, k_s, v_s, s_s, n_s, piece_s, stat_s, *, head):
    tp, par = sc_ref[0], sc_ref[1]
    nq = kvya_ref.shape[2] // FAR_DILATION * 2
    half = kvya_ref.shape[2]
    gather(q_s, nq, [(qn_ref.at[0, :half], par, tp), (qn_ref.at[0, half:], par, 1 - tp), (qn_ref.at[1], 1 - par, None)])
    gather_kv(k_s, v_s, [x.at[head] for x in (kva_ref, kvb_ref, kvya_ref, kvyb_ref)], nq, tp, par)
    pairs = [pair_rows(i, nq) for i in range(FAR_DILATION // 2)]
    items = [(rows, rows, pair_ref[...], i * length(rows)) for i, rows in enumerate(pairs)]
    for item in items:
        scored(item, q_s, k_s, s_s, n_s, True)
    for i, item in enumerate(items):
        ol = weighed(item, v_s, s_s, n_s, length(item[0]))
        total = ol[:, HEAD:]
        pack_rows(piece_s, stat_s, i, ol[:, :HEAD] / total, take(n_s, item[0]), total)
    pack_out(own_ref, piece_s, stat_s, par)
    pack_out(diag_ref, piece_s, stat_s, 1 - par)


def final_kernel(sc_ref, m_ref, l_ref, o_ref, state_ref, own_ref, diag_ref, out_ref, mix_s, *, head):
    par = sc_ref[1]
    m, l, o = (x.at[head] for x in (m_ref, l_ref, o_ref))
    rows = out_ref.shape[1]
    nq = rows // FAR_DILATION
    count = FAR_DILATION // 2
    far = sc_ref[2] >= 2
    eye = diagonal(HEAD)

    def columns(ref):
        stats = unpacked_stats(ref, rows)
        result = []
        for i in range(2 * count):
            spread = jnp.sum(jnp.where(eye, stats[i:i + 1, :], 0.0), axis=1, keepdims=True)
            result.append(jnp.broadcast_to(spread, (HEAD, HEAD)))
        return result

    def rows_of(result, which, r):
        column = result[which * count + r // 2]
        at = (r % 2) * 2 * nq
        return jnp.where(par == 0, column[at:at + nq], column[at + nq:at + 2 * nq])

    def joined(top, total, numerator, ref, result, r):
        top2, total2 = rows_of(result, 0, r), rows_of(result, 1, r)
        top2 = jnp.where(far, top2, MASKED)
        new = jnp.maximum(top, top2)
        keep = jnp.exp2((top - new) * SCALE)
        add = jnp.where(far, jnp.exp2((top2 - new) * SCALE) * total2, 0.0)
        part = jnp.where(far, ref[r * nq:(r + 1) * nq, :].astype(F32), 0.0)
        return (numerator * keep + part * add) / (total * keep + add)

    own_stats, diag_stats, state_stats = columns(own_ref), columns(diag_ref), columns(state_ref)
    for r in range(FAR_DILATION):
        here = pl.ds(pl.multiple_of(r * 2 * nq + par * nq, TILE), nq)
        mix_s[0, pl.ds(r, nq, stride=FAR_DILATION), :] = joined(
            m[here, :], l[here, :], o[here, :], own_ref, own_stats, r)
        top, total = rows_of(state_stats, 0, r), rows_of(state_stats, 1, r)
        mix_s[1, pl.ds(r, nq, stride=FAR_DILATION), :] = joined(
            top, total, state_ref[r * nq:(r + 1) * nq, :].astype(F32) * total, diag_ref, diag_stats, r)
    out_ref[...] = mix_s[...].astype(BF16)


def out_kernel(sc_ref, a_ref, b_ref, c_ref, d_ref, own_ref, tp_ref, w_ref, o_ref):
    tp, par = sc_ref[0], sc_ref[1]
    block = o_ref.shape[1]
    heads = w_ref.shape[0] // HEAD // 4
    column = pl.multiple_of(pl.program_id(0) * block, block)
    order = (2 * tp + par, 2 * tp + 1 - par, 2 * (1 - tp) + par, 2 * (1 - tp) + 1 - par)
    x_refs = (own_ref.at[0], own_ref.at[1], tp_ref.at[0], tp_ref.at[1], a_ref, b_ref, c_ref, d_ref)
    x = jnp.concatenate([x_ref[...] for x_ref in x_refs], axis=1)
    w = jnp.concatenate([w_ref[pl.ds(pl.multiple_of((i * heads + head) * HEAD, HEAD), HEAD), pl.ds(column, block)]
                         for head in (1, 0) for i in order], axis=0)
    o_ref[...] = jnp.dot(x, w, preferred_element_type=F32).astype(BF16)


def out_project(scalars, first, last, weight):
    rows, columns = first[0].shape[0], weight.shape[1]
    steps = 2
    return pl.pallas_call(
        out_kernel,
        grid=(steps,),
        in_specs=[pl.BlockSpec(memory_space=pltpu.SMEM)] + in_vmem(7),
        out_specs=pl.BlockSpec((rows, columns // steps), lambda j: (0, j)),
        out_shape=jax.ShapeDtypeStruct((rows, columns), BF16),
        compiler_params=pltpu.CompilerParams(vmem_limit_bytes=16 * 2 ** 20),
        cost_estimate=pl.CostEstimate(flops=2 * rows * weight.size, transcendentals=0, bytes_accessed=0),
        name="out_project",
    )(scalars, *first, *last, weight)


def swap(x, axis):
    return lax.ppermute(x, axis, [(i, i ^ 1) for i in range(lax.axis_size(axis))])


def onward(x):
    n = lax.axis_size("sp")
    return lax.ppermute(x, "sp", [(i, i + 2) for i in range(n - 2)])


def body(tokens, query_weight, key_weight, value_weight, output_weight):
    half, depth = tokens.shape
    rows = 2 * half
    group = 2 * rows
    nq = rows // FAR_DILATION
    assert 2 * group == FAR_DILATION * REACH_STEPS
    heads = query_weight.shape[1] // HEAD // 2
    width = heads * HEAD
    flops = 2 * rows * depth * width
    sp, tp = lax.axis_index("sp"), lax.axis_index("tp")
    scalars = jnp.stack([tp, sp % 2, sp // 2, sp]).astype(jnp.int32)
    inverse = THETA_BASE ** (-jnp.arange(HEAD // 2, dtype=F32) / (HEAD // 2))
    inverse = jnp.concatenate([inverse, inverse])[None]
    group0, group1, near0, near1, upper, pair2 = biases(nq)
    shape = jax.ShapeDtypeStruct
    kv = shape((heads, 2, half, HEAD), BF16)
    q_shape, q_half = shape((rows, HEAD), BF16), shape((heads, half, HEAD), BF16)
    table = shape((2, half, HEAD), F32)
    buffers = pltpu.VMEM((4 * heads, half, HEAD), F32)

    partner = swap(tokens, "tp")
    weights = shape((2, depth, width), BF16)
    kv_a, own, w_keep, cosine, sine = call(
        own_keep_kernel, scalars, [tokens, key_weight, value_weight, inverse],
        [kv, shape((half, depth), BF16), weights, table, table],
        [buffers, pltpu.VMEM((2, half, width), F32), pltpu.SemaphoreType.DMA((2, 3))], flops, hbm=(0, 1, 2))
    kv1_a = onward(kv_a)
    key_weight, value_weight, own = lax.optimization_barrier((key_weight, value_weight, own))
    send_a, kv_b = call(
        middle_kernel, scalars, [own, partner, key_weight, value_weight, w_keep, cosine, sine], [kv, kv], [buffers],
        2 * flops)
    kv1_b = onward(kv_b)
    kv_ya = swap(send_a, "sp")
    send_b, = call(functools.partial(send_kernel, part=1), scalars, [partner, key_weight, value_weight, cosine, sine],
                   [kv], [buffers],
                   flops)
    kv_yb = swap(send_b, "sp")
    back = shape((heads - RELAYED, 2, half, HEAD), BF16)
    q_a, q_b, q_send0, q_send1, back_own = call(
        q_kernel, scalars, [own, partner, cosine, sine, query_weight], [q_half, q_half, q_shape, q_shape, back],
        [buffers], 2 * flops)
    q_y1 = swap(q_send1, "sp")
    q_y0 = swap(q_send0, "sp")
    behind = jnp.stack([back_own.reshape(rows, HEAD), q_y1])
    n = lax.axis_size("sp")
    q_next = lax.ppermute(behind, "sp", [(i, i - 2) for i in range(2, n)])
    kv1_ya = onward(kv_ya)
    kv1_yb = onward(kv_yb)
    kv2_ab = onward(jnp.stack([kv1_a[0], kv1_b[0]]))
    kv2_y = onward(jnp.stack([kv1_ya[0], kv1_yb[0]]))
    packed = shape((rows + 3 * FAR_DILATION, HEAD), BF16)
    packing = [pltpu.VMEM((2, rows, HEAD), BF16), pltpu.VMEM((FAR_DILATION, HEAD), F32)]
    piece_own, piece_diag = call(
        functools.partial(foreign_kernel, head=1), scalars,
        [q_next, kv1_a, kv1_b, kv1_ya, kv1_yb, pair2], [packed, packed],
        [pltpu.VMEM((group, HEAD), BF16)] * 3 + [pltpu.VMEM((group, HEAD), F32)] * 2 + packing, 10 ** 9)
    n = lax.axis_size("sp")
    piece_diag = lax.ppermute(piece_diag, "sp", [(i, (i ^ 1) + 2) for i in range(n - 2)])
    piece_own = onward(piece_own)
    state = shape((heads, group, HEAD), F32)
    kv_scratch = [pltpu.VMEM((heads, group, HEAD), BF16)] * 2
    q, m, l, o = call(
        local_kernel, scalars, [q_a, q_b, q_y0, q_y1, kv_a, kv_b, kv_ya, kv_yb, group0, near0, upper],
        [shape((heads, group, HEAD), BF16), state, state, state],
        kv_scratch + [pltpu.VMEM((heads, 3 * group, 2 * HEAD), F32)], 3 * 10 ** 9)
    one_scratch = [pltpu.VMEM((group, HEAD), BF16)] * 2 + [
        pltpu.VMEM((2 * group, 2 * HEAD), F32), pltpu.VMEM((group, HEAD), F32)]
    known = [kv1_a, kv1_b, kv1_ya, kv1_yb, group1, near1]
    m, l, o, state_y = call(
        functools.partial(one_kernel, head=1), scalars, [q, m, l, o, *known], [state, state, state, packed],
        one_scratch + packing, 10 ** 9, {2: 0, 3: 1, 4: 2})
    m, l, o = call(
        functools.partial(one_kernel, head=0), scalars, [q, m, l, o, *known], [state, state, state],
        one_scratch, 10 ** 9, {2: 0, 3: 1, 4: 2})
    state_y = swap(state_y, "sp")
    mixed = shape((rows, HEAD), BF16)
    keep, send = call(
        functools.partial(two_kernel, head=0), scalars, [q, m, l, o, kv2_ab, kv2_y, pair2],
        [mixed, mixed], [pltpu.VMEM((group, HEAD), BF16)] * 2 + [pltpu.VMEM((group, HEAD), F32)] * 2
        + [pltpu.VMEM((2, rows, HEAD), F32)], 10 ** 9)
    keep_tp = swap(keep, "tp")
    from_y = swap(send, "sp")
    first = [keep, from_y, keep_tp, swap(from_y, "tp")]
    last, = call(functools.partial(final_kernel, head=1), scalars, [m, l, o, state_y, piece_own, piece_diag],
                 [shape((2, rows, HEAD), BF16)], [pltpu.VMEM((2, rows, HEAD), F32)], 10 ** 9)
    last_tp = swap(last, "tp")
    return out_project(scalars, first, [last, last_tp], output_weight)


def solution(mesh):
    in_specs = (
        P(("grp", "sp", "tp"), None),
        P(None, "tp"),
        P(None, "tp"),
        P(None, "tp"),
        P(None, "tp"),
    )
    out_specs = P(("grp", "sp"), "tp")

    return jax.shard_map(body, mesh=mesh, in_specs=in_specs, out_specs=out_specs, check_vma=False)
```
